512 devices in a mesh: grp: 2 (over y), sp: 32 (over z, core), tp: 8 (over x).
Axes of the slice: x: 8, y: 2, z: 16, core: 2. Of those that a mesh axis runs over, the one named last changes fastest.
The devices are a block of a 8x8x16 slice.
Arguments:
- query_a: bfloat16 [16384, 2048], P(('grp', 'sp'), 'tp'), parts along dimension 0, may hold values from -6 to 6
- key_a: bfloat16 [16384, 2048], P(('grp', 'sp'), 'tp'), parts along dimension 0, may hold values from -6 to 6
- value_a: bfloat16 [16384, 4096], P(('grp', 'sp'), 'tp'), parts along dimension 0, may hold values from -6 to 6
- decay_a: float32 [2, 8, 16384], P(None, 'tp', ('grp', 'sp')), parts along dimension 2, may hold values from -1 to 0
- query_b: bfloat16 [16384, 1024], P(('grp', 'sp'), 'tp'), parts along dimension 0, may hold values from -6 to 6
- key_b: bfloat16 [16384, 1024], P(('grp', 'sp'), 'tp'), parts along dimension 0, may hold values from -6 to 6
- value_b: bfloat16 [16384, 1024], P(('grp', 'sp'), 'tp'), parts along dimension 0, may hold values from -6 to 6
- decay_b: float32 [2, 16, 16384], P(None, 'tp', ('grp', 'sp')), parts along dimension 2, may hold values from -1 to 0
- out_weight_a: bfloat16 [4096, 2048], P('tp'), may hold values from -0.078125 to 0.078125
- out_weight_b: bfloat16 [1024, 2048], P('tp'), may hold values from -0.078125 to 0.078125
- residual: bfloat16 [16384, 2048], P(('grp', 'sp', 'tp')), parts along dimension 0, may hold values from -6 to 6
- norm_gain: float32 [2, 2048], replicated, may hold values from 0.1 to 1.9
- route_group: int32 [16384], P(('grp', 'sp', 'tp')), parts along dimension 0, may hold values from 0 to 3
- route_expert: int32 [16384, 2], P(('grp', 'sp', 'tp')), parts along dimension 0, may hold values from 0 to 7, as said below
- route_weight: float32 [16384, 2], P(('grp', 'sp', 'tp')), parts along dimension 0, may hold values from 0.2 to 1
- expert_gate: bfloat16 [32, 2048, 1024], P('sp', None, 'tp'), may hold values from -0.125 to 0.125
- expert_up: bfloat16 [32, 2048, 1024], P('sp', None, 'tp'), may hold values from -0.125 to 0.125
- expert_down: bfloat16 [32, 1024, 2048], P('sp', 'tp'), may hold values from -0.1875 to 0.1875
Outputs:
- layer_out: bfloat16 [16384, 2048], P(('grp', 'sp', 'tp')), parts along dimension 0
The draws below stay inside these ranges and needn't reach their ends.
There are 2 independent parts, one for each index of `grp`. The reference program is written for one: setup_inputs(seed, part) draws one part's arguments, and reference() takes and returns one part's arrays. A program takes and returns all parts, laid end to end along the dimension named above; an argument that names none is the same for every part. Nothing has to cross between parts.
Inputs may be any that keep to these rules, and one draw needn't show every extreme that they name: `route_expert`: the 2 entries of a row are different.
All inputs are finite; a program needn't handle non-finite values.
Results may differ from the reference program's by a relative error of at most 0.015.
Values may be sent and summed in bfloat16 or wider, within the bound.
No kernel may reach another device: no remote copies, remote signals or barrier semaphores. Data moves between devices by JAX's collectives and lax.ppermute only.
A program may use at most 128 MiB of HBM per device.

```python
import math
import jax
import jax.numpy as jnp
from jax import lax

D = 2048
HA = 8
DKA = 256
DVA = 512
HB = 16
DKB = 64
DVB = 64
BLOCK = 128
EXPERTS = 32
GROUPS = 4
FF = 1024
TOP = 2
CAP = 2
TOK_DEV = 256
TOKENS = 8192
ROWS_DEV = 32
EXP_GROUP = 8
N_TP = 8


def decay_law(key, number_of_heads):
    sequence_length = TOKENS
    key_rows = jax.random.split(key, 6)
    fast = jax.random.randint(key_rows[0], (2, number_of_heads), 0, 2) == 0
    fast_rate = jnp.exp(jax.random.uniform(key_rows[1], (2, number_of_heads), jnp.float32, jnp.log(0.01), jnp.log(1.0 / 30.0)))
    slow_rate = jnp.exp(jax.random.uniform(key_rows[2], (2, number_of_heads), jnp.float32, jnp.log(0.1), jnp.log(0.4))) / sequence_length
    rate = jnp.where(fast, fast_rate, slow_rate)
    devices = sequence_length // TOK_DEV
    factor = jnp.exp(jax.random.uniform(key_rows[3], (2, number_of_heads, devices), jnp.float32, -jnp.log(2.0), jnp.log(2.0)))
    factor = jnp.repeat(factor, TOK_DEV, axis=2)
    smoothing_factor = -rate[..., None] * factor
    spike_location = jax.random.randint(key_rows[4], (2, number_of_heads, 2), 0, sequence_length)
    spike_penalty = jnp.log(jax.random.uniform(key_rows[5], (2, number_of_heads, 2), jnp.float32, 0.5, 0.8))
    token_positions = jnp.arange(sequence_length, dtype=jnp.int32)
    spike_events = jnp.sum(jnp.where(token_positions[None, None, None, :] == spike_location[..., None], spike_penalty[..., None], 0.0), axis=2)
    return (smoothing_factor + spike_events).astype(jnp.float32)


def draw_decay_a(key, part):
    return decay_law(jax.random.fold_in(key, 11), HA)


def draw_decay_b(key, part):
    return decay_law(jax.random.fold_in(key, 12), HB)


def route_law(key):
    key_rows = jax.random.split(jax.random.fold_in(key, 7), 6)
    blocks = TOKENS // ROWS_DEV
    favored = jax.random.randint(key_rows[0], (), 0, EXPERTS)
    favored_group = favored // EXP_GROUP
    favored_slot = favored % EXP_GROUP
    group_draw = jax.random.randint(key_rows[1], (TOKENS,), 0, 2 * GROUPS)
    group_ids = jnp.where(group_draw >= GROUPS, favored_group, group_draw)
    first_pick = jax.random.randint(key_rows[2], (TOKENS,), 0, EXP_GROUP)
    leaning = (jax.random.randint(key_rows[3], (TOKENS,), 0, 3) == 0) & (group_ids == favored_group)
    first_pick = jnp.where(leaning, favored_slot, first_pick)
    scores = jax.random.randint(key_rows[4], (blocks, ROWS_DEV), 0, 1 << 20) * ROWS_DEV + jnp.arange(ROWS_DEV, dtype=jnp.int32)[None, :]
    ranking = jnp.argsort(jnp.argsort(scores, axis=1), axis=1)
    forced = (ranking < CAP).reshape(TOKENS)
    group_ids = jnp.where(forced, favored_group, group_ids)
    first_pick = jnp.where(forced, favored_slot, first_pick)
    second_pick = (first_pick + 1 + jax.random.randint(key_rows[5], (TOKENS,), 0, EXP_GROUP - 1)) % EXP_GROUP
    return (group_ids.astype(jnp.int32), jnp.stack([first_pick, second_pick], axis=1).astype(jnp.int32))


def draw_route_group(key, part):
    return route_law(key)[0]


def draw_route_expert(key, part):
    return route_law(key)[1]


def levels(own_key, extent, shards, least, largest):
    level = 1.0
    for dim, blocks in shards:
        steps = jax.random.uniform(jax.random.fold_in(jax.random.fold_in(own_key, 6), dim), (blocks,), jnp.float32, least / len(shards), largest / len(shards))
        level = level * jnp.repeat(jnp.exp(steps), extent[dim] // blocks).reshape((-1,) + (1,) * (len(extent) - 1 - dim))
    return level


def noise(key, extent, deviation, bound, cuts=(), held_as=jnp.bfloat16):
    values = deviation * jax.random.normal(key, extent, jnp.float32)
    if cuts:
        values = values * levels(key, extent, cuts, -0.22, 0.18)
    return jnp.clip(values, -bound, bound).astype(held_as)


def setup_inputs(seed: int = 0, part: int = 0) -> dict:
    splits = jax.random.split(jax.random.key(seed), 19)
    part_keys = jax.random.split(jax.random.fold_in(splits[18], part), 19)
    query_a = noise(part_keys[0], (TOKENS, HA * DKA), 1.0, 6.0, ((0, 32), (1, 8)))
    key_a = noise(part_keys[1], (TOKENS, HA * DKA), 1.0, 6.0, ((0, 32), (1, 8)))
    value_a = noise(part_keys[2], (TOKENS, HA * DVA), 1.0, 6.0, ((0, 32), (1, 8)))
    decay_a = draw_decay_a(jax.random.fold_in(jax.random.fold_in(splits[18], part), 71), part)
    query_b = noise(part_keys[4], (TOKENS, HB * DKB), 1.0, 6.0, ((0, 32), (1, 8)))
    key_b = noise(part_keys[5], (TOKENS, HB * DKB), 1.0, 6.0, ((0, 32), (1, 8)))
    value_b = noise(part_keys[6], (TOKENS, HB * DVB), 1.0, 6.0, ((0, 32), (1, 8)))
    decay_b = draw_decay_b(jax.random.fold_in(jax.random.fold_in(splits[18], part), 71), part)
    out_weight_a = noise(splits[8], (HA * DVA, D), (HA * DVA + HB * DVB) ** -0.5, 0.078125, ((0, 8),))
    out_weight_b = noise(splits[9], (HB * DVB, D), (HA * DVA + HB * DVB) ** -0.5, 0.078125, ((0, 8),))
    residual = noise(part_keys[10], (TOKENS, D), 1.0, 6.0, ((0, 256),))
    norm_gain = jnp.clip(1.0 + 0.18 * jax.random.normal(splits[11], (2, D), jnp.float32), 0.1, 1.9)
    route_group = draw_route_group(jax.random.fold_in(jax.random.fold_in(splits[18], part), 71), part)
    route_expert = draw_route_expert(jax.random.fold_in(jax.random.fold_in(splits[18], part), 71), part)
    route_weight = jnp.clip(0.2 + 0.8 * jax.random.uniform(part_keys[14], (TOKENS, TOP), jnp.float32) ** levels(part_keys[14], (TOKENS, TOP), ((0, 256),), -0.2, 0.2), 0.2, 1.0)
    expert_gate = noise(splits[15], (EXPERTS, D, FF), D ** -0.5, 0.125, ((0, 32), (2, 8)))
    expert_up = noise(splits[16], (EXPERTS, D, FF), D ** -0.5, 0.125, ((0, 32), (2, 8)))
    expert_down = noise(splits[17], (EXPERTS, FF, D), FF ** -0.5, 0.1875, ((0, 32), (1, 8)))
    return {"query_a": query_a, "key_a": key_a, "value_a": value_a, "decay_a": decay_a, "query_b": query_b, "key_b": key_b, "value_b": value_b, "decay_b": decay_b, "out_weight_a": out_weight_a, "out_weight_b": out_weight_b, "residual": residual, "norm_gain": norm_gain, "route_group": route_group, "route_expert": route_expert, "route_weight": route_weight, "expert_gate": expert_gate, "expert_up": expert_up, "expert_down": expert_down}


HIGHEST = lax.Precision.HIGHEST
RESIDUAL_SCALE = math.sqrt(2.0)
NORM_EPS = 1e-05
GROUP_EPS = 1e-06
ROPE_BASE = 10000.0

def rotate(vectors, token_positions):
    half_width = vectors.shape[-1] // 2
    frequencies = ROPE_BASE ** (-jnp.arange(half_width, dtype=jnp.float32) / half_width)
    angles = token_positions.astype(jnp.float32)[:, None] * frequencies[None, :]
    cosine = jnp.cos(angles)[:, None, :]
    sine_part = jnp.sin(angles)[:, None, :]
    first_half = vectors[..., :half_width].astype(jnp.float32)
    second = vectors[..., half_width:].astype(jnp.float32)
    return jnp.concatenate([first_half * cosine - second * sine_part, first_half * sine_part + second * cosine], axis=-1)

def sweep_blocks(queries, keys_rot, values, log_decay, strict, state_init, span_size):
    length, number_of_heads, key_dim = queries.shape
    value_dim = values.shape[-1]
    block_count = length // span_size

    def split_blocks(array):
        return array.reshape(block_count, span_size, number_of_heads, array.shape[-1])
    decay_blocks = log_decay.reshape(number_of_heads, block_count, span_size).transpose(1, 0, 2)
    position_index = jnp.arange(span_size)
    if strict:
        allowed = position_index[:, None] > position_index[None, :]
    else:
        allowed = position_index[:, None] >= position_index[None, :]

    def advance(state_now, inputs):
        query_blk, key_blk, value_blk, decay_blk = inputs
        cumulative = jnp.cumsum(decay_blk, axis=1)
        log_gap = cumulative[:, :, None] - cumulative[:, None, :]
        weights = jnp.where(allowed[None], jnp.exp(jnp.where(allowed[None], log_gap, 0.0)), 0.0)
        scores = jnp.einsum('ihd,jhd->hij', query_blk, key_blk, preferred_element_type=jnp.float32) * weights
        weighted = scores.astype(jnp.bfloat16)
        inner_part = jnp.einsum('hij,jhv->ihv', weighted, value_blk, preferred_element_type=jnp.float32)
        carried = jnp.einsum('ihd,hdv->ihv', query_blk.astype(jnp.float32), state_now, precision=HIGHEST) * jnp.exp(cumulative).T[:, :, None]
        key_scaled = key_blk.astype(jnp.float32) * jnp.exp(cumulative[:, -1:] - cumulative).T[:, :, None]
        state_next = state_now * jnp.exp(cumulative[:, -1])[:, None, None] + jnp.einsum('jhd,jhv->hdv', key_scaled, value_blk.astype(jnp.float32), precision=HIGHEST)
        return (state_next, inner_part + carried)
    final_state, outputs = lax.scan(advance, state_init, (split_blocks(queries), split_blocks(keys_rot), split_blocks(values), decay_blocks))
    return (outputs.reshape(length, number_of_heads, value_dim), final_state)

def retain(query_w, key_w, value_w, decay, number_of_heads):
    sequence_length = query_w.shape[0]
    token_positions = jnp.arange(sequence_length, dtype=jnp.int32)
    queries_f = rotate(query_w.reshape(sequence_length, number_of_heads, -1), token_positions)
    key_dim = queries_f.shape[-1]
    queries = queries_f.astype(jnp.bfloat16)
    keys_rot = (rotate(key_w.reshape(sequence_length, number_of_heads, -1), token_positions) * (1.0 / math.sqrt(key_dim))).astype(jnp.bfloat16)
    values = value_w.reshape(sequence_length, number_of_heads, -1)
    zero_state = jnp.zeros((number_of_heads, key_dim, values.shape[-1]), jnp.float32)
    forward = sweep_blocks(queries, keys_rot, values, decay[0], False, zero_state, BLOCK)[0]
    backward = sweep_blocks(queries[::-1], keys_rot[::-1], values[::-1], decay[1][:, ::-1], True, zero_state, BLOCK)[0]
    total_sum = forward + backward[::-1]
    normed = total_sum * lax.rsqrt(lax.optimization_barrier(jnp.mean(total_sum * total_sum, axis=-1, keepdims=True)) + GROUP_EPS)
    return normed.reshape(sequence_length, -1).astype(jnp.bfloat16)

def layer_norm(stream, gain):
    center = stream - lax.optimization_barrier(jnp.mean(stream, axis=-1, keepdims=True))
    spread = lax.optimization_barrier(jnp.mean(center * center, axis=-1, keepdims=True))
    return center * lax.rsqrt(spread + NORM_EPS) * gain

def slot_table(expert_ids):
    onehot = (expert_ids[..., None] == jnp.arange(EXPERTS, dtype=jnp.int32)).astype(jnp.int32)
    earlier = jnp.cumsum(onehot, axis=-2) - onehot
    rank_order = lax.optimization_barrier(jnp.sum(earlier * onehot, axis=-1))
    kept_mask = rank_order < CAP
    slot_index = expert_ids * CAP + jnp.minimum(rank_order, CAP - 1)
    return (slot_index.astype(jnp.int32), kept_mask)

def reference(query_a, key_a, value_a, decay_a, query_b, key_b, value_b, decay_b, out_weight_a, out_weight_b, residual, norm_gain, route_group, route_expert, route_weight, expert_gate, expert_up, expert_down):
    sequence_length = query_a.shape[0]
    mixed_a = retain(query_a, key_a, value_a, decay_a, HA)
    mixed_b = retain(query_b, key_b, value_b, decay_b, HB)
    shard_a = mixed_a.reshape(sequence_length, N_TP, -1).transpose(1, 0, 2)
    shard_b = mixed_b.reshape(sequence_length, N_TP, -1).transpose(1, 0, 2)
    weight_a = out_weight_a.reshape(N_TP, -1, D)
    weight_b = out_weight_b.reshape(N_TP, -1, D)

    def add_partial(total_sum, pieces):
        partial_value = jnp.dot(pieces[0], pieces[1], preferred_element_type=jnp.float32) + jnp.dot(pieces[2], pieces[3], preferred_element_type=jnp.float32)
        rounded = lax.optimization_barrier(partial_value.astype(jnp.bfloat16))
        return (total_sum + rounded.astype(jnp.float32), None)
    mix = lax.scan(add_partial, jnp.zeros((sequence_length, D), jnp.float32), (shard_a, weight_a, shard_b, weight_b))[0]
    hidden_in = layer_norm(RESIDUAL_SCALE * residual.astype(jnp.float32) + mix, norm_gain[0]).astype(jnp.bfloat16)
    blocks = sequence_length // ROWS_DEV
    slots = EXPERTS * CAP
    global_ids = route_group[:, None] * EXP_GROUP + route_expert
    slot_index, kept_mask = slot_table(global_ids.reshape(blocks, ROWS_DEV * TOP).astype(jnp.int32))
    hits = (slot_index[..., None] == jnp.arange(slots, dtype=jnp.int32)) & kept_mask[..., None]
    choose = lax.optimization_barrier(jnp.sum(hits.reshape(blocks, ROWS_DEV, TOP, slots).astype(jnp.float32), axis=2))
    outgoing = jnp.einsum('brs,brd->bsd', choose, hidden_in.reshape(blocks, ROWS_DEV, D).astype(jnp.float32))
    outgoing = outgoing.astype(jnp.bfloat16).reshape(blocks, EXPERTS, CAP, D).transpose(1, 0, 2, 3).reshape(EXPERTS, blocks * CAP, D)

    def expert_apply(inputs):
        rows, gate_w, up_w, down_w = inputs
        gate_part = jnp.dot(rows, gate_w, preferred_element_type=jnp.float32)
        up_part = jnp.dot(rows, up_w, preferred_element_type=jnp.float32)
        expert_hidden = (jax.nn.silu(gate_part) * up_part).astype(jnp.bfloat16)
        hidden_sets = expert_hidden.reshape(rows.shape[0], N_TP, -1).transpose(1, 0, 2)
        down_sets = down_w.reshape(N_TP, -1, D)

        def add_set(total_sum, pieces):
            partial_value = jnp.dot(pieces[0], pieces[1], preferred_element_type=jnp.float32)
            rounded = lax.optimization_barrier(partial_value.astype(jnp.bfloat16))
            return (total_sum + rounded.astype(jnp.float32), None)
        expert_sum = lax.scan(add_set, jnp.zeros((rows.shape[0], D), jnp.float32), (hidden_sets, down_sets))[0]
        return expert_sum.astype(jnp.bfloat16)
    expert_out = lax.map(expert_apply, (outgoing, expert_gate, expert_up, expert_down))
    returned = expert_out.reshape(EXPERTS, blocks, CAP, D).transpose(1, 0, 2, 3).reshape(blocks, slots, D)
    picked = jnp.take_along_axis(returned, slot_index[..., None], axis=1).astype(jnp.float32)
    picked = picked.reshape(blocks, ROWS_DEV, TOP, D)
    factor = jnp.where(kept_mask.reshape(blocks, ROWS_DEV, TOP), route_weight.reshape(blocks, ROWS_DEV, TOP), 0.0)
    ffn = lax.optimization_barrier(jnp.sum(picked * factor[..., None], axis=2)).reshape(sequence_length, D)
    return layer_norm(RESIDUAL_SCALE * hidden_in.astype(jnp.float32) + ffn, norm_gain[1]).astype(jnp.bfloat16)
```

```python
import math

import jax
import jax.numpy as jnp
import numpy as np
from jax import lax
from jax.experimental import pallas as pl
from jax.experimental.pallas import tpu as pltpu
from jax.sharding import Mesh
from jax.sharding import PartitionSpec as P

CAP = 2
TOP = 2
EXP_GROUP = 8
SP = ("sp_0", "sp_1")
GRP_SP = ("grp", "sp_0", "sp_1")
GRP_SP_TP = ("grp", "sp_0", "sp_1", "tp")

RESIDUAL_SCALE = math.sqrt(2.0)
NORM_EPS = 1e-05
GROUP_EPS = 1e-06
ROPE_BASE = 10000.0

F32 = jnp.float32
BF16 = jnp.bfloat16
HIGHEST = lax.Precision.HIGHEST
INTERPRET = False

LANES = 128
TILE = 16


def vmem(count):
    return [pl.BlockSpec(memory_space=pltpu.VMEM)] * count


SMEM_SPEC = pl.BlockSpec(memory_space=pltpu.SMEM)


def iota(shape, dim):
    return lax.broadcasted_iota(jnp.int32, shape, dim)


def mm(a, b):
    return jnp.dot(a, b, preferred_element_type=F32)


def mm_nt(a, b, precision=None):
    return lax.dot_general(
        a, b, (((1,), (1,)), ((), ())), precision=precision, preferred_element_type=F32
    )


def split2(x):
    hi = x.astype(BF16).astype(F32)
    return hi, x - hi


def angle_tables(length, half_a, half_b, devices):
    def freqs(half):
        f = np.float32(ROPE_BASE) ** (-np.arange(half, dtype=np.float32) / np.float32(half))
        return f.astype(np.float64)

    fa = freqs(half_a)
    fb = np.tile(freqs(half_b), LANES // half_b)
    inside = np.arange(length, dtype=np.float64)[:, None]
    first = (np.arange(devices, dtype=np.float64) * length)[:, None]
    local = np.stack(
        [np.cos(inside * fa), np.sin(inside * fa), np.cos(inside * fb), np.sin(inside * fb)]
    ).astype(np.float32)
    base = np.zeros((devices, 8, LANES), np.float32)
    for k, row in enumerate(
        [np.cos(first * fa), np.sin(first * fa), np.cos(first * fb), np.sin(first * fb)]
    ):
        base[:, k, :] = row
    return local, base


def retention_body(
    qa_ref, ka_ref, va_ref, qb_ref, kb_ref, vb_ref, dec_ref, tab_ref, base_ref,
    qa_out, qb_out, loc_out, pay_out,
):
    n, dk = qa_ref.shape
    dv = va_ref.shape[1]
    half = dk // 2
    hb = qb_ref.shape[1] // 2
    hq = hb // 2
    row, col = iota((n, n), 0), iota((n, n), 1)
    dec = dec_ref[...]
    cr = jnp.dot(dec, (row <= col).astype(F32), precision=HIGHEST, preferred_element_type=F32)
    cc = mm_nt((col <= row).astype(F32), dec, HIGHEST)
    er = cr - dec
    ec = mm_nt((col < row).astype(F32), dec, HIGHEST)
    tot = cr[:, n - 1 : n]

    def pair_weights(h):
        forward = cc[:, h : h + 1] - cr[h : h + 1, :]
        backward = er[3 + h : 4 + h, :] - ec[:, 3 + h : 4 + h]
        return jnp.exp(jnp.where(col <= row, forward, backward))

    base = base_ref[...]
    cos_a = tab_ref[0] * base[0:1] - tab_ref[1] * base[1:2]
    sin_a = tab_ref[1] * base[0:1] + tab_ref[0] * base[1:2]

    def rotate_a(x, scale):
        x1, x2 = x[:, :half].astype(F32), x[:, half:].astype(F32)
        out = jnp.concatenate([x1 * cos_a - x2 * sin_a, x1 * sin_a + x2 * cos_a], axis=1)
        return (out * scale).astype(BF16)

    qa = rotate_a(qa_ref[...], 1.0)
    ka = rotate_a(ka_ref[...], 1.0 / math.sqrt(dk))
    qa_out[...] = qa

    width = 2 * hb
    lane = iota((n, width), 1)
    cos_b = tab_ref[2] * base[2:3] - tab_ref[3] * base[3:4]
    sin_b = tab_ref[3] * base[2:3] + tab_ref[2] * base[3:4]
    low = (lane % hb) < hq
    sin_b = jnp.where(low, -sin_b, sin_b)
    pr, pc = iota((width, width), 0), iota((width, width), 1)
    partner = jnp.where((pc % hb) < hq, pc + hq, pc - hq)
    swap = (pr == partner).astype(BF16)

    def rotate_b(x, scale):
        return ((x.astype(F32) * cos_b + mm(x, swap) * sin_b) * scale).astype(BF16)

    qb = rotate_b(qb_ref[...], 1.0)
    kb = rotate_b(kb_ref[...], 1.0 / math.sqrt(hb))
    qb_out[...] = qb

    va, vb = va_ref[...], vb_ref[...]
    kat = ka.astype(F32).T
    kbt = kb.astype(F32).T
    top = iota((width, n), 0) < hb
    for d in range(2):
        if d == 0:
            scale = [jnp.exp(tot[h : h + 1] - cr[h : h + 1, :]) for h in range(3)]
        else:
            scale = [jnp.exp(er[3 + h : 4 + h, :]) for h in range(3)]
        state = mm((kat * scale[0]).astype(BF16), va)
        pay_out[d, :dk, :] = state.astype(BF16)
        both = mm((kbt * jnp.where(top, scale[1], scale[2])).astype(BF16), vb)
        packed = jnp.where(iota((hb, width), 1) < hb, both[:hb], both[hb:]).astype(BF16)
        for q in range(dv // LANES):
            pay_out[d, dk : dk + TILE, q * LANES : (q + 1) * LANES] = packed[
                q * TILE : (q + 1) * TILE
            ]
        rows = iota((TILE, dv), 0)
        logs = jnp.zeros((TILE, dv), F32)
        for h in range(3):
            hi, lo = split2(tot[3 * d + h : 3 * d + h + 1])
            logs = jnp.where(rows == 2 * h, hi, jnp.where(rows == 2 * h + 1, lo, logs))
        pay_out[d, dk + TILE : dk + 2 * TILE, :] = logs.astype(BF16)
    weighted = (mm_nt(qa, ka) * pair_weights(0)).astype(BF16)
    loc_out[:, :dv] = mm(weighted, va)
    acc = jnp.zeros((n, width), F32)
    for h in range(2):
        mine = (lane < hb) if h == 0 else (lane >= hb)
        q_h = jnp.where(mine, qb.astype(F32), 0.0).astype(BF16)
        v_h = jnp.where(mine, vb.astype(F32), 0.0).astype(BF16)
        acc += mm((mm_nt(q_h, kb) * pair_weights(1 + h)).astype(BF16), v_h)
    loc_out[:, dv:] = acc


def retention_local(qa, ka, va, qb, kb, vb, dec, tab, base):
    n, dk = qa.shape
    dv, wb = va.shape[1], vb.shape[1]
    return pl.pallas_call(
        retention_body,
        out_shape=(
            jax.ShapeDtypeStruct((n, dk), BF16),
            jax.ShapeDtypeStruct((n, wb), BF16),
            jax.ShapeDtypeStruct((n, dv + wb), F32),
            jax.ShapeDtypeStruct((2, dk + 2 * TILE, dv), BF16),
        ),
        in_specs=vmem(9),
        out_specs=tuple(vmem(4)),
        interpret=INTERPRET,
        name="retention_local",
    )(qa, ka, va, qb, kb, vb, dec, tab, base)


def log_rows(ref, d, dk):
    rows = ref[d, dk + TILE : dk + 2 * TILE, :LANES].astype(F32)
    return [rows[2 * h : 2 * h + 1] + rows[2 * h + 1 : 2 * h + 2] for h in range(3)]


def pack_body(core_ref, own_ref, oth_ref, out_ref, ext_scr):
    chips = out_ref.shape[0]
    dv = own_ref.shape[2]
    dk = own_ref.shape[1] - 2 * TILE
    first = core_ref[0] == 0
    step = dk // chips
    blocks = dv // LANES // 2
    one = jnp.ones((1, LANES), F32)
    own_f, oth_f = log_rows(own_ref, 0, dk), log_rows(oth_ref, 0, dk)
    own_b, oth_b = log_rows(own_ref, 1, dk), log_rows(oth_ref, 1, dk)
    factor_own = [
        [jnp.where(first, jnp.exp(oth_f[h]), one) for h in range(3)],
        [jnp.where(first, one, jnp.exp(oth_b[h])) for h in range(3)],
    ]
    factor_oth = [
        [jnp.where(first, one, jnp.exp(own_f[h])) for h in range(3)],
        [jnp.where(first, jnp.exp(own_b[h]), one) for h in range(3)],
    ]
    lane = iota((1, LANES), 1)
    left = lane < LANES // 2
    for d in range(2):
        for q in range(blocks):
            a = slice(q * LANES, (q + 1) * LANES)
            b = slice((blocks + q) * LANES, (blocks + q + 1) * LANES)

            def mine(ref):
                return jnp.where(first, ref[d, :dk, a].astype(F32), ref[d, :dk, b].astype(F32))

            total = factor_own[d][0] * mine(own_ref) + factor_oth[d][0] * mine(oth_ref)
            at = (d * blocks + q) * step
            out_ref[:, at : at + step, :] = total.astype(BF16).reshape(chips, step, LANES)
    per = (dv // LANES) * TILE // chips
    for q in range(dv // LANES):
        part = []
        for d in range(2):
            fo = jnp.where(left, factor_own[d][1], factor_own[d][2])
            ft = jnp.where(left, factor_oth[d][1], factor_oth[d][2])
            cut = slice(q * LANES, (q + 1) * LANES)
            part.append(
                fo * own_ref[d, dk : dk + TILE, cut].astype(F32)
                + ft * oth_ref[d, dk : dk + TILE, cut].astype(F32)
            )
        part = jnp.where(first, part[0], part[1])
        for k in range(TILE // per):
            ext_scr[q * (TILE // per) + k, 0:per, :] = part[k * per : (k + 1) * per]
    rows = iota((TILE - per, LANES), 0)
    logs = jnp.zeros((TILE - per, LANES), F32)
    sums_f = [x + y for x, y in zip(own_f, oth_f)]
    sums_b = [x + y for x, y in zip(own_b, oth_b)]
    for k, value in enumerate(
        [
            sums_f[0],
            sums_b[0],
            jnp.where(left, sums_f[1], sums_f[2]),
            jnp.where(left, sums_b[1], sums_b[2]),
        ]
    ):
        hi, lo = split2(value)
        logs = jnp.where(rows == 2 * k, hi, jnp.where(rows == 2 * k + 1, lo, logs))
    ext_scr[:, per:, :] = jnp.broadcast_to(logs[None], (chips, TILE - per, LANES))
    at = 2 * blocks * step
    out_ref[:, at : at + TILE, :] = ext_scr[...].astype(BF16)


def pack_states(core, own, other, chips):
    dv = own.shape[2]
    dk = own.shape[1] - 2 * TILE
    rows = dv // LANES * (dk // chips) + TILE
    return pl.pallas_call(
        pack_body,
        out_shape=jax.ShapeDtypeStruct((chips, rows, LANES), BF16),
        in_specs=[SMEM_SPEC] + vmem(2),
        out_specs=vmem(1)[0],
        scratch_shapes=[pltpu.VMEM((chips, TILE, LANES), F32)],
        interpret=INTERPRET,
        name="pack_states",
    )(core, own, other)


def scan_body(per, core_ref, in_ref, out_ref):
    chips, rows, _ = in_ref.shape
    main = rows - TILE
    side = main // 2
    first = core_ref[0] == 0
    ext = [in_ref[i, main:, :].astype(F32) for i in range(chips)]
    decays = [
        [jnp.exp(e[per + 2 * k : per + 2 * k + 1] + e[per + 2 * k + 1 : per + 2 * k + 2]) for k in range(4)]
        for e in ext
    ]
    carry = jnp.zeros((side, LANES), F32)
    group = jnp.zeros((TILE, LANES), F32)
    into = []
    for i in range(chips):
        out_ref[i, :side, :] = carry.astype(BF16)
        into.append(group)
        carry = decays[i][0] * carry + in_ref[i, :side, :].astype(F32)
        group = decays[i][2] * group + ext[i]
    carry = jnp.zeros((side, LANES), F32)
    group = jnp.zeros((TILE, LANES), F32)
    for i in reversed(range(chips)):
        out_ref[i, side:main, :] = carry.astype(BF16)
        out_ref[i, main:, :] = jnp.where(first, into[i], group).astype(BF16)
        carry = decays[i][1] * carry + in_ref[i, side:main, :].astype(F32)
        group = decays[i][3] * group + ext[i]


def scan_states(core, pieces, per):
    def body(*refs):
        scan_body(per, *refs)

    return pl.pallas_call(
        body,
        out_shape=jax.ShapeDtypeStruct(pieces.shape, BF16),
        in_specs=[SMEM_SPEC] + vmem(1),
        out_specs=vmem(1)[0],
        interpret=INTERPRET,
        name="scan_states",
    )(core, pieces)


def mix_body(
    core_ref, qa_ref, qb_ref, loc_ref, own_ref, oth_ref, pay_ref, dec_ref, wa_ref, wb_ref,
    out_ref, grp_scr,
):
    n, dk = qa_ref.shape
    width = qb_ref.shape[1]
    hb = width // 2
    dv = loc_ref.shape[1] - width
    chips, rows, _ = own_ref.shape
    step = dk // chips
    blocks = dv // LANES // 2
    main = rows - TILE
    first = core_ref[0] == 0
    row, col = iota((n, n), 0), iota((n, n), 1)
    dec = dec_ref[...]
    cc = mm_nt((col <= row).astype(F32), dec, HIGHEST)
    rc = mm_nt((col >= row).astype(F32), dec, HIGHEST)
    col_f = [jnp.exp(cc[:, h : h + 1]) for h in range(3)]
    col_b = [jnp.exp(rc[:, 3 + h : 4 + h]) for h in range(3)]
    logs = [log_rows(pay_ref, d, dk) for d in range(2)]
    qa, qb = qa_ref[...], qb_ref[...]
    lane = iota((1, LANES), 1)
    left = lane < LANES // 2
    per = (dv // LANES) * TILE // chips
    total_a = loc_ref[:, :dv]
    total_b = loc_ref[:, dv:]
    for d in range(2):
        between = jnp.logical_not(first) if d == 0 else first
        factor = jnp.where(between, jnp.exp(logs[d][0]), jnp.ones((1, LANES), F32))
        keep = jnp.where(between, 1.0, 0.0)
        parts = []
        for b in range(2 * blocks):
            at = (d * blocks + b % blocks) * step
            own = own_ref[:, at : at + step, :].astype(F32)
            oth = oth_ref[:, at : at + step, :].astype(F32)
            use_own = first if b < blocks else jnp.logical_not(first)
            carry = jnp.where(use_own, own, oth).reshape(dk, LANES)
            near = pay_ref[d, :dk, b * LANES : (b + 1) * LANES].astype(F32)
            parts.append((factor * carry + keep * near).astype(BF16))
        state = jnp.concatenate(parts, axis=1)
        scale = col_f if d == 0 else col_b
        total_a = total_a + scale[0] * mm(qa, state)
        use_own = first if d == 0 else jnp.logical_not(first)
        ext = jnp.where(
            use_own, own_ref[:, main:, :].astype(F32), oth_ref[:, main:, :].astype(F32)
        )
        for i in range(chips):
            grp_scr[i * per : (i + 1) * per, :] = ext[i, 0:per, :]
        near = jnp.concatenate(
            [
                pay_ref[d, dk : dk + TILE, q * LANES : (q + 1) * LANES].astype(F32)
                for q in range(dv // LANES)
            ],
            axis=0,
        )
        factor = jnp.where(
            between,
            jnp.exp(jnp.where(left, logs[d][1], logs[d][2])),
            jnp.ones((1, LANES), F32),
        )
        group = factor * grp_scr[...] + keep * near
        blockdiag = jnp.concatenate(
            [jnp.where(left, group, 0.0), jnp.where(left, 0.0, group)], axis=0
        ).astype(BF16)
        total_b = total_b + jnp.where(left, scale[1], scale[2]) * mm(qb, blockdiag)
    square = jnp.mean(total_a * total_a, axis=1, keepdims=True)
    mixed_a = (total_a * lax.rsqrt(square + GROUP_EPS)).astype(BF16)
    sq = total_b * total_b
    s0 = jnp.sum(jnp.where(left, sq, 0.0), axis=1, keepdims=True) / hb
    s1 = jnp.sum(jnp.where(left, 0.0, sq), axis=1, keepdims=True) / hb
    mixed_b = (total_b * lax.rsqrt(jnp.where(left, s0, s1) + GROUP_EPS)).astype(BF16)
    out_ref[...] = (mm(mixed_a, wa_ref[...]) + mm(mixed_b, wb_ref[...])).astype(BF16)


def mix_project(core, qa, qb, loc, own, other, pay, dec, wa, wb):
    hb = qb.shape[1] // 2
    return pl.pallas_call(
        mix_body,
        out_shape=jax.ShapeDtypeStruct((qa.shape[0], wa.shape[1]), BF16),
        in_specs=[SMEM_SPEC] + vmem(9),
        out_specs=vmem(1)[0],
        scratch_shapes=[pltpu.VMEM((hb, qb.shape[1]), F32)],
        interpret=INTERPRET,
        name="mix_project",
    )(core, qa, qb, loc, own, other, pay, dec, wa, wb)


def layer_norm(stream, gain):
    center = stream - jnp.mean(stream, axis=-1, keepdims=True)
    spread = jnp.mean(center * center, axis=-1, keepdims=True)
    return center * lax.rsqrt(spread + NORM_EPS) * gain


def slots_by_route(ids):
    routes = ids.shape[1]
    row, col = iota((routes, routes), 0), iota((routes, routes), 1)
    ids_f = ids.astype(F32)
    ids_col = jnp.sum(jnp.where(row == col, ids_f, 0.0), axis=1, keepdims=True)
    same = (ids_col == ids_f) & (row < col)
    rank = jnp.sum(jnp.where(same, 1.0, 0.0), axis=0, keepdims=True)
    slot = ids_f * CAP + jnp.minimum(rank, CAP - 1.0)
    return jnp.where((row.astype(F32) == slot) & (rank < CAP), 1.0, 0.0)


def route_rows(rows, routes):
    return iota((rows, routes), 1) // TOP == iota((rows, routes), 0)


def dispatch_body(arr_ref, res_ref, gain_ref, ids_ref, hid_ref, out_ref):
    mix = jnp.sum(arr_ref[...].astype(F32), axis=0)
    stream = RESIDUAL_SCALE * res_ref[...].astype(F32) + mix
    hidden = layer_norm(stream, gain_ref[0:1, :]).astype(BF16)
    hid_ref[...] = hidden
    hot = slots_by_route(ids_ref[...])
    belongs = jnp.where(route_rows(hidden.shape[0], hot.shape[1]), 1.0, 0.0)
    choose = mm_nt(hot.astype(BF16), belongs.astype(BF16)).astype(BF16)
    out_ref[...] = mm(choose, hidden).astype(BF16)


def dispatch(arrived, residual, gain, ids):
    rows, width = residual.shape
    return pl.pallas_call(
        dispatch_body,
        out_shape=(
            jax.ShapeDtypeStruct((rows, width), BF16),
            jax.ShapeDtypeStruct((ids.shape[1], width), BF16),
        ),
        in_specs=vmem(4),
        out_specs=tuple(vmem(2)),
        interpret=INTERPRET,
        name="dispatch",
    )(arrived, residual, gain, ids)


def pack_weights_body(gate_ref, up_ref, down_ref, out_ref):
    width, units = gate_ref.shape[1:]
    pair = 2 * units
    out_ref[:width, :units] = gate_ref[0]
    out_ref[:width, units:] = up_ref[0]
    for k in range(width // pair):
        out_ref[width + k * units : width + (k + 1) * units, :] = down_ref[
            0, :, k * pair : (k + 1) * pair
        ]


def pack_weights(gate, up, down):
    _, width, units = gate.shape
    return pl.pallas_call(
        pack_weights_body,
        out_shape=jax.ShapeDtypeStruct((width + width // 2, 2 * units), BF16),
        in_specs=vmem(3),
        out_specs=vmem(1)[0],
        interpret=INTERPRET,
        name="pack_weights",
    )(gate, up, down)


def expert_body(x_ref, w_ref, out_ref, acc_ref):
    step = pl.program_id(0)
    sets, _, pair = w_ref.shape
    width = x_ref.shape[1]
    units = pair // 2

    @pl.when(step == 0)
    def _():
        acc_ref[...] = jnp.zeros_like(acc_ref)

    x = x_ref[...]
    hidden = []
    for s in range(sets):
        both = mm(x, w_ref[s, :width, :])
        gate, up = both[:, :units], both[:, units:]
        hidden.append((gate / (1.0 + jnp.exp(-gate)) * up).astype(BF16))
    hidden = jnp.concatenate(hidden, axis=1)
    for k in range(width // pair):
        at = width + k * units
        down = jnp.concatenate([w_ref[s, at : at + units, :] for s in range(sets)], axis=0)
        acc_ref[:, k * pair : (k + 1) * pair] += mm(hidden, down)

    @pl.when(step == pl.num_programs(0) - 1)
    def _():
        out_ref[...] = acc_ref[...].astype(BF16)


def experts(x, weights, sets=2):
    count, depth, pair = weights.shape
    rows, width = x.shape
    return pl.pallas_call(
        expert_body,
        grid=(count // sets,),
        out_shape=jax.ShapeDtypeStruct((rows, width), BF16),
        in_specs=[
            pl.BlockSpec((rows, width), lambda i: (0, 0)),
            pl.BlockSpec((sets, depth, pair), lambda i: (i, 0, 0)),
        ],
        out_specs=pl.BlockSpec((rows, width), lambda i: (0, 0)),
        scratch_shapes=[pltpu.VMEM((rows, width), F32)],
        interpret=INTERPRET,
        name="experts",
    )(x, weights)


def combine_body(ret_ref, hid_ref, gain_ref, ids_ref, w_ref, out_ref):
    hidden = hid_ref[...]
    hot = slots_by_route(ids_ref[...])
    factor = jnp.where(route_rows(hidden.shape[0], hot.shape[1]), w_ref[...], 0.0)
    weights = mm_nt(factor, hot, HIGHEST)
    returned = ret_ref[...]
    hi = weights.astype(BF16)
    rest = weights - hi.astype(F32)
    mid = rest.astype(BF16)
    low = (rest - mid.astype(F32)).astype(BF16)
    ffn = mm(hi, returned) + mm(mid, returned) + mm(low, returned)
    stream = RESIDUAL_SCALE * hidden.astype(F32) + ffn
    out_ref[...] = layer_norm(stream, gain_ref[1:2, :]).astype(BF16)


def combine(returned, hidden, gain, ids, weights):
    return pl.pallas_call(
        combine_body,
        out_shape=jax.ShapeDtypeStruct(hidden.shape, BF16),
        in_specs=vmem(5),
        out_specs=vmem(1)[0],
        interpret=INTERPRET,
        name="combine",
    )(returned, hidden, gain, ids, weights)


def exchange(array, axis):
    return lax.all_to_all(array, axis, split_axis=0, concat_axis=0, tiled=True)


def decay_rows(decay_a, decay_b):
    length = decay_a.shape[-1]
    return jnp.concatenate(
        [decay_a[0], decay_b[0], decay_a[1], decay_b[1], jnp.zeros((2, length), F32)], axis=0
    )


def shards(
    query_a, key_a, value_a, decay_a, query_b, key_b, value_b, decay_b, out_weight_a,
    out_weight_b, residual, norm_gain, route_group, route_expert, route_weight, expert_gate,
    expert_up, expert_down,
):
    length = query_a.shape[0]
    chips = lax.axis_size("sp_0")
    sp_count = lax.axis_size(SP)
    tp = lax.axis_size("tp")
    rows_dev, width = residual.shape
    routes = rows_dev * TOP
    weights_all = lax.all_gather(pack_weights(expert_gate, expert_up, expert_down), "tp")

    core = lax.axis_index("sp_1").astype(jnp.int32).reshape(1)
    local, base = angle_tables(
        length, query_a.shape[1] // 2, query_b.shape[1] // 4, sp_count
    )
    base = lax.dynamic_index_in_dim(jnp.asarray(base), lax.axis_index(SP), 0, keepdims=False)
    dec = decay_rows(decay_a, decay_b)
    qa, qb, loc, pay = retention_local(
        query_a, key_a, value_a, query_b, key_b, value_b, dec, jnp.asarray(local), base
    )
    swap = [(0, 1), (1, 0)]
    pay_other = lax.ppermute(pay, "sp_1", swap)
    pieces = exchange(pack_states(core, pay, pay_other, chips), "sp_0")
    per = value_a.shape[1] // LANES * TILE // chips
    carried = exchange(scan_states(core, pieces, per), "sp_0")
    carried_other = lax.ppermute(carried, "sp_1", swap)
    partial = mix_project(
        core, qa, qb, loc, carried, carried_other, pay_other, dec, out_weight_a, out_weight_b
    )
    arrived = exchange(partial.reshape(tp, rows_dev, width), "tp")
    ids = (route_group[:, None] * EXP_GROUP + route_expert).reshape(1, routes)
    hidden, outgoing = dispatch(arrived, residual, norm_gain, ids)
    slots = outgoing.shape[0]
    received = exchange(outgoing.reshape(sp_count, slots // sp_count, width), SP)
    back = experts(received.reshape(slots, width), weights_all)
    returned = exchange(back.reshape(sp_count, slots // sp_count, width), SP)
    return combine(
        returned.reshape(slots, width), hidden, norm_gain, ids, route_weight.reshape(1, routes)
    )


def solution(mesh):
    sp = mesh.shape["sp"]
    finer = Mesh(
        mesh.devices.reshape(mesh.shape["grp"], sp // 2, 2, mesh.shape["tp"]),
        ("grp", "sp_0", "sp_1", "tp"),
    )
    in_specs = (
        P(GRP_SP, "tp"),
        P(GRP_SP, "tp"),
        P(GRP_SP, "tp"),
        P(None, "tp", GRP_SP),
        P(GRP_SP, "tp"),
        P(GRP_SP, "tp"),
        P(GRP_SP, "tp"),
        P(None, "tp", GRP_SP),
        P("tp", None),
        P("tp", None),
        P(GRP_SP_TP, None),
        P(),
        P(GRP_SP_TP),
        P(GRP_SP_TP, None),
        P(GRP_SP_TP, None),
        P(SP, None, "tp"),
        P(SP, None, "tp"),
        P(SP, "tp", None),
    )
    out_specs = P(GRP_SP_TP, None)
    return jax.shard_map(
        shards, mesh=finer, in_specs=in_specs, out_specs=out_specs, check_vma=False
    )
```

```python
import math

import jax
import jax.numpy as jnp
import numpy as np
from jax import lax
from jax.experimental import pallas as pl
from jax.experimental.pallas import tpu as pltpu
from jax.sharding import Mesh
from jax.sharding import PartitionSpec as P

CAP = 2
TOP = 2
EXP_GROUP = 8
SP = ("sp_0", "sp_1")
GRP_SP = ("grp", "sp_0", "sp_1")
GRP_SP_TP = ("grp", "sp_0", "sp_1", "tp")

RESIDUAL_SCALE = math.sqrt(2.0)
NORM_EPS = 1e-05
GROUP_EPS = 1e-06
ROPE_BASE = 10000.0

F32 = jnp.float32
BF16 = jnp.bfloat16
HIGHEST = lax.Precision.HIGHEST
INTERPRET = False

LANES = 128
TILE = 16


def vmem(count):
    return [pl.BlockSpec(memory_space=pltpu.VMEM)] * count


SMEM_SPEC = pl.BlockSpec(memory_space=pltpu.SMEM)
ANY_SPEC = pl.BlockSpec(memory_space=pl.ANY)


def iota(shape, dim):
    return lax.broadcasted_iota(jnp.int32, shape, dim)


def mm(a, b):
    return jnp.dot(a, b, preferred_element_type=F32)


def mm_nt(a, b, precision=None):
    return lax.dot_general(
        a, b, (((1,), (1,)), ((), ())), precision=precision, preferred_element_type=F32
    )


def split2(x):
    hi = x.astype(BF16).astype(F32)
    return hi, x - hi


def angle_tables(length, half_a, half_b, devices):
    def freqs(half):
        f = np.float32(ROPE_BASE) ** (-np.arange(half, dtype=np.float32) / np.float32(half))
        return f.astype(np.float64)

    fa = freqs(half_a)
    fb = np.tile(freqs(half_b), LANES // half_b)
    inside = np.arange(length, dtype=np.float64)[:, None]
    first = (np.arange(devices, dtype=np.float64) * length)[:, None]
    local = np.stack(
        [np.cos(inside * fa), np.sin(inside * fa), np.cos(inside * fb), np.sin(inside * fb)]
    ).astype(np.float32)
    base = np.zeros((devices, 8, LANES), np.float32)
    for k, row in enumerate(
        [np.cos(first * fa), np.sin(first * fa), np.cos(first * fb), np.sin(first * fb)]
    ):
        base[:, k, :] = row
    return local, base


def retention_body(
    qa_ref, ka_ref, va_ref, qb_ref, kb_ref, vb_ref, dec_ref, tab_ref, base_ref,
    qa_out, qb_out, loc_out, pay_out,
):
    n, dk = qa_ref.shape
    dv = va_ref.shape[1]
    half = dk // 2
    hb = qb_ref.shape[1] // 2
    hq = hb // 2
    row, col = iota((n, n), 0), iota((n, n), 1)
    dec = dec_ref[...]
    cr = jnp.dot(dec, (row <= col).astype(F32), precision=HIGHEST, preferred_element_type=F32)
    cc = mm_nt((col <= row).astype(F32), dec, HIGHEST)
    er = cr - dec
    ec = mm_nt((col < row).astype(F32), dec, HIGHEST)
    tot = cr[:, n - 1 : n]

    def pair_weights(h):
        forward = cc[:, h : h + 1] - cr[h : h + 1, :]
        backward = er[3 + h : 4 + h, :] - ec[:, 3 + h : 4 + h]
        return jnp.exp(jnp.where(col <= row, forward, backward))

    base = base_ref[...]
    cos_a = tab_ref[0] * base[0:1] - tab_ref[1] * base[1:2]
    sin_a = tab_ref[1] * base[0:1] + tab_ref[0] * base[1:2]

    def rotate_a(x, scale):
        x1, x2 = x[:, :half].astype(F32), x[:, half:].astype(F32)
        out = jnp.concatenate([x1 * cos_a - x2 * sin_a, x1 * sin_a + x2 * cos_a], axis=1)
        return (out * scale).astype(BF16)

    qa = rotate_a(qa_ref[...], 1.0)
    ka = rotate_a(ka_ref[...], 1.0 / math.sqrt(dk))
    qa_out[...] = qa

    width = 2 * hb
    lane = iota((n, width), 1)
    cos_b = tab_ref[2] * base[2:3] - tab_ref[3] * base[3:4]
    sin_b = tab_ref[3] * base[2:3] + tab_ref[2] * base[3:4]
    low = (lane % hb) < hq
    sin_b = jnp.where(low, -sin_b, sin_b)
    pr, pc = iota((width, width), 0), iota((width, width), 1)
    partner = jnp.where((pc % hb) < hq, pc + hq, pc - hq)
    swap = (pr == partner).astype(BF16)

    def rotate_b(x, scale):
        return ((x.astype(F32) * cos_b + mm(x, swap) * sin_b) * scale).astype(BF16)

    qb = rotate_b(qb_ref[...], 1.0)
    kb = rotate_b(kb_ref[...], 1.0 / math.sqrt(hb))
    qb_out[...] = qb

    va, vb = va_ref[...], vb_ref[...]
    kat = ka.astype(F32).T
    kbt = kb.astype(F32).T
    top = iota((width, n), 0) < hb
    for d in range(2):
        if d == 0:
            scale = [jnp.exp(tot[h : h + 1] - cr[h : h + 1, :]) for h in range(3)]
        else:
            scale = [jnp.exp(er[3 + h : 4 + h, :]) for h in range(3)]
        state = mm((kat * scale[0]).astype(BF16), va)
        pay_out[d, :dk, :] = state.astype(BF16)
        both = mm((kbt * jnp.where(top, scale[1], scale[2])).astype(BF16), vb)
        packed = jnp.where(iota((hb, width), 1) < hb, both[:hb], both[hb:]).astype(BF16)
        for q in range(dv // LANES):
            pay_out[d, dk : dk + TILE, q * LANES : (q + 1) * LANES] = packed[
                q * TILE : (q + 1) * TILE
            ]
        rows = iota((TILE, dv), 0)
        logs = jnp.zeros((TILE, dv), F32)
        for h in range(3):
            hi, lo = split2(tot[3 * d + h : 3 * d + h + 1])
            logs = jnp.where(rows == 2 * h, hi, jnp.where(rows == 2 * h + 1, lo, logs))
        pay_out[d, dk + TILE : dk + 2 * TILE, :] = logs.astype(BF16)
    weighted = (mm_nt(qa, ka) * pair_weights(0)).astype(BF16)
    loc_out[:, :dv] = mm(weighted, va)
    acc = jnp.zeros((n, width), F32)
    for h in range(2):
        mine = (lane < hb) if h == 0 else (lane >= hb)
        q_h = jnp.where(mine, qb.astype(F32), 0.0).astype(BF16)
        v_h = jnp.where(mine, vb.astype(F32), 0.0).astype(BF16)
        acc += mm((mm_nt(q_h, kb) * pair_weights(1 + h)).astype(BF16), v_h)
    loc_out[:, dv:] = acc


def retention_local(qa, ka, va, qb, kb, vb, dec, tab, base):
    n, dk = qa.shape
    dv, wb = va.shape[1], vb.shape[1]
    return pl.pallas_call(
        retention_body,
        out_shape=(
            jax.ShapeDtypeStruct((n, dk), BF16),
            jax.ShapeDtypeStruct((n, wb), BF16),
            jax.ShapeDtypeStruct((n, dv + wb), F32),
            jax.ShapeDtypeStruct((2, dk + 2 * TILE, dv), BF16),
        ),
        in_specs=vmem(9),
        out_specs=tuple(vmem(4)),
        interpret=INTERPRET,
        name="retention_local",
    )(qa, ka, va, qb, kb, vb, dec, tab, base)


def log_rows(ref, d, dk):
    rows = ref[d, dk + TILE : dk + 2 * TILE, :LANES].astype(F32)
    return [rows[2 * h : 2 * h + 1] + rows[2 * h + 1 : 2 * h + 2] for h in range(3)]


def pack_body(core_ref, own_ref, oth_ref, out_ref, ext_scr):
    chips = out_ref.shape[0]
    dv = own_ref.shape[2]
    dk = own_ref.shape[1] - 2 * TILE
    first = core_ref[0] == 0
    step = dk // chips
    blocks = dv // LANES // 2
    one = jnp.ones((1, LANES), F32)
    own_f, oth_f = log_rows(own_ref, 0, dk), log_rows(oth_ref, 0, dk)
    own_b, oth_b = log_rows(own_ref, 1, dk), log_rows(oth_ref, 1, dk)
    factor_own = [
        [jnp.where(first, jnp.exp(oth_f[h]), one) for h in range(3)],
        [jnp.where(first, one, jnp.exp(oth_b[h])) for h in range(3)],
    ]
    factor_oth = [
        [jnp.where(first, one, jnp.exp(own_f[h])) for h in range(3)],
        [jnp.where(first, jnp.exp(own_b[h]), one) for h in range(3)],
    ]
    lane = iota((1, LANES), 1)
    left = lane < LANES // 2
    for d in range(2):
        for q in range(blocks):
            a = slice(q * LANES, (q + 1) * LANES)
            b = slice((blocks + q) * LANES, (blocks + q + 1) * LANES)

            def mine(ref):
                return jnp.where(first, ref[d, :dk, a].astype(F32), ref[d, :dk, b].astype(F32))

            total = factor_own[d][0] * mine(own_ref) + factor_oth[d][0] * mine(oth_ref)
            at = (d * blocks + q) * step
            out_ref[:, at : at + step, :] = total.astype(BF16).reshape(chips, step, LANES)
    per = (dv // LANES) * TILE // chips
    for q in range(dv // LANES):
        part = []
        for d in range(2):
            fo = jnp.where(left, factor_own[d][1], factor_own[d][2])
            ft = jnp.where(left, factor_oth[d][1], factor_oth[d][2])
            cut = slice(q * LANES, (q + 1) * LANES)
            part.append(
                fo * own_ref[d, dk : dk + TILE, cut].astype(F32)
                + ft * oth_ref[d, dk : dk + TILE, cut].astype(F32)
            )
        part = jnp.where(first, part[0], part[1])
        for k in range(TILE // per):
            ext_scr[q * (TILE // per) + k, 0:per, :] = part[k * per : (k + 1) * per]
    rows = iota((TILE - per, LANES), 0)
    logs = jnp.zeros((TILE - per, LANES), F32)
    sums_f = [x + y for x, y in zip(own_f, oth_f)]
    sums_b = [x + y for x, y in zip(own_b, oth_b)]
    for k, value in enumerate(
        [
            sums_f[0],
            sums_b[0],
            jnp.where(left, sums_f[1], sums_f[2]),
            jnp.where(left, sums_b[1], sums_b[2]),
        ]
    ):
        hi, lo = split2(value)
        logs = jnp.where(rows == 2 * k, hi, jnp.where(rows == 2 * k + 1, lo, logs))
    ext_scr[:, per:, :] = jnp.broadcast_to(logs[None], (chips, TILE - per, LANES))
    at = 2 * blocks * step
    out_ref[:, at : at + TILE, :] = ext_scr[...].astype(BF16)


def pack_states(core, own, other, chips):
    dv = own.shape[2]
    dk = own.shape[1] - 2 * TILE
    rows = dv // LANES * (dk // chips) + TILE
    return pl.pallas_call(
        pack_body,
        out_shape=jax.ShapeDtypeStruct((chips, rows, LANES), BF16),
        in_specs=[SMEM_SPEC] + vmem(2),
        out_specs=vmem(1)[0],
        scratch_shapes=[pltpu.VMEM((chips, TILE, LANES), F32)],
        interpret=INTERPRET,
        name="pack_states",
    )(core, own, other)


def scan_body(per, core_ref, in_ref, out_ref):
    chips, rows, _ = in_ref.shape
    main = rows - TILE
    side = main // 2
    first = core_ref[0] == 0
    ext = [in_ref[i, main:, :].astype(F32) for i in range(chips)]
    decays = [
        [jnp.exp(e[per + 2 * k : per + 2 * k + 1] + e[per + 2 * k + 1 : per + 2 * k + 2]) for k in range(4)]
        for e in ext
    ]
    carry = jnp.zeros((side, LANES), F32)
    group = jnp.zeros((TILE, LANES), F32)
    into = []
    for i in range(chips):
        out_ref[i, :side, :] = carry.astype(BF16)
        into.append(group)
        carry = decays[i][0] * carry + in_ref[i, :side, :].astype(F32)
        group = decays[i][2] * group + ext[i]
    carry = jnp.zeros((side, LANES), F32)
    group = jnp.zeros((TILE, LANES), F32)
    for i in reversed(range(chips)):
        out_ref[i, side:main, :] = carry.astype(BF16)
        out_ref[i, main:, :] = jnp.where(first, into[i], group).astype(BF16)
        carry = decays[i][1] * carry + in_ref[i, side:main, :].astype(F32)
        group = decays[i][3] * group + ext[i]


def passed_through(arrays, inputs, outputs):
    shapes = tuple(jax.ShapeDtypeStruct(x.shape, x.dtype) for x in arrays)
    return shapes, [ANY_SPEC] * len(arrays), {inputs + k: outputs + k for k in range(len(arrays))}


def scan_states(core, pieces, per, held):
    def body(core_ref, in_ref, *refs):
        scan_body(per, core_ref, in_ref, refs[len(held)])

    shapes, specs, aliases = passed_through(held, 2, 1)
    out = pl.pallas_call(
        body,
        out_shape=(jax.ShapeDtypeStruct(pieces.shape, BF16),) + shapes,
        in_specs=[SMEM_SPEC] + vmem(1) + specs,
        out_specs=tuple(vmem(1) + specs),
        input_output_aliases=aliases,
        interpret=INTERPRET,
        name="scan_states",
    )(core, pieces, *held)
    return out[0], out[1:]


def mix_body(
    core_ref, qa_ref, qb_ref, loc_ref, own_ref, oth_ref, pay_ref, dec_ref, wa_ref, wb_ref,
    out_ref, grp_scr,
):
    n, dk = qa_ref.shape
    width = qb_ref.shape[1]
    hb = width // 2
    dv = loc_ref.shape[1] - width
    chips, rows, _ = own_ref.shape
    step = dk // chips
    blocks = dv // LANES // 2
    main = rows - TILE
    first = core_ref[0] == 0
    row, col = iota((n, n), 0), iota((n, n), 1)
    dec = dec_ref[...]
    cc = mm_nt((col <= row).astype(F32), dec, HIGHEST)
    rc = mm_nt((col >= row).astype(F32), dec, HIGHEST)
    col_f = [jnp.exp(cc[:, h : h + 1]) for h in range(3)]
    col_b = [jnp.exp(rc[:, 3 + h : 4 + h]) for h in range(3)]
    logs = [log_rows(pay_ref, d, dk) for d in range(2)]
    qa, qb = qa_ref[...], qb_ref[...]
    lane = iota((1, LANES), 1)
    left = lane < LANES // 2
    per = (dv // LANES) * TILE // chips
    total_a = loc_ref[:, :dv]
    total_b = loc_ref[:, dv:]
    for d in range(2):
        between = jnp.logical_not(first) if d == 0 else first
        factor = jnp.where(between, jnp.exp(logs[d][0]), jnp.ones((1, LANES), F32))
        keep = jnp.where(between, 1.0, 0.0)
        parts = []
        for b in range(2 * blocks):
            at = (d * blocks + b % blocks) * step
            own = own_ref[:, at : at + step, :].astype(F32)
            oth = oth_ref[:, at : at + step, :].astype(F32)
            use_own = first if b < blocks else jnp.logical_not(first)
            carry = jnp.where(use_own, own, oth).reshape(dk, LANES)
            near = pay_ref[d, :dk, b * LANES : (b + 1) * LANES].astype(F32)
            parts.append((factor * carry + keep * near).astype(BF16))
        state = jnp.concatenate(parts, axis=1)
        scale = col_f if d == 0 else col_b
        total_a = total_a + scale[0] * mm(qa, state)
        use_own = first if d == 0 else jnp.logical_not(first)
        ext = jnp.where(
            use_own, own_ref[:, main:, :].astype(F32), oth_ref[:, main:, :].astype(F32)
        )
        for i in range(chips):
            grp_scr[i * per : (i + 1) * per, :] = ext[i, 0:per, :]
        near = jnp.concatenate(
            [
                pay_ref[d, dk : dk + TILE, q * LANES : (q + 1) * LANES].astype(F32)
                for q in range(dv // LANES)
            ],
            axis=0,
        )
        factor = jnp.where(
            between,
            jnp.exp(jnp.where(left, logs[d][1], logs[d][2])),
            jnp.ones((1, LANES), F32),
        )
        group = factor * grp_scr[...] + keep * near
        blockdiag = jnp.concatenate(
            [jnp.where(left, group, 0.0), jnp.where(left, 0.0, group)], axis=0
        ).astype(BF16)
        total_b = total_b + jnp.where(left, scale[1], scale[2]) * mm(qb, blockdiag)
    square = jnp.mean(total_a * total_a, axis=1, keepdims=True)
    mixed_a = (total_a * lax.rsqrt(square + GROUP_EPS)).astype(BF16)
    sq = total_b * total_b
    s0 = jnp.sum(jnp.where(left, sq, 0.0), axis=1, keepdims=True) / hb
    s1 = jnp.sum(jnp.where(left, 0.0, sq), axis=1, keepdims=True) / hb
    mixed_b = (total_b * lax.rsqrt(jnp.where(left, s0, s1) + GROUP_EPS)).astype(BF16)
    out_ref[...] = (mm(mixed_a, wa_ref[...]) + mm(mixed_b, wb_ref[...])).astype(BF16)


def mix_project(core, qa, qb, loc, own, other, pay, dec, wa, wb, held):
    hb = qb.shape[1] // 2

    def body(*refs):
        mix_body(*refs[:10], refs[10 + len(held)], refs[-1])

    shapes, specs, aliases = passed_through(held, 10, 1)
    out = pl.pallas_call(
        body,
        out_shape=(jax.ShapeDtypeStruct((qa.shape[0], wa.shape[1]), BF16),) + shapes,
        in_specs=[SMEM_SPEC] + vmem(9) + specs,
        out_specs=tuple(vmem(1) + specs),
        scratch_shapes=[pltpu.VMEM((hb, qb.shape[1]), F32)],
        input_output_aliases=aliases,
        interpret=INTERPRET,
        name="mix_project",
    )(core, qa, qb, loc, own, other, pay, dec, wa, wb, *held)
    return out[0], out[1:]


def layer_norm(stream, gain):
    center = stream - jnp.mean(stream, axis=-1, keepdims=True)
    spread = jnp.mean(center * center, axis=-1, keepdims=True)
    return center * lax.rsqrt(spread + NORM_EPS) * gain


def slots_by_route(ids):
    routes = ids.shape[1]
    row, col = iota((routes, routes), 0), iota((routes, routes), 1)
    ids_f = ids.astype(F32)
    ids_col = jnp.sum(jnp.where(row == col, ids_f, 0.0), axis=1, keepdims=True)
    same = (ids_col == ids_f) & (row < col)
    rank = jnp.sum(jnp.where(same, 1.0, 0.0), axis=0, keepdims=True)
    slot = ids_f * CAP + jnp.minimum(rank, CAP - 1.0)
    return jnp.where((row.astype(F32) == slot) & (rank < CAP), 1.0, 0.0)


def route_rows(rows, routes):
    return iota((rows, routes), 1) // TOP == iota((rows, routes), 0)


def dispatch_body(
    arr_ref, res_ref, gain_ref, ids_ref, up_ref, down_ref,
    hid_ref, out_ref, up_half, down_half, up_out, down_out, sems,
):
    half = up_half.shape[0]
    copies = [
        pltpu.make_async_copy(up_ref.at[pl.ds(0, half), :], up_half, sems.at[0]),
        pltpu.make_async_copy(down_ref.at[pl.ds(half, half), :], down_half, sems.at[1]),
    ]
    for copy in copies:
        copy.start()
    mix = jnp.sum(arr_ref[...].astype(F32), axis=0)
    stream = RESIDUAL_SCALE * res_ref[...].astype(F32) + mix
    hidden = layer_norm(stream, gain_ref[0:1, :]).astype(BF16)
    hid_ref[...] = hidden
    hot = slots_by_route(ids_ref[...])
    belongs = jnp.where(route_rows(hidden.shape[0], hot.shape[1]), 1.0, 0.0)
    choose = mm_nt(hot.astype(BF16), belongs.astype(BF16)).astype(BF16)
    out_ref[...] = mm(choose, hidden).astype(BF16)
    for copy in copies:
        copy.wait()


def dispatch(arrived, residual, gain, ids, held):
    rows, width = residual.shape
    depth, pair = held[0].shape
    shapes, specs, aliases = passed_through(held, 4, 4)
    half = jax.ShapeDtypeStruct((depth // 2, pair), BF16)
    return pl.pallas_call(
        dispatch_body,
        out_shape=(
            jax.ShapeDtypeStruct((rows, width), BF16),
            jax.ShapeDtypeStruct((ids.shape[1], width), BF16),
            half,
            half,
        ) + shapes,
        in_specs=vmem(4) + specs,
        out_specs=tuple(vmem(2) + [ANY_SPEC] * 2 + specs),
        scratch_shapes=[pltpu.SemaphoreType.DMA((2,))],
        input_output_aliases=aliases,
        interpret=INTERPRET,
        name="dispatch",
    )(arrived, residual, gain, ids, *held)


def pack_weights_body(gate_ref, up_ref, down_ref, out_ref):
    width, units = gate_ref.shape[1:]
    pair = 2 * units
    out_ref[:width, :units] = gate_ref[0]
    out_ref[:width, units:] = up_ref[0]
    for k in range(width // pair):
        out_ref[width + k * units : width + (k + 1) * units, :] = down_ref[
            0, :, k * pair : (k + 1) * pair
        ]


def pack_weights(gate, up, down):
    _, width, units = gate.shape
    return pl.pallas_call(
        pack_weights_body,
        out_shape=jax.ShapeDtypeStruct((width + width // 2, 2 * units), BF16),
        in_specs=vmem(3),
        out_specs=vmem(1)[0],
        interpret=INTERPRET,
        name="pack_weights",
    )(gate, up, down)


def expert_body(x_ref, *refs):
    *blocks, top_ref, bottom_ref, out_ref, w_scr, acc_ref, sems = refs
    count, depth, pair = w_scr.shape
    width = x_ref.shape[1]
    units = pair // 2
    half = depth // 2
    copies = [
        [pltpu.make_async_copy(ref, w_scr.at[k], sems.at[k])] for k, ref in enumerate(blocks)
    ]
    copies.append(
        [
            pltpu.make_async_copy(top_ref, w_scr.at[count - 1, pl.ds(0, half), :], sems.at[count - 1]),
            pltpu.make_async_copy(bottom_ref, w_scr.at[count - 1, pl.ds(half, half), :], sems.at[count]),
        ]
    )
    for group in copies:
        for copy in group:
            copy.start()
    x = x_ref[...]
    for first in range(0, count, 2):
        hidden = []
        for k in (first, first + 1):
            for copy in copies[k]:
                copy.wait()
            both = mm(x, w_scr[k, :width, :])
            gate, up = both[:, :units], both[:, units:]
            hidden.append((gate / (1.0 + jnp.exp(-gate)) * up).astype(BF16))
        hidden = jnp.concatenate(hidden, axis=1)
        for c in range(width // pair):
            at = width + c * units
            cut = slice(c * pair, (c + 1) * pair)
            down = jnp.concatenate(
                [w_scr[k, at : at + units, :] for k in (first, first + 1)], axis=0
            )
            part = mm(hidden, down)
            if first == 0:
                acc_ref[:, cut] = part
            elif first < count - 2:
                acc_ref[:, cut] += part
            else:
                out_ref[:, cut] = (acc_ref[:, cut] + part).astype(BF16)


def experts(x, blocks):
    depth, pair = blocks[0].shape
    count = len(blocks) - 1
    rows, width = x.shape
    return pl.pallas_call(
        expert_body,
        out_shape=jax.ShapeDtypeStruct((rows, width), BF16),
        in_specs=vmem(1) + [ANY_SPEC] * len(blocks),
        out_specs=vmem(1)[0],
        scratch_shapes=[
            pltpu.VMEM((count, depth, pair), BF16),
            pltpu.VMEM((rows, width), F32),
            pltpu.SemaphoreType.DMA((count + 1,)),
        ],
        interpret=INTERPRET,
        name="experts",
    )(x, *blocks)


def combine_body(ret_ref, hid_ref, gain_ref, ids_ref, w_ref, out_ref):
    hidden = hid_ref[...]
    hot = slots_by_route(ids_ref[...])
    factor = jnp.where(route_rows(hidden.shape[0], hot.shape[1]), w_ref[...], 0.0)
    weights = mm_nt(factor, hot, HIGHEST)
    returned = ret_ref[...]
    hi = weights.astype(BF16)
    rest = weights - hi.astype(F32)
    mid = rest.astype(BF16)
    low = (rest - mid.astype(F32)).astype(BF16)
    ffn = mm(hi, returned) + mm(mid, returned) + mm(low, returned)
    stream = RESIDUAL_SCALE * hidden.astype(F32) + ffn
    out_ref[...] = layer_norm(stream, gain_ref[1:2, :]).astype(BF16)


def combine(returned, hidden, gain, ids, weights):
    return pl.pallas_call(
        combine_body,
        out_shape=jax.ShapeDtypeStruct(hidden.shape, BF16),
        in_specs=vmem(5),
        out_specs=vmem(1)[0],
        interpret=INTERPRET,
        name="combine",
    )(returned, hidden, gain, ids, weights)


def exchange(array, axis):
    return lax.all_to_all(array, axis, split_axis=0, concat_axis=0, tiled=True)


def decay_rows(decay_a, decay_b):
    length = decay_a.shape[-1]
    return jnp.concatenate(
        [decay_a[0], decay_b[0], decay_a[1], decay_b[1], jnp.zeros((2, length), F32)], axis=0
    )


def shards(
    query_a, key_a, value_a, decay_a, query_b, key_b, value_b, decay_b, out_weight_a,
    out_weight_b, residual, norm_gain, route_group, route_expert, route_weight, expert_gate,
    expert_up, expert_down,
):
    length = query_a.shape[0]
    chips = lax.axis_size("sp_0")
    sp_count = lax.axis_size(SP)
    tp = lax.axis_size("tp")
    rows_dev, width = residual.shape
    routes = rows_dev * TOP
    blocks = [pack_weights(expert_gate, expert_up, expert_down)]
    up_ring = [(k, (k + 1) % tp) for k in range(tp)]
    down_ring = [(k, (k - 1) % tp) for k in range(tp)]

    def passed_on(going_up, going_down):
        return (
            lax.ppermute(going_up, "tp", up_ring),
            lax.ppermute(going_down, "tp", down_ring),
        )

    held = passed_on(blocks[0], blocks[0])

    core = lax.axis_index("sp_1").astype(jnp.int32).reshape(1)
    local, base = angle_tables(
        length, query_a.shape[1] // 2, query_b.shape[1] // 4, sp_count
    )
    base = lax.dynamic_index_in_dim(jnp.asarray(base), lax.axis_index(SP), 0, keepdims=False)
    dec = decay_rows(decay_a, decay_b)
    qa, qb, loc, pay = retention_local(
        query_a, key_a, value_a, query_b, key_b, value_b, dec, jnp.asarray(local), base
    )
    swap = [(0, 1), (1, 0)]
    pay_other = lax.ppermute(pay, "sp_1", swap)
    pieces = exchange(pack_states(core, pay, pay_other, chips), "sp_0")
    per = value_a.shape[1] // LANES * TILE // chips
    scanned, held = scan_states(core, pieces, per, held)
    blocks += held
    held = passed_on(*held)
    carried = exchange(scanned, "sp_0")
    carried_other = lax.ppermute(carried, "sp_1", swap)
    partial, held = mix_project(
        core, qa, qb, loc, carried, carried_other, pay_other, dec, out_weight_a, out_weight_b, held
    )
    blocks += held
    held = passed_on(*held)
    arrived = exchange(partial.reshape(tp, rows_dev, width), "tp")
    ids = (route_group[:, None] * EXP_GROUP + route_expert).reshape(1, routes)
    hidden, outgoing, up_half, down_half, *held = dispatch(
        arrived, residual, norm_gain, ids, held
    )
    blocks += held
    blocks += passed_on(up_half, down_half)
    slots = outgoing.shape[0]
    received = exchange(outgoing.reshape(sp_count, slots // sp_count, width), SP)
    back = experts(received.reshape(slots, width), blocks)
    returned = exchange(back.reshape(sp_count, slots // sp_count, width), SP)
    return combine(
        returned.reshape(slots, width), hidden, norm_gain, ids, route_weight.reshape(1, routes)
    )


def solution(mesh):
    sp = mesh.shape["sp"]
    finer = Mesh(
        mesh.devices.reshape(mesh.shape["grp"], sp // 2, 2, mesh.shape["tp"]),
        ("grp", "sp_0", "sp_1", "tp"),
    )
    in_specs = (
        P(GRP_SP, "tp"),
        P(GRP_SP, "tp"),
        P(GRP_SP, "tp"),
        P(None, "tp", GRP_SP),
        P(GRP_SP, "tp"),
        P(GRP_SP, "tp"),
        P(GRP_SP, "tp"),
        P(None, "tp", GRP_SP),
        P("tp", None),
        P("tp", None),
        P(GRP_SP_TP, None),
        P(),
        P(GRP_SP_TP),
        P(GRP_SP_TP, None),
        P(GRP_SP_TP, None),
        P(SP, None, "tp"),
        P(SP, None, "tp"),
        P(SP, "tp", None),
    )
    out_specs = P(GRP_SP_TP, None)
    return jax.shard_map(
        shards, mesh=finer, in_specs=in_specs, out_specs=out_specs, check_vma=False
    )
```

```python
import math

import jax
import jax.numpy as jnp
import numpy as np
from jax import lax
from jax.experimental import pallas as pl
from jax.experimental.pallas import tpu as pltpu
from jax.sharding import Mesh
from jax.sharding import PartitionSpec as P

CAP = 2
TOP = 2
EXP_GROUP = 8
SP = ("sp_0", "sp_1")
GRP_SP = ("grp", "sp_0", "sp_1")
GRP_SP_TP = ("grp", "sp_0", "sp_1", "tp")

RESIDUAL_SCALE = math.sqrt(2.0)
NORM_EPS = 1e-05
GROUP_EPS = 1e-06
ROPE_BASE = 10000.0

F32 = jnp.float32
BF16 = jnp.bfloat16
HIGHEST = lax.Precision.HIGHEST
INTERPRET = False

LANES = 128
TILE = 16


def vmem(count):
    return [pl.BlockSpec(memory_space=pltpu.VMEM)] * count


SMEM_SPEC = pl.BlockSpec(memory_space=pltpu.SMEM)
ANY_SPEC = pl.BlockSpec(memory_space=pl.ANY)


def iota(shape, dim):
    return lax.broadcasted_iota(jnp.int32, shape, dim)


def mm(a, b):
    return jnp.dot(a, b, preferred_element_type=F32)


def mm_nt(a, b, precision=None):
    return lax.dot_general(
        a, b, (((1,), (1,)), ((), ())), precision=precision, preferred_element_type=F32
    )


def split2(x):
    hi = x.astype(BF16).astype(F32)
    return hi, x - hi


def angle_tables(length, half_a, half_b, devices):
    def freqs(half):
        f = np.float32(ROPE_BASE) ** (-np.arange(half, dtype=np.float32) / np.float32(half))
        return f.astype(np.float64)

    fa = freqs(half_a)
    fb = np.tile(freqs(half_b), LANES // half_b)
    inside = np.arange(length, dtype=np.float64)[:, None]
    first = (np.arange(devices, dtype=np.float64) * length)[:, None]
    local = np.stack(
        [np.cos(inside * fa), np.sin(inside * fa), np.cos(inside * fb), np.sin(inside * fb)]
    ).astype(np.float32)
    base = np.zeros((devices, 8, LANES), np.float32)
    for k, row in enumerate(
        [np.cos(first * fa), np.sin(first * fa), np.cos(first * fb), np.sin(first * fb)]
    ):
        base[:, k, :] = row
    return local, base


def retention_body(
    qa_ref, ka_ref, va_ref, qb_ref, kb_ref, vb_ref, dec_ref, tab_ref, base_ref,
    qa_out, qb_out, loc_out, pay_out,
):
    n, dk = qa_ref.shape
    dv = va_ref.shape[1]
    half = dk // 2
    hb = qb_ref.shape[1] // 2
    hq = hb // 2
    row, col = iota((n, n), 0), iota((n, n), 1)
    dec = dec_ref[...]
    cr = jnp.dot(dec, (row <= col).astype(F32), precision=HIGHEST, preferred_element_type=F32)
    cc = mm_nt((col <= row).astype(F32), dec, HIGHEST)
    er = cr - dec
    ec = mm_nt((col < row).astype(F32), dec, HIGHEST)
    tot = cr[:, n - 1 : n]

    def pair_weights(h):
        forward = cc[:, h : h + 1] - cr[h : h + 1, :]
        backward = er[3 + h : 4 + h, :] - ec[:, 3 + h : 4 + h]
        return jnp.exp(jnp.where(col <= row, forward, backward))

    base = base_ref[...]
    cos_a = tab_ref[0] * base[0:1] - tab_ref[1] * base[1:2]
    sin_a = tab_ref[1] * base[0:1] + tab_ref[0] * base[1:2]

    def rotate_a(x, scale):
        x1, x2 = x[:, :half].astype(F32), x[:, half:].astype(F32)
        out = jnp.concatenate([x1 * cos_a - x2 * sin_a, x1 * sin_a + x2 * cos_a], axis=1)
        return (out * scale).astype(BF16)

    qa = rotate_a(qa_ref[...], 1.0)
    ka = rotate_a(ka_ref[...], 1.0 / math.sqrt(dk))
    qa_out[...] = qa

    width = 2 * hb
    lane = iota((n, width), 1)
    cos_b = tab_ref[2] * base[2:3] - tab_ref[3] * base[3:4]
    sin_b = tab_ref[3] * base[2:3] + tab_ref[2] * base[3:4]
    low = (lane % hb) < hq
    sin_b = jnp.where(low, -sin_b, sin_b)
    pr, pc = iota((width, width), 0), iota((width, width), 1)
    partner = jnp.where((pc % hb) < hq, pc + hq, pc - hq)
    swap = (pr == partner).astype(BF16)

    def rotate_b(x, scale):
        return ((x.astype(F32) * cos_b + mm(x, swap) * sin_b) * scale).astype(BF16)

    qb = rotate_b(qb_ref[...], 1.0)
    kb = rotate_b(kb_ref[...], 1.0 / math.sqrt(hb))
    qb_out[...] = qb

    va, vb = va_ref[...], vb_ref[...]
    kat = ka.astype(F32).T
    kbt = kb.astype(F32).T
    top = iota((width, n), 0) < hb
    for d in range(2):
        if d == 0:
            scale = [jnp.exp(tot[h : h + 1] - cr[h : h + 1, :]) for h in range(3)]
        else:
            scale = [jnp.exp(er[3 + h : 4 + h, :]) for h in range(3)]
        state = mm((kat * scale[0]).astype(BF16), va)
        pay_out[d, :dk, :] = state.astype(BF16)
        both = mm((kbt * jnp.where(top, scale[1], scale[2])).astype(BF16), vb)
        packed = jnp.where(iota((hb, width), 1) < hb, both[:hb], both[hb:]).astype(BF16)
        for q in range(dv // LANES):
            pay_out[d, dk : dk + TILE, q * LANES : (q + 1) * LANES] = packed[
                q * TILE : (q + 1) * TILE
            ]
        rows = iota((TILE, dv), 0)
        logs = jnp.zeros((TILE, dv), F32)
        for h in range(3):
            hi, lo = split2(tot[3 * d + h : 3 * d + h + 1])
            logs = jnp.where(rows == 2 * h, hi, jnp.where(rows == 2 * h + 1, lo, logs))
        pay_out[d, dk + TILE : dk + 2 * TILE, :] = logs.astype(BF16)
    weighted = (mm_nt(qa, ka) * pair_weights(0)).astype(BF16)
    loc_out[:, :dv] = mm(weighted, va)
    acc = jnp.zeros((n, width), F32)
    for h in range(2):
        mine = (lane < hb) if h == 0 else (lane >= hb)
        q_h = jnp.where(mine, qb.astype(F32), 0.0).astype(BF16)
        v_h = jnp.where(mine, vb.astype(F32), 0.0).astype(BF16)
        acc += mm((mm_nt(q_h, kb) * pair_weights(1 + h)).astype(BF16), v_h)
    loc_out[:, dv:] = acc


def retention_local(qa, ka, va, qb, kb, vb, dec, tab, base):
    n, dk = qa.shape
    dv, wb = va.shape[1], vb.shape[1]
    return pl.pallas_call(
        retention_body,
        out_shape=(
            jax.ShapeDtypeStruct((n, dk), BF16),
            jax.ShapeDtypeStruct((n, wb), BF16),
            jax.ShapeDtypeStruct((n, dv + wb), F32),
            jax.ShapeDtypeStruct((2, dk + 2 * TILE, dv), BF16),
        ),
        in_specs=vmem(9),
        out_specs=tuple(vmem(4)),
        interpret=INTERPRET,
        name="retention_local",
    )(qa, ka, va, qb, kb, vb, dec, tab, base)


def log_rows(ref, d, dk):
    rows = ref[d, dk + TILE : dk + 2 * TILE, :LANES].astype(F32)
    return [rows[2 * h : 2 * h + 1] + rows[2 * h + 1 : 2 * h + 2] for h in range(3)]


def pack_body(core_ref, own_ref, oth_ref, out_ref, ext_scr):
    chips = out_ref.shape[0]
    dv = own_ref.shape[2]
    dk = own_ref.shape[1] - 2 * TILE
    first = core_ref[0] == 0
    step = dk // chips
    blocks = dv // LANES // 2
    one = jnp.ones((1, LANES), F32)
    own_f, oth_f = log_rows(own_ref, 0, dk), log_rows(oth_ref, 0, dk)
    own_b, oth_b = log_rows(own_ref, 1, dk), log_rows(oth_ref, 1, dk)
    factor_own = [
        [jnp.where(first, jnp.exp(oth_f[h]), one) for h in range(3)],
        [jnp.where(first, one, jnp.exp(oth_b[h])) for h in range(3)],
    ]
    factor_oth = [
        [jnp.where(first, one, jnp.exp(own_f[h])) for h in range(3)],
        [jnp.where(first, jnp.exp(own_b[h]), one) for h in range(3)],
    ]
    lane = iota((1, LANES), 1)
    left = lane < LANES // 2
    for d in range(2):
        for q in range(blocks):
            a = slice(q * LANES, (q + 1) * LANES)
            b = slice((blocks + q) * LANES, (blocks + q + 1) * LANES)

            def mine(ref):
                return jnp.where(first, ref[d, :dk, a].astype(F32), ref[d, :dk, b].astype(F32))

            total = factor_own[d][0] * mine(own_ref) + factor_oth[d][0] * mine(oth_ref)
            at = (d * blocks + q) * step
            out_ref[:, at : at + step, :] = total.astype(BF16).reshape(chips, step, LANES)
    per = (dv // LANES) * TILE // chips
    for q in range(dv // LANES):
        part = []
        for d in range(2):
            fo = jnp.where(left, factor_own[d][1], factor_own[d][2])
            ft = jnp.where(left, factor_oth[d][1], factor_oth[d][2])
            cut = slice(q * LANES, (q + 1) * LANES)
            part.append(
                fo * own_ref[d, dk : dk + TILE, cut].astype(F32)
                + ft * oth_ref[d, dk : dk + TILE, cut].astype(F32)
            )
        part = jnp.where(first, part[0], part[1])
        for k in range(TILE // per):
            ext_scr[q * (TILE // per) + k, 0:per, :] = part[k * per : (k + 1) * per]
    rows = iota((TILE - per, LANES), 0)
    logs = jnp.zeros((TILE - per, LANES), F32)
    sums_f = [x + y for x, y in zip(own_f, oth_f)]
    sums_b = [x + y for x, y in zip(own_b, oth_b)]
    for k, value in enumerate(
        [
            sums_f[0],
            sums_b[0],
            jnp.where(left, sums_f[1], sums_f[2]),
            jnp.where(left, sums_b[1], sums_b[2]),
        ]
    ):
        hi, lo = split2(value)
        logs = jnp.where(rows == 2 * k, hi, jnp.where(rows == 2 * k + 1, lo, logs))
    ext_scr[:, per:, :] = jnp.broadcast_to(logs[None], (chips, TILE - per, LANES))
    at = 2 * blocks * step
    out_ref[:, at : at + TILE, :] = ext_scr[...].astype(BF16)


def pack_states(core, own, other, chips):
    dv = own.shape[2]
    dk = own.shape[1] - 2 * TILE
    rows = dv // LANES * (dk // chips) + TILE
    return pl.pallas_call(
        pack_body,
        out_shape=jax.ShapeDtypeStruct((chips, rows, LANES), BF16),
        in_specs=[SMEM_SPEC] + vmem(2),
        out_specs=vmem(1)[0],
        scratch_shapes=[pltpu.VMEM((chips, TILE, LANES), F32)],
        interpret=INTERPRET,
        name="pack_states",
    )(core, own, other)


def scan_body(per, core_ref, in_ref, out_ref):
    chips, rows, _ = in_ref.shape
    main = rows - TILE
    side = main // 2
    first = core_ref[0] == 0
    ext = [in_ref[i, main:, :].astype(F32) for i in range(chips)]
    decays = [
        [jnp.exp(e[per + 2 * k : per + 2 * k + 1] + e[per + 2 * k + 1 : per + 2 * k + 2]) for k in range(4)]
        for e in ext
    ]
    carry = jnp.zeros((side, LANES), F32)
    group = jnp.zeros((TILE, LANES), F32)
    into = []
    for i in range(chips):
        out_ref[i, :side, :] = carry.astype(BF16)
        into.append(group)
        carry = decays[i][0] * carry + in_ref[i, :side, :].astype(F32)
        group = decays[i][2] * group + ext[i]
    carry = jnp.zeros((side, LANES), F32)
    group = jnp.zeros((TILE, LANES), F32)
    for i in reversed(range(chips)):
        out_ref[i, side:main, :] = carry.astype(BF16)
        out_ref[i, main:, :] = jnp.where(first, into[i], group).astype(BF16)
        carry = decays[i][1] * carry + in_ref[i, side:main, :].astype(F32)
        group = decays[i][3] * group + ext[i]


def scan_states(core, pieces, per):
    def body(*refs):
        scan_body(per, *refs)

    return pl.pallas_call(
        body,
        out_shape=jax.ShapeDtypeStruct(pieces.shape, BF16),
        in_specs=[SMEM_SPEC] + vmem(1),
        out_specs=vmem(1)[0],
        interpret=INTERPRET,
        name="scan_states",
    )(core, pieces)


def mix_body(
    core_ref, qa_ref, qb_ref, loc_ref, own_ref, oth_ref, pay_ref, dec_ref, wa_ref, wb_ref,
    out_ref, grp_scr,
):
    n, dk = qa_ref.shape
    width = qb_ref.shape[1]
    hb = width // 2
    dv = loc_ref.shape[1] - width
    chips, rows, _ = own_ref.shape
    step = dk // chips
    blocks = dv // LANES // 2
    main = rows - TILE
    first = core_ref[0] == 0
    row, col = iota((n, n), 0), iota((n, n), 1)
    dec = dec_ref[...]
    cc = mm_nt((col <= row).astype(F32), dec, HIGHEST)
    rc = mm_nt((col >= row).astype(F32), dec, HIGHEST)
    col_f = [jnp.exp(cc[:, h : h + 1]) for h in range(3)]
    col_b = [jnp.exp(rc[:, 3 + h : 4 + h]) for h in range(3)]
    logs = [log_rows(pay_ref, d, dk) for d in range(2)]
    qa, qb = qa_ref[...], qb_ref[...]
    lane = iota((1, LANES), 1)
    left = lane < LANES // 2
    per = (dv // LANES) * TILE // chips
    total_a = loc_ref[:, :dv]
    total_b = loc_ref[:, dv:]
    for d in range(2):
        between = jnp.logical_not(first) if d == 0 else first
        factor = jnp.where(between, jnp.exp(logs[d][0]), jnp.ones((1, LANES), F32))
        keep = jnp.where(between, 1.0, 0.0)
        parts = []
        for b in range(2 * blocks):
            at = (d * blocks + b % blocks) * step
            own = own_ref[:, at : at + step, :].astype(F32)
            oth = oth_ref[:, at : at + step, :].astype(F32)
            use_own = first if b < blocks else jnp.logical_not(first)
            carry = jnp.where(use_own, own, oth).reshape(dk, LANES)
            near = pay_ref[d, :dk, b * LANES : (b + 1) * LANES].astype(F32)
            parts.append((factor * carry + keep * near).astype(BF16))
        state = jnp.concatenate(parts, axis=1)
        scale = col_f if d == 0 else col_b
        total_a = total_a + scale[0] * mm(qa, state)
        use_own = first if d == 0 else jnp.logical_not(first)
        ext = jnp.where(
            use_own, own_ref[:, main:, :].astype(F32), oth_ref[:, main:, :].astype(F32)
        )
        for i in range(chips):
            grp_scr[i * per : (i + 1) * per, :] = ext[i, 0:per, :]
        near = jnp.concatenate(
            [
                pay_ref[d, dk : dk + TILE, q * LANES : (q + 1) * LANES].astype(F32)
                for q in range(dv // LANES)
            ],
            axis=0,
        )
        factor = jnp.where(
            between,
            jnp.exp(jnp.where(left, logs[d][1], logs[d][2])),
            jnp.ones((1, LANES), F32),
        )
        group = factor * grp_scr[...] + keep * near
        blockdiag = jnp.concatenate(
            [jnp.where(left, group, 0.0), jnp.where(left, 0.0, group)], axis=0
        ).astype(BF16)
        total_b = total_b + jnp.where(left, scale[1], scale[2]) * mm(qb, blockdiag)
    square = jnp.mean(total_a * total_a, axis=1, keepdims=True)
    mixed_a = (total_a * lax.rsqrt(square + GROUP_EPS)).astype(BF16)
    sq = total_b * total_b
    s0 = jnp.sum(jnp.where(left, sq, 0.0), axis=1, keepdims=True) / hb
    s1 = jnp.sum(jnp.where(left, 0.0, sq), axis=1, keepdims=True) / hb
    mixed_b = (total_b * lax.rsqrt(jnp.where(left, s0, s1) + GROUP_EPS)).astype(BF16)
    out_ref[...] = (mm(mixed_a, wa_ref[...]) + mm(mixed_b, wb_ref[...])).astype(BF16)


def mix_project(core, qa, qb, loc, own, other, pay, dec, wa, wb):
    hb = qb.shape[1] // 2
    return pl.pallas_call(
        mix_body,
        out_shape=jax.ShapeDtypeStruct((qa.shape[0], wa.shape[1]), BF16),
        in_specs=[SMEM_SPEC] + vmem(9),
        out_specs=vmem(1)[0],
        scratch_shapes=[pltpu.VMEM((hb, qb.shape[1]), F32)],
        interpret=INTERPRET,
        name="mix_project",
    )(core, qa, qb, loc, own, other, pay, dec, wa, wb)


def layer_norm(stream, gain):
    center = stream - jnp.mean(stream, axis=-1, keepdims=True)
    spread = jnp.mean(center * center, axis=-1, keepdims=True)
    return center * lax.rsqrt(spread + NORM_EPS) * gain


def slots_by_route(ids):
    routes = ids.shape[1]
    row, col = iota((routes, routes), 0), iota((routes, routes), 1)
    ids_f = ids.astype(F32)
    ids_col = jnp.sum(jnp.where(row == col, ids_f, 0.0), axis=1, keepdims=True)
    same = (ids_col == ids_f) & (row < col)
    rank = jnp.sum(jnp.where(same, 1.0, 0.0), axis=0, keepdims=True)
    slot = ids_f * CAP + jnp.minimum(rank, CAP - 1.0)
    return jnp.where((row.astype(F32) == slot) & (rank < CAP), 1.0, 0.0)


def route_rows(rows, routes):
    return iota((rows, routes), 1) // TOP == iota((rows, routes), 0)


def store_chunks(value, out_ref, scr):
    rows, width = value.shape
    cuts = width // LANES
    for k in range(cuts):
        scr[pl.ds(k, rows, stride=cuts), :] = value[:, k * LANES : (k + 1) * LANES]
    out_ref[...] = scr[...].astype(BF16).reshape(out_ref.shape)


def load_chunks(ref, rows, scr):
    cuts = scr.shape[0] // rows
    scr[...] = ref[...].reshape(scr.shape).astype(F32)
    return jnp.concatenate(
        [scr[pl.ds(k, rows, stride=cuts), :] for k in range(cuts)], axis=1
    ).astype(BF16)


def dispatch_body(arr_ref, res_ref, gain_ref, ids_ref, hid_ref, out_ref, scr):
    mix = jnp.sum(arr_ref[...].astype(F32), axis=0)
    stream = RESIDUAL_SCALE * res_ref[...].astype(F32) + mix
    hidden = layer_norm(stream, gain_ref[0:1, :]).astype(BF16)
    hid_ref[...] = hidden
    hot = slots_by_route(ids_ref[...])
    belongs = jnp.where(route_rows(hidden.shape[0], hot.shape[1]), 1.0, 0.0)
    choose = mm_nt(hot.astype(BF16), belongs.astype(BF16)).astype(BF16)
    store_chunks(mm(choose, hidden), out_ref, scr)


def dispatch(arrived, residual, gain, ids, peers):
    rows, width = residual.shape
    lines = ids.shape[1] * width // LANES
    return pl.pallas_call(
        dispatch_body,
        out_shape=(
            jax.ShapeDtypeStruct((rows, width), BF16),
            jax.ShapeDtypeStruct((peers, lines // peers, LANES), BF16),
        ),
        in_specs=vmem(4),
        out_specs=tuple(vmem(2)),
        scratch_shapes=[pltpu.VMEM((lines, LANES), F32)],
        interpret=INTERPRET,
        name="dispatch",
    )(arrived, residual, gain, ids)


def pack_weights_body(part_ref, gate_ref, up_ref, down_ref, out_ref):
    _, width, units = gate_ref.shape
    half = units // 2
    part = part_ref[0]
    low = part == 0
    left = iota((width, units), 1) < half
    gate = gate_ref[0].astype(F32)
    up = up_ref[0].astype(F32)
    gate = jnp.where(low, gate, pltpu.roll(gate, half, 1))
    up = jnp.where(low, pltpu.roll(up, half, 1), up)
    out_ref[:width, :] = jnp.where(left, gate, up).astype(BF16)
    rows = pl.ds(pl.multiple_of(part * half, half), half)
    for k in range(width // units):
        out_ref[width + k * half : width + (k + 1) * half, :] = down_ref[
            0, rows, k * units : (k + 1) * units
        ]


def pack_weights(part, gate, up, down):
    _, width, units = gate.shape
    return pl.pallas_call(
        pack_weights_body,
        out_shape=jax.ShapeDtypeStruct((width + width // 2, units), BF16),
        in_specs=[SMEM_SPEC] + vmem(3),
        out_specs=vmem(1)[0],
        interpret=INTERPRET,
        name="pack_weights",
    )(part, gate, up, down)


def expert_body(own_ref, oth_ref, w_ref, mine_ref, send_ref, x_scr, w_scr, acc_ref, sems):
    count, depth, units = w_scr.shape
    rows = mine_ref.shape[0]
    width = mine_ref.shape[1]
    half = units // 2
    copies = [
        pltpu.make_async_copy(w_ref.at[k], w_scr.at[k], sems.at[k]) for k in range(count)
    ]
    for copy in copies:
        copy.start()
    x = jnp.concatenate(
        [load_chunks(own_ref, rows, x_scr), load_chunks(oth_ref, rows, x_scr)], axis=0
    )
    left = iota((2 * rows, units), 1) < half

    def silu(v):
        return v / (1.0 + jnp.exp(-v))

    group = 4
    for first in range(0, count, group):
        hidden = []
        for k in range(first, first + group, 2):
            copies[k].wait()
            copies[k + 1].wait()
            both = mm(x, jnp.concatenate([w_scr[k, :width, :], w_scr[k + 1, :width, :]], axis=1))
            one, two = both[:, :units], both[:, units:]
            one = silu(one) * pltpu.roll(one, half, 1)
            two = silu(pltpu.roll(two, half, 1)) * two
            hidden.append(jnp.where(left, one, two).astype(BF16))
        hidden = jnp.concatenate(hidden, axis=1)
        for c in range(0, width // units, 2):
            cols = []
            for j in (c, c + 1):
                at = width + j * half
                cols.append(
                    jnp.concatenate(
                        [w_scr[k, at : at + half, :] for k in range(first, first + group)], axis=0
                    )
                )
            part = mm(hidden, jnp.concatenate(cols, axis=1))
            cut = slice(c * units, (c + 2) * units)
            if first == 0:
                acc_ref[:, cut] = part
            elif first < count - group:
                acc_ref[:, cut] += part
            else:
                part = acc_ref[:, cut] + part
                mine_ref[:, cut] = part[:rows]
                send_ref[:, cut] = part[rows:].astype(BF16)


def experts(own, other, weights):
    count, depth, units = weights.shape
    width = depth * 2 // 3
    lines = own.shape[0] * own.shape[1]
    rows = lines * LANES // width
    return pl.pallas_call(
        expert_body,
        out_shape=(
            jax.ShapeDtypeStruct((rows, width), F32),
            jax.ShapeDtypeStruct((rows, width), BF16),
        ),
        in_specs=vmem(2) + [ANY_SPEC],
        out_specs=tuple(vmem(2)),
        scratch_shapes=[
            pltpu.VMEM((lines, LANES), F32),
            pltpu.VMEM((count, depth, units), BF16),
            pltpu.VMEM((2 * rows, width), F32),
            pltpu.SemaphoreType.DMA((count,)),
        ],
        interpret=INTERPRET,
        name="experts",
    )(own, other, weights)


def finish_body(mine_ref, arrived_ref, out_ref, scr):
    store_chunks(mine_ref[...] + arrived_ref[...].astype(F32), out_ref, scr)


def finish(mine, arrived, peers):
    rows, width = mine.shape
    lines = rows * width // LANES
    return pl.pallas_call(
        finish_body,
        out_shape=jax.ShapeDtypeStruct((peers, lines // peers, LANES), BF16),
        in_specs=vmem(2),
        out_specs=vmem(1)[0],
        scratch_shapes=[pltpu.VMEM((lines, LANES), F32)],
        interpret=INTERPRET,
        name="finish",
    )(mine, arrived)


def combine_body(ret_ref, hid_ref, gain_ref, ids_ref, w_ref, out_ref, scr):
    hidden = hid_ref[...]
    hot = slots_by_route(ids_ref[...])
    factor = jnp.where(route_rows(hidden.shape[0], hot.shape[1]), w_ref[...], 0.0)
    weights = mm_nt(factor, hot, HIGHEST)
    returned = load_chunks(ret_ref, hot.shape[0], scr)
    hi = weights.astype(BF16)
    rest = weights - hi.astype(F32)
    mid = rest.astype(BF16)
    low = (rest - mid.astype(F32)).astype(BF16)
    ffn = mm(hi, returned) + mm(mid, returned) + mm(low, returned)
    stream = RESIDUAL_SCALE * hidden.astype(F32) + ffn
    out_ref[...] = layer_norm(stream, gain_ref[1:2, :]).astype(BF16)


def combine(returned, hidden, gain, ids, weights):
    lines = returned.shape[0] * returned.shape[1]
    return pl.pallas_call(
        combine_body,
        out_shape=jax.ShapeDtypeStruct(hidden.shape, BF16),
        in_specs=vmem(5),
        out_specs=vmem(1)[0],
        scratch_shapes=[pltpu.VMEM((lines, LANES), F32)],
        interpret=INTERPRET,
        name="combine",
    )(returned, hidden, gain, ids, weights)


def exchange(array, axis):
    return lax.all_to_all(array, axis, split_axis=0, concat_axis=0, tiled=True)


def decay_rows(decay_a, decay_b):
    length = decay_a.shape[-1]
    return jnp.concatenate(
        [decay_a[0], decay_b[0], decay_a[1], decay_b[1], jnp.zeros((2, length), F32)], axis=0
    )


def shards(
    query_a, key_a, value_a, decay_a, query_b, key_b, value_b, decay_b, out_weight_a,
    out_weight_b, residual, norm_gain, route_group, route_expert, route_weight, expert_gate,
    expert_up, expert_down,
):
    length = query_a.shape[0]
    chips = lax.axis_size("sp_0")
    sp_count = lax.axis_size(SP)
    tp = lax.axis_size("tp")
    rows_dev, width = residual.shape
    routes = rows_dev * TOP
    part = (lax.axis_index("grp") % 2).astype(jnp.int32).reshape(1)
    partner = [(k, k ^ 1) for k in range(lax.axis_size("grp"))]
    weights_all = lax.all_gather(
        pack_weights(part, expert_gate, expert_up, expert_down), "tp"
    )

    core = lax.axis_index("sp_1").astype(jnp.int32).reshape(1)
    local, base = angle_tables(
        length, query_a.shape[1] // 2, query_b.shape[1] // 4, sp_count
    )
    base = lax.dynamic_index_in_dim(jnp.asarray(base), lax.axis_index(SP), 0, keepdims=False)
    dec = decay_rows(decay_a, decay_b)
    qa, qb, loc, pay = retention_local(
        query_a, key_a, value_a, query_b, key_b, value_b, dec, jnp.asarray(local), base
    )
    swap = [(0, 1), (1, 0)]
    pay_other = lax.ppermute(pay, "sp_1", swap)
    pieces = exchange(pack_states(core, pay, pay_other, chips), "sp_0")
    per = value_a.shape[1] // LANES * TILE // chips
    carried = exchange(scan_states(core, pieces, per), "sp_0")
    carried_other = lax.ppermute(carried, "sp_1", swap)
    partial = mix_project(
        core, qa, qb, loc, carried, carried_other, pay_other, dec, out_weight_a, out_weight_b
    )
    arrived = exchange(partial.reshape(tp, rows_dev, width), "tp")
    ids = (route_group[:, None] * EXP_GROUP + route_expert).reshape(1, routes)
    hidden, outgoing = dispatch(arrived, residual, norm_gain, ids, sp_count)
    received = exchange(outgoing, SP)
    received_other = lax.ppermute(received, "grp", partner)
    mine, send = experts(received, received_other, weights_all)
    back = finish(mine, lax.ppermute(send, "grp", partner), sp_count)
    returned = exchange(back, SP)
    return combine(returned, hidden, norm_gain, ids, route_weight.reshape(1, routes))


def solution(mesh):
    sp = mesh.shape["sp"]
    finer = Mesh(
        mesh.devices.reshape(mesh.shape["grp"], sp // 2, 2, mesh.shape["tp"]),
        ("grp", "sp_0", "sp_1", "tp"),
    )
    in_specs = (
        P(GRP_SP, "tp"),
        P(GRP_SP, "tp"),
        P(GRP_SP, "tp"),
        P(None, "tp", GRP_SP),
        P(GRP_SP, "tp"),
        P(GRP_SP, "tp"),
        P(GRP_SP, "tp"),
        P(None, "tp", GRP_SP),
        P("tp", None),
        P("tp", None),
        P(GRP_SP_TP, None),
        P(),
        P(GRP_SP_TP),
        P(GRP_SP_TP, None),
        P(GRP_SP_TP, None),
        P(SP, None, "tp"),
        P(SP, None, "tp"),
        P(SP, "tp", None),
    )
    out_specs = P(GRP_SP_TP, None)
    return jax.shard_map(
        shards, mesh=finer, in_specs=in_specs, out_specs=out_specs, check_vma=False
    )
```

```python
import math

import jax
import jax.numpy as jnp
import numpy as np
from jax import lax
from jax.experimental import pallas as pl
from jax.experimental.pallas import tpu as pltpu
from jax.sharding import Mesh
from jax.sharding import PartitionSpec as P

CAP = 2
TOP = 2
EXP_GROUP = 8
SP = ("sp_0", "sp_1")
GRP_SP = ("grp", "sp_0", "sp_1")
GRP_SP_TP = ("grp", "sp_0", "sp_1", "tp")

RESIDUAL_SCALE = math.sqrt(2.0)
NORM_EPS = 1e-05
GROUP_EPS = 1e-06
ROPE_BASE = 10000.0

F32 = jnp.float32
BF16 = jnp.bfloat16
HIGHEST = lax.Precision.HIGHEST
INTERPRET = False

LANES = 128
TILE = 16
SIDE = 8


def vmem(count):
    return [pl.BlockSpec(memory_space=pltpu.VMEM)] * count


def near(array):
    return array if INTERPRET else pltpu.with_memory_space_constraint(array, pltpu.VMEM)


def far(array):
    return array if INTERPRET else pltpu.with_memory_space_constraint(array, pltpu.HBM)


def near_shape(shape, dtype):
    return jax.ShapeDtypeStruct(shape, dtype) if INTERPRET else pltpu.VMEM(shape, dtype)


SMEM_SPEC = pl.BlockSpec(memory_space=pltpu.SMEM)
PARAMS = pltpu.CompilerParams(vmem_limit_bytes=20 << 20)
ANY_SPEC = pl.BlockSpec(memory_space=pl.ANY)


def iota(shape, dim):
    return lax.broadcasted_iota(jnp.int32, shape, dim)


def mm(a, b):
    return jnp.dot(a, b, preferred_element_type=F32)


def mm_nt(a, b, precision=None):
    return lax.dot_general(
        a, b, (((1,), (1,)), ((), ())), precision=precision, preferred_element_type=F32
    )


def split2(x):
    hi = x.astype(BF16).astype(F32)
    return hi, x - hi


def angle_tables(length, half_a, half_b, devices):
    def freqs(half):
        f = np.float32(ROPE_BASE) ** (-np.arange(half, dtype=np.float32) / np.float32(half))
        return f.astype(np.float64)

    fa = freqs(half_a)
    fb = np.tile(freqs(half_b), LANES // half_b)
    inside = np.arange(length, dtype=np.float64)[:, None]
    first = (np.arange(devices, dtype=np.float64) * length)[:, None]
    local = np.stack(
        [np.cos(inside * fa), np.sin(inside * fa), np.cos(inside * fb), np.sin(inside * fb)]
    ).astype(np.float32)
    base = np.zeros((devices, 8, LANES), np.float32)
    for k, row in enumerate(
        [np.cos(first * fa), np.sin(first * fa), np.cos(first * fb), np.sin(first * fb)]
    ):
        base[:, k, :] = row
    return local, base


def retention_body(
    index_ref, qa_ref, ka_ref, va_ref, qb_ref, kb_ref, vb_ref, da_ref, db_ref, tab_ref, base_ref,
    qa_out, qb_out, loc_out, pay_out, dec_out,
):
    n, dk = qa_ref.shape
    dv = va_ref.shape[1]
    half = dk // 2
    hb = qb_ref.shape[1] // 2
    hq = hb // 2
    row, col = iota((n, n), 0), iota((n, n), 1)
    for d in range(2):
        dec_out[3 * d : 3 * d + 1, :] = da_ref[d]
        dec_out[3 * d + 1 : 3 * d + 3, :] = db_ref[d]
    dec_out[6:8, :] = jnp.zeros((2, n), F32)
    dec = dec_out[...]
    cr = jnp.dot(dec, (row <= col).astype(F32), precision=HIGHEST, preferred_element_type=F32)
    cc = mm_nt((col <= row).astype(F32), dec, HIGHEST)
    er = cr - dec
    ec = mm_nt((col < row).astype(F32), dec, HIGHEST)
    tot = cr[:, n - 1 : n]

    def pair_weights(h):
        forward = cc[:, h : h + 1] - cr[h : h + 1, :]
        backward = er[3 + h : 4 + h, :] - ec[:, 3 + h : 4 + h]
        return jnp.exp(jnp.where(col <= row, forward, backward))

    base = base_ref[index_ref[0]]
    cos_a = tab_ref[0] * base[0:1] - tab_ref[1] * base[1:2]
    sin_a = tab_ref[1] * base[0:1] + tab_ref[0] * base[1:2]

    def rotate_a(x, scale):
        x1, x2 = x[:, :half].astype(F32), x[:, half:].astype(F32)
        out = jnp.concatenate([x1 * cos_a - x2 * sin_a, x1 * sin_a + x2 * cos_a], axis=1)
        return (out * scale).astype(BF16)

    qa = rotate_a(qa_ref[...], 1.0)
    ka = rotate_a(ka_ref[...], 1.0 / math.sqrt(dk))
    qa_out[...] = qa

    width = 2 * hb
    lane = iota((n, width), 1)
    cos_b = tab_ref[2] * base[2:3] - tab_ref[3] * base[3:4]
    sin_b = tab_ref[3] * base[2:3] + tab_ref[2] * base[3:4]
    low = (lane % hb) < hq
    sin_b = jnp.where(low, -sin_b, sin_b)
    pr, pc = iota((width, width), 0), iota((width, width), 1)
    partner = jnp.where((pc % hb) < hq, pc + hq, pc - hq)
    swap = (pr == partner).astype(BF16)

    def rotate_b(x, scale):
        return ((x.astype(F32) * cos_b + mm(x, swap) * sin_b) * scale).astype(BF16)

    qb = rotate_b(qb_ref[...], 1.0)
    kb = rotate_b(kb_ref[...], 1.0 / math.sqrt(hb))
    qb_out[...] = qb

    va, vb = va_ref[...], vb_ref[...]
    kat = ka.astype(F32).T
    kbt = kb.astype(F32).T
    top = iota((width, n), 0) < hb
    for d in range(2):
        if d == 0:
            scale = [jnp.exp(tot[h : h + 1] - cr[h : h + 1, :]) for h in range(3)]
        else:
            scale = [jnp.exp(er[3 + h : 4 + h, :]) for h in range(3)]
        state = mm((kat * scale[0]).astype(BF16), va)
        pay_out[d, :dk, :] = state.astype(BF16)
        both = mm((kbt * jnp.where(top, scale[1], scale[2])).astype(BF16), vb)
        packed = jnp.where(iota((hb, width), 1) < hb, both[:hb], both[hb:]).astype(BF16)
        for q in range(dv // LANES):
            pay_out[d, dk : dk + TILE, q * LANES : (q + 1) * LANES] = packed[
                q * TILE : (q + 1) * TILE
            ]
        rows = iota((TILE, dv), 0)
        logs = jnp.zeros((TILE, dv), F32)
        for h in range(3):
            hi, lo = split2(tot[3 * d + h : 3 * d + h + 1])
            logs = jnp.where(rows == 2 * h, hi, jnp.where(rows == 2 * h + 1, lo, logs))
        pay_out[d, dk + TILE : dk + 2 * TILE, :] = logs.astype(BF16)
    weighted = (mm_nt(qa, ka) * pair_weights(0)).astype(BF16)
    loc_out[:, :dv] = mm(weighted, va)
    acc = jnp.zeros((n, width), F32)
    for h in range(2):
        mine = (lane < hb) if h == 0 else (lane >= hb)
        q_h = jnp.where(mine, qb.astype(F32), 0.0).astype(BF16)
        v_h = jnp.where(mine, vb.astype(F32), 0.0).astype(BF16)
        acc += mm((mm_nt(q_h, kb) * pair_weights(1 + h)).astype(BF16), v_h)
    loc_out[:, dv:] = acc


def retention_local(index, qa, ka, va, qb, kb, vb, da, db, tab, base):
    n, dk = qa.shape
    dv, wb = va.shape[1], vb.shape[1]
    return pl.pallas_call(
        retention_body,
        out_shape=(
            near_shape((n, dk), BF16),
            near_shape((n, wb), BF16),
            near_shape((n, dv + wb), F32),
            near_shape((2, dk + 2 * TILE, dv), BF16),
            near_shape((8, n), F32),
        ),
        in_specs=[SMEM_SPEC] + vmem(10),
        out_specs=tuple(vmem(5)),
        interpret=INTERPRET,
        compiler_params=PARAMS,
        name="retention_local",
    )(index, *map(far, (qa, ka, va, qb, kb, vb, da, db, tab, base)))


def log_rows(ref, d, dk):
    rows = ref[d, dk + TILE : dk + 2 * TILE, :LANES].astype(F32)
    return [rows[2 * h : 2 * h + 1] + rows[2 * h + 1 : 2 * h + 2] for h in range(3)]


def pack_body(core_ref, own_ref, oth_ref, out_ref, ext_scr):
    chips = out_ref.shape[0]
    dv = own_ref.shape[2]
    dk = own_ref.shape[1] - 2 * TILE
    first = core_ref[0] == 0
    step = dk // chips
    blocks = dv // LANES // 2
    one = jnp.ones((1, LANES), F32)
    own_f, oth_f = log_rows(own_ref, 0, dk), log_rows(oth_ref, 0, dk)
    own_b, oth_b = log_rows(own_ref, 1, dk), log_rows(oth_ref, 1, dk)
    factor_own = [
        [jnp.where(first, jnp.exp(oth_f[h]), one) for h in range(3)],
        [jnp.where(first, one, jnp.exp(oth_b[h])) for h in range(3)],
    ]
    factor_oth = [
        [jnp.where(first, one, jnp.exp(own_f[h])) for h in range(3)],
        [jnp.where(first, jnp.exp(own_b[h]), one) for h in range(3)],
    ]
    lane = iota((1, LANES), 1)
    left = lane < LANES // 2
    for d in range(2):
        for q in range(blocks):
            a = slice(q * LANES, (q + 1) * LANES)
            b = slice((blocks + q) * LANES, (blocks + q + 1) * LANES)

            def mine(ref):
                return jnp.where(first, ref[d, :dk, a].astype(F32), ref[d, :dk, b].astype(F32))

            total = factor_own[d][0] * mine(own_ref) + factor_oth[d][0] * mine(oth_ref)
            at = (d * blocks + q) * step
            out_ref[:, at : at + step, :] = total.astype(BF16).reshape(chips, step, LANES)
    per = (dv // LANES) * TILE // chips
    for q in range(dv // LANES):
        part = []
        for d in range(2):
            fo = jnp.where(left, factor_own[d][1], factor_own[d][2])
            ft = jnp.where(left, factor_oth[d][1], factor_oth[d][2])
            cut = slice(q * LANES, (q + 1) * LANES)
            part.append(
                fo * own_ref[d, dk : dk + TILE, cut].astype(F32)
                + ft * oth_ref[d, dk : dk + TILE, cut].astype(F32)
            )
        part = jnp.where(first, part[0], part[1])
        for k in range(TILE // per):
            ext_scr[q * (TILE // per) + k, 0:per, :] = part[k * per : (k + 1) * per]
    quarter = lane // (LANES // 4)

    def quarters(values):
        out = values[0]
        for k in range(1, len(values)):
            out = jnp.where(quarter == k, values[k], out)
        return out

    sums_f = [x + y for x, y in zip(own_f, oth_f)]
    sums_b = [x + y for x, y in zip(own_b, oth_b)]
    lines = [
        *split2(quarters([sums_f[1], sums_f[2], sums_f[0], sums_b[0]])),
        *split2(quarters([sums_b[1], sums_b[2]])),
    ]
    for k, line in enumerate(lines):
        ext_scr[:, per + k : per + k + 1, :] = jnp.broadcast_to(line[None], (chips, 1, LANES))
    at = 2 * blocks * step
    out_ref[:, at : at + SIDE, :] = ext_scr[...].astype(BF16)


def pack_states(core, own, other, chips):
    dv = own.shape[2]
    dk = own.shape[1] - 2 * TILE
    rows = dv // LANES * (dk // chips) + SIDE
    return pl.pallas_call(
        pack_body,
        out_shape=near_shape((chips, rows, LANES), BF16),
        in_specs=[SMEM_SPEC] + vmem(2),
        out_specs=vmem(1)[0],
        scratch_shapes=[pltpu.VMEM((chips, SIDE, LANES), F32)],
        interpret=INTERPRET,
        compiler_params=PARAMS,
        name="pack_states",
    )(core, near(own), near(other))


def scan_body(per, core_ref, in_ref, out_ref):
    chips, rows, _ = in_ref.shape
    main = rows - SIDE
    side = main // 2
    first = core_ref[0] == 0
    left = iota((1, LANES), 1) < LANES // 2
    ext = [in_ref[i, main:, :].astype(F32) for i in range(chips)]
    decays = []
    for e in ext:
        one = jnp.exp(e[per : per + 1] + e[per + 1 : per + 2])
        two = jnp.exp(e[per + 2 : per + 3] + e[per + 3 : per + 4])

        def lane(line, k):
            at = k * (LANES // 4)
            return line[:, at : at + 1]

        decays.append(
            [
                lane(one, 2),
                lane(one, 3),
                jnp.where(left, lane(one, 0), lane(one, 1)),
                jnp.where(left, lane(two, 0), lane(two, 1)),
            ]
        )
    carry = jnp.zeros((side, LANES), F32)
    group = jnp.zeros((SIDE, LANES), F32)
    into = []
    for i in range(chips):
        out_ref[i, :side, :] = carry.astype(BF16)
        into.append(group)
        carry = decays[i][0] * carry + in_ref[i, :side, :].astype(F32)
        group = decays[i][2] * group + ext[i]
    carry = jnp.zeros((side, LANES), F32)
    group = jnp.zeros((SIDE, LANES), F32)
    for i in reversed(range(chips)):
        out_ref[i, side:main, :] = carry.astype(BF16)
        out_ref[i, main:, :] = jnp.where(first, into[i], group).astype(BF16)
        carry = decays[i][1] * carry + in_ref[i, side:main, :].astype(F32)
        group = decays[i][3] * group + ext[i]


def scan_states(core, pieces, per):
    def body(*refs):
        scan_body(per, *refs)

    return pl.pallas_call(
        body,
        out_shape=near_shape(pieces.shape, BF16),
        in_specs=[SMEM_SPEC] + vmem(1),
        out_specs=vmem(1)[0],
        interpret=INTERPRET,
        compiler_params=PARAMS,
        name="scan_states",
    )(core, near(pieces))


def mix_body(
    core_ref, qa_ref, qb_ref, loc_ref, own_ref, oth_ref, pay_ref, dec_ref, wa_ref, wb_ref,
    out_ref, grp_scr,
):
    n, dk = qa_ref.shape
    width = qb_ref.shape[1]
    hb = width // 2
    dv = loc_ref.shape[1] - width
    chips, rows, _ = own_ref.shape
    step = dk // chips
    blocks = dv // LANES // 2
    main = rows - SIDE
    first = core_ref[0] == 0
    row, col = iota((n, n), 0), iota((n, n), 1)
    dec = dec_ref[...]
    cc = mm_nt((col <= row).astype(F32), dec, HIGHEST)
    rc = mm_nt((col >= row).astype(F32), dec, HIGHEST)
    col_f = [jnp.exp(cc[:, h : h + 1]) for h in range(3)]
    col_b = [jnp.exp(rc[:, 3 + h : 4 + h]) for h in range(3)]
    logs = [log_rows(pay_ref, d, dk) for d in range(2)]
    qa, qb = qa_ref[...], qb_ref[...]
    lane = iota((1, LANES), 1)
    left = lane < LANES // 2
    per = (dv // LANES) * TILE // chips
    total_a = loc_ref[:, :dv]
    total_b = loc_ref[:, dv:]
    for d in range(2):
        between = jnp.logical_not(first) if d == 0 else first
        factor = jnp.where(between, jnp.exp(logs[d][0]), jnp.ones((1, LANES), F32))
        keep = jnp.where(between, 1.0, 0.0)
        parts = []
        for b in range(2 * blocks):
            at = (d * blocks + b % blocks) * step
            own = own_ref[:, at : at + step, :].astype(F32)
            oth = oth_ref[:, at : at + step, :].astype(F32)
            use_own = first if b < blocks else jnp.logical_not(first)
            carry = jnp.where(use_own, own, oth).reshape(dk, LANES)
            near = pay_ref[d, :dk, b * LANES : (b + 1) * LANES].astype(F32)
            parts.append((factor * carry + keep * near).astype(BF16))
        state = jnp.concatenate(parts, axis=1)
        scale = col_f if d == 0 else col_b
        total_a = total_a + scale[0] * mm(qa, state)
        use_own = first if d == 0 else jnp.logical_not(first)
        ext = jnp.where(
            use_own, own_ref[:, main:, :].astype(F32), oth_ref[:, main:, :].astype(F32)
        )
        for i in range(chips):
            grp_scr[i * per : (i + 1) * per, :] = ext[i, 0:per, :]
        near = jnp.concatenate(
            [
                pay_ref[d, dk : dk + TILE, q * LANES : (q + 1) * LANES].astype(F32)
                for q in range(dv // LANES)
            ],
            axis=0,
        )
        factor = jnp.where(
            between,
            jnp.exp(jnp.where(left, logs[d][1], logs[d][2])),
            jnp.ones((1, LANES), F32),
        )
        group = factor * grp_scr[...] + keep * near
        blockdiag = jnp.concatenate(
            [jnp.where(left, group, 0.0), jnp.where(left, 0.0, group)], axis=0
        ).astype(BF16)
        total_b = total_b + jnp.where(left, scale[1], scale[2]) * mm(qb, blockdiag)
    square = jnp.mean(total_a * total_a, axis=1, keepdims=True)
    mixed_a = (total_a * lax.rsqrt(square + GROUP_EPS)).astype(BF16)
    sq = total_b * total_b
    s0 = jnp.sum(jnp.where(left, sq, 0.0), axis=1, keepdims=True) / hb
    s1 = jnp.sum(jnp.where(left, 0.0, sq), axis=1, keepdims=True) / hb
    mixed_b = (total_b * lax.rsqrt(jnp.where(left, s0, s1) + GROUP_EPS)).astype(BF16)
    out_ref[...] = (mm(mixed_a, wa_ref[...]) + mm(mixed_b, wb_ref[...])).astype(BF16)


def mix_project(core, qa, qb, loc, own, other, pay, dec, wa, wb):
    hb = qb.shape[1] // 2
    return pl.pallas_call(
        mix_body,
        out_shape=near_shape((qa.shape[0], wa.shape[1]), BF16),
        in_specs=[SMEM_SPEC] + vmem(9),
        out_specs=vmem(1)[0],
        scratch_shapes=[pltpu.VMEM((hb, qb.shape[1]), F32)],
        interpret=INTERPRET,
        compiler_params=PARAMS,
        name="mix_project",
    )(core, *map(near, (qa, qb, loc, own, other, pay, dec)), wa, wb)


def layer_norm(stream, gain):
    center = stream - jnp.mean(stream, axis=-1, keepdims=True)
    spread = jnp.mean(center * center, axis=-1, keepdims=True)
    return center * lax.rsqrt(spread + NORM_EPS) * gain


def slots_by_route(ids):
    routes = ids.shape[1]
    row, col = iota((routes, routes), 0), iota((routes, routes), 1)
    ids_f = ids.astype(F32)
    ids_col = jnp.sum(jnp.where(row == col, ids_f, 0.0), axis=1, keepdims=True)
    same = (ids_col == ids_f) & (row < col)
    rank = jnp.sum(jnp.where(same, 1.0, 0.0), axis=0, keepdims=True)
    slot = ids_f * CAP + jnp.minimum(rank, CAP - 1.0)
    return jnp.where((row.astype(F32) == slot) & (rank < CAP), 1.0, 0.0)


def route_rows(rows, routes):
    return iota((rows, routes), 1) // TOP == iota((rows, routes), 0)


def store_chunks(value, out_ref, scr):
    rows, width = value.shape
    cuts = width // LANES
    for k in range(cuts):
        scr[pl.ds(k, rows, stride=cuts), :] = value[:, k * LANES : (k + 1) * LANES]
    out_ref[...] = scr[...].astype(BF16).reshape(out_ref.shape)


def load_chunks(ref, rows, scr):
    cuts = scr.shape[0] // rows
    scr[...] = ref[...].reshape(scr.shape).astype(F32)
    return jnp.concatenate(
        [scr[pl.ds(k, rows, stride=cuts), :] for k in range(cuts)], axis=1
    ).astype(BF16)


def dispatch_body(arr_ref, res_ref, gain_ref, ids_ref, hid_ref, out_ref, scr):
    mix = jnp.sum(arr_ref[...].astype(F32), axis=0)
    stream = RESIDUAL_SCALE * res_ref[...].astype(F32) + mix
    hidden = layer_norm(stream, gain_ref[0:1, :]).astype(BF16)
    hid_ref[...] = hidden
    hot = slots_by_route(ids_ref[...])
    belongs = jnp.where(route_rows(hidden.shape[0], hot.shape[1]), 1.0, 0.0)
    choose = mm_nt(hot.astype(BF16), belongs.astype(BF16)).astype(BF16)
    store_chunks(mm(choose, hidden), out_ref, scr)


def dispatch(arrived, residual, gain, ids, peers):
    rows, width = residual.shape
    lines = ids.shape[1] * width // LANES
    return pl.pallas_call(
        dispatch_body,
        out_shape=(
            near_shape((rows, width), BF16),
            near_shape((peers, lines // peers, LANES), BF16),
        ),
        in_specs=vmem(4),
        out_specs=tuple(vmem(2)),
        scratch_shapes=[pltpu.VMEM((lines, LANES), F32)],
        interpret=INTERPRET,
        compiler_params=PARAMS,
        name="dispatch",
    )(near(arrived), residual, gain, ids)


def pack_weights_body(part_ref, gate_ref, up_ref, down_ref, out_ref):
    _, width, units = gate_ref.shape
    half = units // 2
    part = part_ref[0]
    low = part == 0
    left = iota((width, units), 1) < half
    gate = gate_ref[0].astype(F32)
    up = up_ref[0].astype(F32)
    gate = jnp.where(low, gate, pltpu.roll(gate, half, 1))
    up = jnp.where(low, pltpu.roll(up, half, 1), up)
    out_ref[:width, :] = jnp.where(left, gate, up).astype(BF16)
    rows = pl.ds(pl.multiple_of(part * half, half), half)
    for k in range(width // units):
        out_ref[width + k * half : width + (k + 1) * half, :] = down_ref[
            0, rows, k * units : (k + 1) * units
        ]


def pack_weights(part, gate, up, down):
    _, width, units = gate.shape
    return pl.pallas_call(
        pack_weights_body,
        out_shape=jax.ShapeDtypeStruct((width + width // 2, units), BF16),
        in_specs=[SMEM_SPEC] + vmem(3),
        out_specs=vmem(1)[0],
        interpret=INTERPRET,
        compiler_params=PARAMS,
        name="pack_weights",
    )(part, far(gate), far(up), far(down))


def expert_body(own_ref, oth_ref, w_ref, mine_ref, send_ref, x_scr, w_scr, acc_ref, sems):
    count, depth, units = w_scr.shape
    rows = mine_ref.shape[0]
    width = mine_ref.shape[1]
    half = units // 2
    copies = [
        pltpu.make_async_copy(w_ref.at[k], w_scr.at[k], sems.at[k]) for k in range(count)
    ]
    for copy in copies:
        copy.start()
    x = jnp.concatenate(
        [load_chunks(own_ref, rows, x_scr), load_chunks(oth_ref, rows, x_scr)], axis=0
    )
    left = iota((2 * rows, units), 1) < half

    def silu(v):
        return v / (1.0 + jnp.exp(-v))

    group = 4
    for first in range(0, count, group):
        hidden = []
        for k in range(first, first + group, 2):
            copies[k].wait()
            copies[k + 1].wait()
            both = mm(x, jnp.concatenate([w_scr[k, :width, :], w_scr[k + 1, :width, :]], axis=1))
            one, two = both[:, :units], both[:, units:]
            one = silu(one) * pltpu.roll(one, half, 1)
            two = silu(pltpu.roll(two, half, 1)) * two
            hidden.append(jnp.where(left, one, two).astype(BF16))
        hidden = jnp.concatenate(hidden, axis=1)
        for c in range(0, width // units, 2):
            cols = []
            for j in (c, c + 1):
                at = width + j * half
                cols.append(
                    jnp.concatenate(
                        [w_scr[k, at : at + half, :] for k in range(first, first + group)], axis=0
                    )
                )
            part = mm(hidden, jnp.concatenate(cols, axis=1))
            cut = slice(c * units, (c + 2) * units)
            if first == 0:
                acc_ref[:, cut] = part
            elif first < count - group:
                acc_ref[:, cut] += part
            else:
                part = acc_ref[:, cut] + part
                mine_ref[:, cut] = part[:rows]
                send_ref[:, cut] = part[rows:].astype(BF16)


def experts(own, other, weights):
    count, depth, units = weights.shape
    width = depth * 2 // 3
    lines = own.shape[0] * own.shape[1]
    rows = lines * LANES // width
    return pl.pallas_call(
        expert_body,
        out_shape=(
            near_shape((rows, width), F32),
            near_shape((rows, width), BF16),
        ),
        in_specs=vmem(2) + [ANY_SPEC],
        out_specs=tuple(vmem(2)),
        scratch_shapes=[
            pltpu.VMEM((lines, LANES), F32),
            pltpu.VMEM((count, depth, units), BF16),
            pltpu.VMEM((2 * rows, width), F32),
            pltpu.SemaphoreType.DMA((count,)),
        ],
        interpret=INTERPRET,
        compiler_params=PARAMS,
        name="experts",
    )(near(own), near(other), far(weights))


def finish_body(mine_ref, arrived_ref, out_ref, scr):
    store_chunks(mine_ref[...] + arrived_ref[...].astype(F32), out_ref, scr)


def finish(mine, arrived, peers):
    rows, width = mine.shape
    lines = rows * width // LANES
    return pl.pallas_call(
        finish_body,
        out_shape=near_shape((peers, lines // peers, LANES), BF16),
        in_specs=vmem(2),
        out_specs=vmem(1)[0],
        scratch_shapes=[pltpu.VMEM((lines, LANES), F32)],
        interpret=INTERPRET,
        compiler_params=PARAMS,
        name="finish",
    )(near(mine), near(arrived))


def combine_body(ret_ref, hid_ref, gain_ref, ids_ref, w_ref, out_ref, scr):
    hidden = hid_ref[...]
    hot = slots_by_route(ids_ref[...])
    factor = jnp.where(route_rows(hidden.shape[0], hot.shape[1]), w_ref[...], 0.0)
    weights = mm_nt(factor, hot, HIGHEST)
    returned = load_chunks(ret_ref, hot.shape[0], scr)
    hi = weights.astype(BF16)
    rest = weights - hi.astype(F32)
    mid = rest.astype(BF16)
    low = (rest - mid.astype(F32)).astype(BF16)
    ffn = mm(hi, returned) + mm(mid, returned) + mm(low, returned)
    stream = RESIDUAL_SCALE * hidden.astype(F32) + ffn
    out_ref[...] = layer_norm(stream, gain_ref[1:2, :]).astype(BF16)


def combine(returned, hidden, gain, ids, weights):
    lines = returned.shape[0] * returned.shape[1]
    return pl.pallas_call(
        combine_body,
        out_shape=jax.ShapeDtypeStruct(hidden.shape, BF16),
        in_specs=vmem(5),
        out_specs=vmem(1)[0],
        scratch_shapes=[pltpu.VMEM((lines, LANES), F32)],
        interpret=INTERPRET,
        compiler_params=PARAMS,
        name="combine",
    )(near(returned), near(hidden), gain, ids, weights)


def exchange(array, axis):
    return lax.all_to_all(array, axis, split_axis=0, concat_axis=0, tiled=True)


def shards(
    query_a, key_a, value_a, decay_a, query_b, key_b, value_b, decay_b, out_weight_a,
    out_weight_b, residual, norm_gain, route_group, route_expert, route_weight, expert_gate,
    expert_up, expert_down,
):
    length = query_a.shape[0]
    chips = lax.axis_size("sp_0")
    sp_count = lax.axis_size(SP)
    tp = lax.axis_size("tp")
    rows_dev, width = residual.shape
    routes = rows_dev * TOP
    part = (lax.axis_index("grp") % 2).astype(jnp.int32).reshape(1)
    partner = [(k, k ^ 1) for k in range(lax.axis_size("grp"))]
    weights_all = lax.all_gather(
        pack_weights(part, expert_gate, expert_up, expert_down), "tp"
    )

    core = lax.axis_index("sp_1").astype(jnp.int32).reshape(1)
    local, base = angle_tables(
        length, query_a.shape[1] // 2, query_b.shape[1] // 4, sp_count
    )
    index = lax.axis_index(SP).astype(jnp.int32).reshape(1)
    qa, qb, loc, pay, dec = retention_local(
        index, query_a, key_a, value_a, query_b, key_b, value_b, decay_a, decay_b,
        jnp.asarray(local), jnp.asarray(base),
    )
    swap = [(0, 1), (1, 0)]
    pay_other = lax.ppermute(pay, "sp_1", swap)
    pieces = exchange(pack_states(core, pay, pay_other, chips), "sp_0")
    per = value_a.shape[1] // LANES * TILE // chips
    carried = exchange(scan_states(core, pieces, per), "sp_0")
    carried_other = lax.ppermute(carried, "sp_1", swap)
    partial = mix_project(
        core, qa, qb, loc, carried, carried_other, pay_other, dec, out_weight_a, out_weight_b
    )
    arrived = exchange(partial.reshape(tp, rows_dev, width), "tp")
    ids = (route_group[:, None] * EXP_GROUP + route_expert).reshape(1, routes)
    hidden, outgoing = dispatch(arrived, residual, norm_gain, ids, sp_count)
    received = exchange(outgoing, SP)
    received_other = lax.ppermute(received, "grp", partner)
    mine, send = experts(received, received_other, weights_all)
    back = finish(mine, lax.ppermute(send, "grp", partner), sp_count)
    returned = exchange(back, SP)
    return combine(returned, hidden, norm_gain, ids, route_weight.reshape(1, routes))


def solution(mesh):
    sp = mesh.shape["sp"]
    finer = Mesh(
        mesh.devices.reshape(mesh.shape["grp"], sp // 2, 2, mesh.shape["tp"]),
        ("grp", "sp_0", "sp_1", "tp"),
    )
    in_specs = (
        P(GRP_SP, "tp"),
        P(GRP_SP, "tp"),
        P(GRP_SP, "tp"),
        P(None, "tp", GRP_SP),
        P(GRP_SP, "tp"),
        P(GRP_SP, "tp"),
        P(GRP_SP, "tp"),
        P(None, "tp", GRP_SP),
        P("tp", None),
        P("tp", None),
        P(GRP_SP_TP, None),
        P(),
        P(GRP_SP_TP),
        P(GRP_SP_TP, None),
        P(GRP_SP_TP, None),
        P(SP, None, "tp"),
        P(SP, None, "tp"),
        P(SP, "tp", None),
    )
    out_specs = P(GRP_SP_TP, None)
    return jax.shard_map(
        shards, mesh=finer, in_specs=in_specs, out_specs=out_specs, check_vma=False
    )
```

```python
import math

import jax
import jax.numpy as jnp
import numpy as np
from jax import lax
from jax.experimental import pallas as pl
from jax.experimental.pallas import tpu as pltpu
from jax.sharding import Mesh
from jax.sharding import PartitionSpec as P


CAP = 2
TOP = 2
EXP_GROUP = 8
SP = ("sp_0", "sp_1")
GRP_SP = ("grp", "sp_0", "sp_1")
GRP_SP_TP = ("grp", "sp_0", "sp_1", "tp")

RESIDUAL_SCALE = math.sqrt(2.0)
NORM_EPS = 1e-05
GROUP_EPS = 1e-06
ROPE_BASE = 10000.0

F32 = jnp.float32
BF16 = jnp.bfloat16
HIGHEST = lax.Precision.HIGHEST
INTERPRET = False

LANES = 128
TILE = 16
SIDE = 8


def vmem(count):
    return [pl.BlockSpec(memory_space=pltpu.VMEM)] * count


def near(array):
    return array if INTERPRET else pltpu.with_memory_space_constraint(array, pltpu.VMEM)


def far(array):
    return array if INTERPRET else pltpu.with_memory_space_constraint(array, pltpu.HBM)


def near_shape(shape, dtype):
    return jax.ShapeDtypeStruct(shape, dtype) if INTERPRET else pltpu.VMEM(shape, dtype)


SMEM_SPEC = pl.BlockSpec(memory_space=pltpu.SMEM)
PARAMS = pltpu.CompilerParams(vmem_limit_bytes=20 << 20)
ANY_SPEC = pl.BlockSpec(memory_space=pl.ANY)


def iota(shape, dim):
    return lax.broadcasted_iota(jnp.int32, shape, dim)


def mm(a, b):
    return jnp.dot(a, b, preferred_element_type=F32)


def mm_nt(a, b, precision=None):
    return lax.dot_general(
        a, b, (((1,), (1,)), ((), ())), precision=precision, preferred_element_type=F32
    )


def split2(x):
    hi = x.astype(BF16).astype(F32)
    return hi, x - hi


def angle_tables(length, half_a, half_b, devices):
    def freqs(half):
        f = np.float32(ROPE_BASE) ** (-np.arange(half, dtype=np.float32) / np.float32(half))
        return f.astype(np.float64)

    fa = freqs(half_a)
    fb = np.tile(freqs(half_b), LANES // half_b)
    inside = np.arange(length, dtype=np.float64)[:, None]
    first = (np.arange(devices, dtype=np.float64) * length)[:, None]
    local = np.stack(
        [np.cos(inside * fa), np.sin(inside * fa), np.cos(inside * fb), np.sin(inside * fb)]
    ).astype(np.float32)
    base = np.zeros((devices, 8, LANES), np.float32)
    for k, row in enumerate(
        [np.cos(first * fa), np.sin(first * fa), np.cos(first * fb), np.sin(first * fb)]
    ):
        base[:, k, :] = row
    return local, base


def retention_body(
    index_ref, qa_ref, ka_ref, va_ref, qb_ref, kb_ref, vb_ref, da_ref, db_ref, tab_ref, base_ref,
    qa_out, qb_out, loc_out, pay_out, dec_out,
):
    n, dk = qa_ref.shape
    dv = va_ref.shape[1]
    half = dk // 2
    hb = qb_ref.shape[1] // 2
    hq = hb // 2
    row, col = iota((n, n), 0), iota((n, n), 1)
    for d in range(2):
        dec_out[3 * d : 3 * d + 1, :] = da_ref[d]
        dec_out[3 * d + 1 : 3 * d + 3, :] = db_ref[d]
    dec_out[6:8, :] = jnp.zeros((2, n), F32)
    dec = dec_out[...]
    cr = jnp.dot(dec, (row <= col).astype(F32), precision=HIGHEST, preferred_element_type=F32)
    cc = mm_nt((col <= row).astype(F32), dec, HIGHEST)
    er = cr - dec
    ec = mm_nt((col < row).astype(F32), dec, HIGHEST)
    tot = cr[:, n - 1 : n]

    def pair_weights(h):
        forward = cc[:, h : h + 1] - cr[h : h + 1, :]
        backward = er[3 + h : 4 + h, :] - ec[:, 3 + h : 4 + h]
        return jnp.exp(jnp.where(col <= row, forward, backward))

    base = base_ref[index_ref[0]]
    cos_a = tab_ref[0] * base[0:1] - tab_ref[1] * base[1:2]
    sin_a = tab_ref[1] * base[0:1] + tab_ref[0] * base[1:2]

    def rotate_a(x, scale):
        x1, x2 = x[:, :half].astype(F32), x[:, half:].astype(F32)
        out = jnp.concatenate([x1 * cos_a - x2 * sin_a, x1 * sin_a + x2 * cos_a], axis=1)
        return (out * scale).astype(BF16)

    qa = rotate_a(qa_ref[...], 1.0)
    ka = rotate_a(ka_ref[...], 1.0 / math.sqrt(dk))
    qa_out[...] = qa

    width = 2 * hb
    lane = iota((n, width), 1)
    cos_b = tab_ref[2] * base[2:3] - tab_ref[3] * base[3:4]
    sin_b = tab_ref[3] * base[2:3] + tab_ref[2] * base[3:4]
    low = (lane % hb) < hq
    sin_b = jnp.where(low, -sin_b, sin_b)
    pr, pc = iota((width, width), 0), iota((width, width), 1)
    partner = jnp.where((pc % hb) < hq, pc + hq, pc - hq)
    swap = (pr == partner).astype(BF16)

    def rotate_b(x, scale):
        return ((x.astype(F32) * cos_b + mm(x, swap) * sin_b) * scale).astype(BF16)

    qb = rotate_b(qb_ref[...], 1.0)
    kb = rotate_b(kb_ref[...], 1.0 / math.sqrt(hb))
    qb_out[...] = qb

    va, vb = va_ref[...], vb_ref[...]
    kat = ka.astype(F32).T
    kbt = kb.astype(F32).T
    top = iota((width, n), 0) < hb
    for d in range(2):
        if d == 0:
            scale = [jnp.exp(tot[h : h + 1] - cr[h : h + 1, :]) for h in range(3)]
        else:
            scale = [jnp.exp(er[3 + h : 4 + h, :]) for h in range(3)]
        state = mm((kat * scale[0]).astype(BF16), va)
        pay_out[d, :dk, :] = state.astype(BF16)
        both = mm((kbt * jnp.where(top, scale[1], scale[2])).astype(BF16), vb)
        packed = jnp.where(iota((hb, width), 1) < hb, both[:hb], both[hb:]).astype(BF16)
        for q in range(dv // LANES):
            pay_out[d, dk : dk + TILE, q * LANES : (q + 1) * LANES] = packed[
                q * TILE : (q + 1) * TILE
            ]
        rows = iota((TILE, dv), 0)
        logs = jnp.zeros((TILE, dv), F32)
        for h in range(3):
            hi, lo = split2(tot[3 * d + h : 3 * d + h + 1])
            logs = jnp.where(rows == 2 * h, hi, jnp.where(rows == 2 * h + 1, lo, logs))
        pay_out[d, dk + TILE : dk + 2 * TILE, :] = logs.astype(BF16)
    weighted = (mm_nt(qa, ka) * pair_weights(0)).astype(BF16)
    loc_out[:, :dv] = mm(weighted, va)
    acc = jnp.zeros((n, width), F32)
    for h in range(2):
        mine = (lane < hb) if h == 0 else (lane >= hb)
        q_h = jnp.where(mine, qb.astype(F32), 0.0).astype(BF16)
        v_h = jnp.where(mine, vb.astype(F32), 0.0).astype(BF16)
        acc += mm((mm_nt(q_h, kb) * pair_weights(1 + h)).astype(BF16), v_h)
    loc_out[:, dv:] = acc


def retention_local(index, qa, ka, va, qb, kb, vb, da, db, tab, base):
    n, dk = qa.shape
    dv, wb = va.shape[1], vb.shape[1]
    return pl.pallas_call(
        retention_body,
        out_shape=(
            near_shape((n, dk), BF16),
            near_shape((n, wb), BF16),
            near_shape((n, dv + wb), F32),
            near_shape((2, dk + 2 * TILE, dv), BF16),
            near_shape((8, n), F32),
        ),
        in_specs=[SMEM_SPEC] + vmem(10),
        out_specs=tuple(vmem(5)),
        interpret=INTERPRET,
        compiler_params=PARAMS,
        name="retention_local",
    )(index, *map(far, (qa, ka, va, qb, kb, vb, da, db, tab, base)))


def log_rows(ref, d, dk):
    rows = ref[d, dk + TILE : dk + 2 * TILE, :LANES].astype(F32)
    return [rows[2 * h : 2 * h + 1] + rows[2 * h + 1 : 2 * h + 2] for h in range(3)]


def pack_body(core_ref, own_ref, oth_ref, out_ref, ext_scr):
    chips = out_ref.shape[0]
    dv = own_ref.shape[2]
    dk = own_ref.shape[1] - 2 * TILE
    first = core_ref[0] == 0
    step = dk // chips
    blocks = dv // LANES // 2
    one = jnp.ones((1, LANES), F32)
    own_f, oth_f = log_rows(own_ref, 0, dk), log_rows(oth_ref, 0, dk)
    own_b, oth_b = log_rows(own_ref, 1, dk), log_rows(oth_ref, 1, dk)
    factor_own = [
        [jnp.where(first, jnp.exp(oth_f[h]), one) for h in range(3)],
        [jnp.where(first, one, jnp.exp(oth_b[h])) for h in range(3)],
    ]
    factor_oth = [
        [jnp.where(first, one, jnp.exp(own_f[h])) for h in range(3)],
        [jnp.where(first, jnp.exp(own_b[h]), one) for h in range(3)],
    ]
    lane = iota((1, LANES), 1)
    left = lane < LANES // 2
    for d in range(2):
        for q in range(blocks):
            a = slice(q * LANES, (q + 1) * LANES)
            b = slice((blocks + q) * LANES, (blocks + q + 1) * LANES)

            def mine(ref):
                return jnp.where(first, ref[d, :dk, a].astype(F32), ref[d, :dk, b].astype(F32))

            total = factor_own[d][0] * mine(own_ref) + factor_oth[d][0] * mine(oth_ref)
            at = (d * blocks + q) * step
            out_ref[:, at : at + step, :] = total.astype(BF16).reshape(chips, step, LANES)
    per = (dv // LANES) * TILE // chips
    for q in range(dv // LANES):
        part = []
        for d in range(2):
            fo = jnp.where(left, factor_own[d][1], factor_own[d][2])
            ft = jnp.where(left, factor_oth[d][1], factor_oth[d][2])
            cut = slice(q * LANES, (q + 1) * LANES)
            part.append(
                fo * own_ref[d, dk : dk + TILE, cut].astype(F32)
                + ft * oth_ref[d, dk : dk + TILE, cut].astype(F32)
            )
        part = jnp.where(first, part[0], part[1])
        for k in range(TILE // per):
            ext_scr[q * (TILE // per) + k, 0:per, :] = part[k * per : (k + 1) * per]
    quarter = lane // (LANES // 4)

    def quarters(values):
        out = values[0]
        for k in range(1, len(values)):
            out = jnp.where(quarter == k, values[k], out)
        return out

    sums_f = [x + y for x, y in zip(own_f, oth_f)]
    sums_b = [x + y for x, y in zip(own_b, oth_b)]
    lines = [
        *split2(quarters([sums_f[1], sums_f[2], sums_f[0], sums_b[0]])),
        *split2(quarters([sums_b[1], sums_b[2]])),
    ]
    for k, line in enumerate(lines):
        ext_scr[:, per + k : per + k + 1, :] = jnp.broadcast_to(line[None], (chips, 1, LANES))
    at = 2 * blocks * step
    out_ref[:, at : at + SIDE, :] = ext_scr[...].astype(BF16)


def pack_states(core, own, other, chips):
    dv = own.shape[2]
    dk = own.shape[1] - 2 * TILE
    rows = dv // LANES * (dk // chips) + SIDE
    return pl.pallas_call(
        pack_body,
        out_shape=near_shape((chips, rows, LANES), BF16),
        in_specs=[SMEM_SPEC] + vmem(2),
        out_specs=vmem(1)[0],
        scratch_shapes=[pltpu.VMEM((chips, SIDE, LANES), F32)],
        interpret=INTERPRET,
        compiler_params=PARAMS,
        name="pack_states",
    )(core, near(own), near(other))


def scan_body(per, core_ref, in_ref, out_ref):
    chips, rows, _ = in_ref.shape
    main = rows - SIDE
    side = main // 2
    first = core_ref[0] == 0
    left = iota((1, LANES), 1) < LANES // 2
    ext = [in_ref[i, main:, :].astype(F32) for i in range(chips)]
    decays = []
    for e in ext:
        one = jnp.exp(e[per : per + 1] + e[per + 1 : per + 2])
        two = jnp.exp(e[per + 2 : per + 3] + e[per + 3 : per + 4])

        def lane(line, k):
            at = k * (LANES // 4)
            return line[:, at : at + 1]

        decays.append(
            [
                lane(one, 2),
                lane(one, 3),
                jnp.where(left, lane(one, 0), lane(one, 1)),
                jnp.where(left, lane(two, 0), lane(two, 1)),
            ]
        )
    carry = jnp.zeros((side, LANES), F32)
    group = jnp.zeros((SIDE, LANES), F32)
    into = []
    for i in range(chips):
        out_ref[i, :side, :] = carry.astype(BF16)
        into.append(group)
        carry = decays[i][0] * carry + in_ref[i, :side, :].astype(F32)
        group = decays[i][2] * group + ext[i]
    carry = jnp.zeros((side, LANES), F32)
    group = jnp.zeros((SIDE, LANES), F32)
    for i in reversed(range(chips)):
        out_ref[i, side:main, :] = carry.astype(BF16)
        out_ref[i, main:, :] = jnp.where(first, into[i], group).astype(BF16)
        carry = decays[i][1] * carry + in_ref[i, side:main, :].astype(F32)
        group = decays[i][3] * group + ext[i]


def scan_states(core, pieces, per):
    def body(*refs):
        scan_body(per, *refs)

    return pl.pallas_call(
        body,
        out_shape=near_shape(pieces.shape, BF16),
        in_specs=[SMEM_SPEC] + vmem(1),
        out_specs=vmem(1)[0],
        interpret=INTERPRET,
        compiler_params=PARAMS,
        name="scan_states",
    )(core, near(pieces))


def mix_body(
    core_ref, qa_ref, qb_ref, loc_ref, own_ref, oth_ref, pay_ref, dec_ref, wa_ref, wb_ref,
    out_ref, grp_scr, wa_scr, wb_scr, sems,
):
    copies = [
        pltpu.make_async_copy(wa_ref, wa_scr, sems.at[0]),
        pltpu.make_async_copy(wb_ref, wb_scr, sems.at[1]),
    ]
    for copy in copies:
        copy.start()
    n, dk = qa_ref.shape
    width = qb_ref.shape[1]
    hb = width // 2
    dv = loc_ref.shape[1] - width
    chips, rows, _ = own_ref.shape
    step = dk // chips
    blocks = dv // LANES // 2
    main = rows - SIDE
    first = core_ref[0] == 0
    row, col = iota((n, n), 0), iota((n, n), 1)
    dec = dec_ref[...]
    cc = mm_nt((col <= row).astype(F32), dec, HIGHEST)
    rc = mm_nt((col >= row).astype(F32), dec, HIGHEST)
    col_f = [jnp.exp(cc[:, h : h + 1]) for h in range(3)]
    col_b = [jnp.exp(rc[:, 3 + h : 4 + h]) for h in range(3)]
    logs = [log_rows(pay_ref, d, dk) for d in range(2)]
    qa, qb = qa_ref[...], qb_ref[...]
    lane = iota((1, LANES), 1)
    left = lane < LANES // 2
    per = (dv // LANES) * TILE // chips
    total_a = loc_ref[:, :dv]
    total_b = loc_ref[:, dv:]
    for d in range(2):
        between = jnp.logical_not(first) if d == 0 else first
        factor = jnp.where(between, jnp.exp(logs[d][0]), jnp.ones((1, LANES), F32))
        keep = jnp.where(between, 1.0, 0.0)
        parts = []
        for b in range(2 * blocks):
            at = (d * blocks + b % blocks) * step
            own = own_ref[:, at : at + step, :].astype(F32)
            oth = oth_ref[:, at : at + step, :].astype(F32)
            use_own = first if b < blocks else jnp.logical_not(first)
            carry = jnp.where(use_own, own, oth).reshape(dk, LANES)
            near = pay_ref[d, :dk, b * LANES : (b + 1) * LANES].astype(F32)
            parts.append((factor * carry + keep * near).astype(BF16))
        state = jnp.concatenate(parts, axis=1)
        scale = col_f if d == 0 else col_b
        total_a = total_a + scale[0] * mm(qa, state)
        use_own = first if d == 0 else jnp.logical_not(first)
        ext = jnp.where(
            use_own, own_ref[:, main:, :].astype(F32), oth_ref[:, main:, :].astype(F32)
        )
        for i in range(chips):
            grp_scr[i * per : (i + 1) * per, :] = ext[i, 0:per, :]
        near = jnp.concatenate(
            [
                pay_ref[d, dk : dk + TILE, q * LANES : (q + 1) * LANES].astype(F32)
                for q in range(dv // LANES)
            ],
            axis=0,
        )
        factor = jnp.where(
            between,
            jnp.exp(jnp.where(left, logs[d][1], logs[d][2])),
            jnp.ones((1, LANES), F32),
        )
        group = factor * grp_scr[...] + keep * near
        blockdiag = jnp.concatenate(
            [jnp.where(left, group, 0.0), jnp.where(left, 0.0, group)], axis=0
        ).astype(BF16)
        total_b = total_b + jnp.where(left, scale[1], scale[2]) * mm(qb, blockdiag)
    square = jnp.mean(total_a * total_a, axis=1, keepdims=True)
    mixed_a = (total_a * lax.rsqrt(square + GROUP_EPS)).astype(BF16)
    sq = total_b * total_b
    s0 = jnp.sum(jnp.where(left, sq, 0.0), axis=1, keepdims=True) / hb
    s1 = jnp.sum(jnp.where(left, 0.0, sq), axis=1, keepdims=True) / hb
    mixed_b = (total_b * lax.rsqrt(jnp.where(left, s0, s1) + GROUP_EPS)).astype(BF16)
    for copy in copies:
        copy.wait()
    out_ref[...] = (mm(mixed_a, wa_scr[...]) + mm(mixed_b, wb_scr[...])).astype(BF16)


def mix_project(core, qa, qb, loc, own, other, pay, dec, wa, wb):
    hb = qb.shape[1] // 2
    return pl.pallas_call(
        mix_body,
        out_shape=near_shape((qa.shape[0], wa.shape[1]), BF16),
        in_specs=[SMEM_SPEC] + vmem(7) + [ANY_SPEC] * 2,
        out_specs=vmem(1)[0],
        scratch_shapes=[
            pltpu.VMEM((hb, qb.shape[1]), F32),
            pltpu.VMEM(wa.shape, BF16),
            pltpu.VMEM(wb.shape, BF16),
            pltpu.SemaphoreType.DMA((2,)),
        ],
        interpret=INTERPRET,
        compiler_params=PARAMS,
        name="mix_project",
    )(core, *map(near, (qa, qb, loc, own, other, pay, dec)), far(wa), far(wb))


def layer_norm(stream, gain):
    center = stream - jnp.mean(stream, axis=-1, keepdims=True)
    spread = jnp.mean(center * center, axis=-1, keepdims=True)
    return center * lax.rsqrt(spread + NORM_EPS) * gain


def slots_by_route(ids):
    routes = ids.shape[1]
    row, col = iota((routes, routes), 0), iota((routes, routes), 1)
    ids_f = ids.astype(F32)
    ids_col = jnp.sum(jnp.where(row == col, ids_f, 0.0), axis=1, keepdims=True)
    same = (ids_col == ids_f) & (row < col)
    rank = jnp.sum(jnp.where(same, 1.0, 0.0), axis=0, keepdims=True)
    slot = ids_f * CAP + jnp.minimum(rank, CAP - 1.0)
    return jnp.where((row.astype(F32) == slot) & (rank < CAP), 1.0, 0.0)


def route_rows(rows, routes):
    return iota((rows, routes), 1) // TOP == iota((rows, routes), 0)


def store_chunks(value, out_ref, scr):
    rows, width = value.shape
    cuts = width // LANES
    for k in range(cuts):
        scr[pl.ds(k, rows, stride=cuts), :] = value[:, k * LANES : (k + 1) * LANES]
    out_ref[...] = scr[...].astype(BF16).reshape(out_ref.shape)


def load_chunks(ref, rows, scr):
    cuts = scr.shape[0] // rows
    scr[...] = ref[...].reshape(scr.shape).astype(F32)
    return jnp.concatenate(
        [scr[pl.ds(k, rows, stride=cuts), :] for k in range(cuts)], axis=1
    ).astype(BF16)


def dispatch_body(arr_ref, res_ref, gain_ref, ids_ref, hid_ref, out_ref, scr):
    mix = jnp.sum(arr_ref[...].astype(F32), axis=0)
    stream = RESIDUAL_SCALE * res_ref[...].astype(F32) + mix
    hidden = layer_norm(stream, gain_ref[0:1, :]).astype(BF16)
    hid_ref[...] = hidden
    hot = slots_by_route(ids_ref[...])
    belongs = jnp.where(route_rows(hidden.shape[0], hot.shape[1]), 1.0, 0.0)
    choose = mm_nt(hot.astype(BF16), belongs.astype(BF16)).astype(BF16)
    store_chunks(mm(choose, hidden), out_ref, scr)


def dispatch(arrived, residual, gain, ids, peers):
    rows, width = residual.shape
    lines = ids.shape[1] * width // LANES
    return pl.pallas_call(
        dispatch_body,
        out_shape=(
            near_shape((rows, width), BF16),
            near_shape((peers, lines // peers, LANES), BF16),
        ),
        in_specs=vmem(4),
        out_specs=tuple(vmem(2)),
        scratch_shapes=[pltpu.VMEM((lines, LANES), F32)],
        interpret=INTERPRET,
        compiler_params=PARAMS,
        name="dispatch",
    )(near(arrived), residual, gain, ids)


def hand_on(*arrays):
    count = len(arrays)

    def body(*refs):
        del refs

    return pl.pallas_call(
        body,
        out_shape=tuple(jax.ShapeDtypeStruct(x.shape, x.dtype) for x in arrays),
        in_specs=[ANY_SPEC] * count,
        out_specs=tuple([ANY_SPEC] * count),
        input_output_aliases={k: k for k in range(count)},
        interpret=INTERPRET,
        compiler_params=PARAMS,
        name="hand_on",
    )(*map(far, arrays))


def pack_weights_body(part_ref, gate_ref, up_ref, down_ref, out_ref):
    _, width, units = gate_ref.shape
    half = units // 2
    part = part_ref[0]
    low = part == 0
    left = iota((width, units), 1) < half
    gate = gate_ref[0].astype(F32)
    up = up_ref[0].astype(F32)
    gate = jnp.where(low, gate, pltpu.roll(gate, half, 1))
    up = jnp.where(low, pltpu.roll(up, half, 1), up)
    out_ref[:width, :] = jnp.where(left, gate, up).astype(BF16)
    rows = pl.ds(pl.multiple_of(part * half, half), half)
    for k in range(width // units):
        out_ref[width + k * half : width + (k + 1) * half, :] = down_ref[
            0, rows, k * units : (k + 1) * units
        ]


def pack_weights(part, gate, up, down):
    _, width, units = gate.shape
    return pl.pallas_call(
        pack_weights_body,
        out_shape=jax.ShapeDtypeStruct((width + width // 2, units), BF16),
        in_specs=[SMEM_SPEC] + vmem(3),
        out_specs=vmem(1)[0],
        interpret=INTERPRET,
        compiler_params=PARAMS,
        name="pack_weights",
    )(part, far(gate), far(up), far(down))


def expert_body(own_ref, oth_ref, *refs):
    *held, mine_ref, send_ref, x_scr, blocks, acc_ref, sems = refs
    count, _, units = blocks.shape
    rows = mine_ref.shape[0]
    width = mine_ref.shape[1]
    half = units // 2
    copies = [pltpu.make_async_copy(held[k], blocks.at[k], sems.at[k]) for k in range(count)]
    for copy in copies:
        copy.start()
    x = jnp.concatenate(
        [load_chunks(own_ref, rows, x_scr), load_chunks(oth_ref, rows, x_scr)], axis=0
    )
    left = iota((2 * rows, units), 1) < half

    def silu(v):
        return v / (1.0 + jnp.exp(-v))

    group = 4
    for first in range(0, count, group):
        hidden = []
        for k in range(first, first + group, 2):
            copies[k].wait()
            copies[k + 1].wait()
            both = mm(x, jnp.concatenate([blocks[k, :width, :], blocks[k + 1, :width, :]], axis=1))
            one, two = both[:, :units], both[:, units:]
            one = silu(one) * pltpu.roll(one, half, 1)
            two = silu(pltpu.roll(two, half, 1)) * two
            hidden.append(jnp.where(left, one, two).astype(BF16))
        hidden = jnp.concatenate(hidden, axis=1)
        for c in range(0, width // units, 2):
            cols = []
            for j in (c, c + 1):
                at = width + j * half
                cols.append(
                    jnp.concatenate(
                        [blocks[k, at : at + half, :] for k in range(first, first + group)], axis=0
                    )
                )
            part = mm(hidden, jnp.concatenate(cols, axis=1))
            cut = slice(c * units, (c + 2) * units)
            if first == 0:
                acc_ref[:, cut] = part
            elif first < count - group:
                acc_ref[:, cut] += part
            else:
                part = acc_ref[:, cut] + part
                mine_ref[:, cut] = part[:rows]
                send_ref[:, cut] = part[rows:].astype(BF16)


def experts(own, other, blocks):
    depth, units = blocks[0].shape
    width = depth * 2 // 3
    lines = own.shape[0] * own.shape[1]
    rows = lines * LANES // width
    return pl.pallas_call(
        expert_body,
        out_shape=(
            near_shape((rows, width), F32),
            near_shape((rows, width), BF16),
        ),
        in_specs=vmem(2) + [ANY_SPEC] * len(blocks),
        out_specs=tuple(vmem(2)),
        scratch_shapes=[
            pltpu.VMEM((lines, LANES), F32),
            pltpu.VMEM((len(blocks), depth, units), BF16),
            pltpu.VMEM((2 * rows, width), F32),
            pltpu.SemaphoreType.DMA((len(blocks),)),
        ],
        interpret=INTERPRET,
        compiler_params=PARAMS,
        name="experts",
    )(near(own), near(other), *map(far, blocks))


def finish_body(mine_ref, arrived_ref, out_ref, scr):
    store_chunks(mine_ref[...] + arrived_ref[...].astype(F32), out_ref, scr)


def finish(mine, arrived, peers):
    rows, width = mine.shape
    lines = rows * width // LANES
    return pl.pallas_call(
        finish_body,
        out_shape=near_shape((peers, lines // peers, LANES), BF16),
        in_specs=vmem(2),
        out_specs=vmem(1)[0],
        scratch_shapes=[pltpu.VMEM((lines, LANES), F32)],
        interpret=INTERPRET,
        compiler_params=PARAMS,
        name="finish",
    )(near(mine), near(arrived))


def combine_body(ret_ref, hid_ref, gain_ref, ids_ref, w_ref, out_ref, scr):
    hidden = hid_ref[...]
    hot = slots_by_route(ids_ref[...])
    factor = jnp.where(route_rows(hidden.shape[0], hot.shape[1]), w_ref[...], 0.0)
    weights = mm_nt(factor, hot, HIGHEST)
    returned = load_chunks(ret_ref, hot.shape[0], scr)
    hi = weights.astype(BF16)
    rest = weights - hi.astype(F32)
    mid = rest.astype(BF16)
    low = (rest - mid.astype(F32)).astype(BF16)
    ffn = mm(hi, returned) + mm(mid, returned) + mm(low, returned)
    stream = RESIDUAL_SCALE * hidden.astype(F32) + ffn
    out_ref[...] = layer_norm(stream, gain_ref[1:2, :]).astype(BF16)


def combine(returned, hidden, gain, ids, weights):
    lines = returned.shape[0] * returned.shape[1]
    return pl.pallas_call(
        combine_body,
        out_shape=jax.ShapeDtypeStruct(hidden.shape, BF16),
        in_specs=vmem(5),
        out_specs=vmem(1)[0],
        scratch_shapes=[pltpu.VMEM((lines, LANES), F32)],
        interpret=INTERPRET,
        compiler_params=PARAMS,
        name="combine",
    )(near(returned), near(hidden), gain, ids, weights)


def exchange(array, axis):
    return lax.all_to_all(array, axis, split_axis=0, concat_axis=0, tiled=True)


def shards(
    query_a, key_a, value_a, decay_a, query_b, key_b, value_b, decay_b, out_weight_a,
    out_weight_b, residual, norm_gain, route_group, route_expert, route_weight, expert_gate,
    expert_up, expert_down,
):
    length = query_a.shape[0]
    chips = lax.axis_size("sp_0")
    sp_count = lax.axis_size(SP)
    tp = lax.axis_size("tp")
    rows_dev, width = residual.shape
    routes = rows_dev * TOP
    part = (lax.axis_index("grp") % 2).astype(jnp.int32).reshape(1)
    partner = [(k, k ^ 1) for k in range(lax.axis_size("grp"))]
    up_ring = [(k, (k + 1) % tp) for k in range(tp)]
    down_ring = [(k, (k - 1) % tp) for k in range(tp)]

    core = lax.axis_index("sp_1").astype(jnp.int32).reshape(1)
    local, base = angle_tables(
        length, query_a.shape[1] // 2, query_b.shape[1] // 4, sp_count
    )
    index = lax.axis_index(SP).astype(jnp.int32).reshape(1)
    qa, qb, loc, pay, dec = retention_local(
        index, query_a, key_a, value_a, query_b, key_b, value_b, decay_a, decay_b,
        jnp.asarray(local), jnp.asarray(base),
    )
    swap = [(0, 1), (1, 0)]
    pay_other = lax.ppermute(pay, "sp_1", swap)
    packed = pack_weights(part, expert_gate, expert_up, expert_down)
    blocks = [packed]
    held = (lax.ppermute(packed, "tp", up_ring), lax.ppermute(packed, "tp", down_ring))
    outgoing_states = pack_states(core, pay, pay_other, chips)
    pieces = exchange(outgoing_states, "sp_0")
    held = hand_on(*held)
    blocks += held
    held = (lax.ppermute(held[0], "tp", up_ring), lax.ppermute(held[1], "tp", down_ring))
    per = value_a.shape[1] // LANES * TILE // chips
    scanned = scan_states(core, pieces, per)
    carried = exchange(scanned, "sp_0")
    held = hand_on(*held)
    blocks += held
    held = (lax.ppermute(held[0], "tp", up_ring), lax.ppermute(held[1], "tp", down_ring))
    carried_other = lax.ppermute(carried, "sp_1", swap)
    partial = mix_project(
        core, qa, qb, loc, carried, carried_other, pay_other, dec, out_weight_a, out_weight_b
    )
    arrived = exchange(partial.reshape(tp, rows_dev, width), "tp")
    ids = (route_group[:, None] * EXP_GROUP + route_expert).reshape(1, routes)
    hidden, outgoing = dispatch(arrived, residual, norm_gain, ids, sp_count)
    received = exchange(outgoing, SP)
    held = hand_on(*held)
    blocks += held
    blocks.append(lax.ppermute(held[0], "tp", up_ring))
    received_other = lax.ppermute(received, "grp", partner)
    mine, send = experts(received, received_other, blocks)
    arrived_sums = lax.ppermute(send, "grp", partner)
    back = finish(mine, arrived_sums, sp_count)
    returned = exchange(back, SP)
    return combine(returned, hidden, norm_gain, ids, route_weight.reshape(1, routes))


def solution(mesh):
    sp = mesh.shape["sp"]
    finer = Mesh(
        mesh.devices.reshape(mesh.shape["grp"], sp // 2, 2, mesh.shape["tp"]),
        ("grp", "sp_0", "sp_1", "tp"),
    )
    in_specs = (
        P(GRP_SP, "tp"),
        P(GRP_SP, "tp"),
        P(GRP_SP, "tp"),
        P(None, "tp", GRP_SP),
        P(GRP_SP, "tp"),
        P(GRP_SP, "tp"),
        P(GRP_SP, "tp"),
        P(None, "tp", GRP_SP),
        P("tp", None),
        P("tp", None),
        P(GRP_SP_TP, None),
        P(),
        P(GRP_SP_TP),
        P(GRP_SP_TP, None),
        P(GRP_SP_TP, None),
        P(SP, None, "tp"),
        P(SP, None, "tp"),
        P(SP, "tp", None),
    )
    out_specs = P(GRP_SP_TP, None)

    return jax.shard_map(
        shards, mesh=finer, in_specs=in_specs, out_specs=out_specs, check_vma=False
    )
```

```python
import math

import jax
import jax.numpy as jnp
import numpy as np
from jax import lax
from jax.experimental import pallas as pl
from jax.experimental.pallas import tpu as pltpu
from jax.sharding import Mesh
from jax.sharding import PartitionSpec as P


CAP = 2
TOP = 2
EXP_GROUP = 8
SP = ("sp_0", "sp_1")
GRP_SP = ("grp", "sp_0", "sp_1")
GRP_SP_TP = ("grp", "sp_0", "sp_1", "tp")

RESIDUAL_SCALE = math.sqrt(2.0)
NORM_EPS = 1e-05
GROUP_EPS = 1e-06
ROPE_BASE = 10000.0

F32 = jnp.float32
BF16 = jnp.bfloat16
HIGHEST = lax.Precision.HIGHEST
INTERPRET = False

LANES = 128
TILE = 16
SIDE = 8


def vmem(count):
    return [pl.BlockSpec(memory_space=pltpu.VMEM)] * count


def near(array):
    return array if INTERPRET else pltpu.with_memory_space_constraint(array, pltpu.VMEM)


def far(array):
    return array if INTERPRET else pltpu.with_memory_space_constraint(array, pltpu.HBM)


def near_shape(shape, dtype):
    return jax.ShapeDtypeStruct(shape, dtype) if INTERPRET else pltpu.VMEM(shape, dtype)


def far_shape(shape, dtype):
    return jax.ShapeDtypeStruct(shape, dtype) if INTERPRET else pltpu.HBM(shape, dtype)


SMEM_SPEC = pl.BlockSpec(memory_space=pltpu.SMEM)
PARAMS = pltpu.CompilerParams(vmem_limit_bytes=20 << 20)
ANY_SPEC = pl.BlockSpec(memory_space=pl.ANY)


def iota(shape, dim):
    return lax.broadcasted_iota(jnp.int32, shape, dim)


def mm(a, b):
    return jnp.dot(a, b, preferred_element_type=F32)


def mm_nt(a, b, precision=None):
    return lax.dot_general(
        a, b, (((1,), (1,)), ((), ())), precision=precision, preferred_element_type=F32
    )


def split2(x):
    hi = x.astype(BF16).astype(F32)
    return hi, x - hi


def angle_tables(length, half_a, half_b, devices):
    def freqs(half):
        f = np.float32(ROPE_BASE) ** (-np.arange(half, dtype=np.float32) / np.float32(half))
        return f.astype(np.float64)

    fa = freqs(half_a)
    fb = np.tile(freqs(half_b), LANES // half_b)
    inside = np.arange(length, dtype=np.float64)[:, None]
    first = (np.arange(devices, dtype=np.float64) * length)[:, None]
    local = np.stack(
        [np.cos(inside * fa), np.sin(inside * fa), np.cos(inside * fb), np.sin(inside * fb)]
    ).astype(np.float32)
    base = np.zeros((devices, 8, LANES), np.float32)
    for k, row in enumerate(
        [np.cos(first * fa), np.sin(first * fa), np.cos(first * fb), np.sin(first * fb)]
    ):
        base[:, k, :] = row
    return local, base


def retention_body(
    index_ref, qa_ref, ka_ref, va_ref, qb_ref, kb_ref, vb_ref, da_ref, db_ref, tab_ref, base_ref,
    qa_out, qb_out, loc_out, pay_out, dec_out,
):
    n, dk = qa_ref.shape
    dv = va_ref.shape[1]
    half = dk // 2
    hb = qb_ref.shape[1] // 2
    hq = hb // 2
    row, col = iota((n, n), 0), iota((n, n), 1)
    for d in range(2):
        dec_out[3 * d : 3 * d + 1, :] = da_ref[d]
        dec_out[3 * d + 1 : 3 * d + 3, :] = db_ref[d]
    dec_out[6:8, :] = jnp.zeros((2, n), F32)
    dec = dec_out[...]
    cr = jnp.dot(dec, (row <= col).astype(F32), precision=HIGHEST, preferred_element_type=F32)
    cc = mm_nt((col <= row).astype(F32), dec, HIGHEST)
    er = cr - dec
    ec = mm_nt((col < row).astype(F32), dec, HIGHEST)
    tot = cr[:, n - 1 : n]

    def pair_weights(h):
        forward = cc[:, h : h + 1] - cr[h : h + 1, :]
        backward = er[3 + h : 4 + h, :] - ec[:, 3 + h : 4 + h]
        return jnp.exp(jnp.where(col <= row, forward, backward))

    base = base_ref[index_ref[0]]
    cos_a = tab_ref[0] * base[0:1] - tab_ref[1] * base[1:2]
    sin_a = tab_ref[1] * base[0:1] + tab_ref[0] * base[1:2]

    def rotate_a(x, scale):
        x1, x2 = x[:, :half].astype(F32), x[:, half:].astype(F32)
        out = jnp.concatenate([x1 * cos_a - x2 * sin_a, x1 * sin_a + x2 * cos_a], axis=1)
        return (out * scale).astype(BF16)

    qa = rotate_a(qa_ref[...], 1.0)
    ka = rotate_a(ka_ref[...], 1.0 / math.sqrt(dk))
    qa_out[...] = qa

    width = 2 * hb
    lane = iota((n, width), 1)
    cos_b = tab_ref[2] * base[2:3] - tab_ref[3] * base[3:4]
    sin_b = tab_ref[3] * base[2:3] + tab_ref[2] * base[3:4]
    low = (lane % hb) < hq
    sin_b = jnp.where(low, -sin_b, sin_b)
    pr, pc = iota((width, width), 0), iota((width, width), 1)
    partner = jnp.where((pc % hb) < hq, pc + hq, pc - hq)
    swap = (pr == partner).astype(BF16)

    def rotate_b(x, scale):
        return ((x.astype(F32) * cos_b + mm(x, swap) * sin_b) * scale).astype(BF16)

    qb = rotate_b(qb_ref[...], 1.0)
    kb = rotate_b(kb_ref[...], 1.0 / math.sqrt(hb))
    qb_out[...] = qb

    va, vb = va_ref[...], vb_ref[...]
    kat = ka.astype(F32).T
    kbt = kb.astype(F32).T
    top = iota((width, n), 0) < hb
    for d in range(2):
        if d == 0:
            scale = [jnp.exp(tot[h : h + 1] - cr[h : h + 1, :]) for h in range(3)]
        else:
            scale = [jnp.exp(er[3 + h : 4 + h, :]) for h in range(3)]
        state = mm((kat * scale[0]).astype(BF16), va)
        pay_out[d, :dk, :] = state.astype(BF16)
        both = mm((kbt * jnp.where(top, scale[1], scale[2])).astype(BF16), vb)
        packed = jnp.where(iota((hb, width), 1) < hb, both[:hb], both[hb:]).astype(BF16)
        for q in range(dv // LANES):
            pay_out[d, dk : dk + TILE, q * LANES : (q + 1) * LANES] = packed[
                q * TILE : (q + 1) * TILE
            ]
        rows = iota((TILE, dv), 0)
        logs = jnp.zeros((TILE, dv), F32)
        for h in range(3):
            hi, lo = split2(tot[3 * d + h : 3 * d + h + 1])
            logs = jnp.where(rows == 2 * h, hi, jnp.where(rows == 2 * h + 1, lo, logs))
        pay_out[d, dk + TILE : dk + 2 * TILE, :] = logs.astype(BF16)
    weighted = (mm_nt(qa, ka) * pair_weights(0)).astype(BF16)
    loc_out[:, :dv] = mm(weighted, va)
    acc = jnp.zeros((n, width), F32)
    for h in range(2):
        mine = (lane < hb) if h == 0 else (lane >= hb)
        q_h = jnp.where(mine, qb.astype(F32), 0.0).astype(BF16)
        v_h = jnp.where(mine, vb.astype(F32), 0.0).astype(BF16)
        acc += mm((mm_nt(q_h, kb) * pair_weights(1 + h)).astype(BF16), v_h)
    loc_out[:, dv:] = acc


def retention_local(index, qa, ka, va, qb, kb, vb, da, db, tab, base):
    n, dk = qa.shape
    dv, wb = va.shape[1], vb.shape[1]
    return pl.pallas_call(
        retention_body,
        out_shape=(
            far_shape((n, dk), BF16),
            far_shape((n, wb), BF16),
            far_shape((n, dv + wb), F32),
            near_shape((2, dk + 2 * TILE, dv), BF16),
            near_shape((8, n), F32),
        ),
        in_specs=[SMEM_SPEC] + vmem(10),
        out_specs=tuple(vmem(5)),
        interpret=INTERPRET,
        compiler_params=PARAMS,
        name="retention_local",
    )(index, *map(far, (qa, ka, va, qb, kb, vb, da, db, tab, base)))


def log_rows(ref, d, dk):
    rows = ref[d, dk + TILE : dk + 2 * TILE, :LANES].astype(F32)
    return [rows[2 * h : 2 * h + 1] + rows[2 * h + 1 : 2 * h + 2] for h in range(3)]


def pack_body(core_ref, own_ref, oth_ref, out_ref, ext_scr):
    chips = out_ref.shape[0]
    dv = own_ref.shape[2]
    dk = own_ref.shape[1] - 2 * TILE
    first = core_ref[0] == 0
    step = dk // chips
    blocks = dv // LANES // 2
    one = jnp.ones((1, LANES), F32)
    own_f, oth_f = log_rows(own_ref, 0, dk), log_rows(oth_ref, 0, dk)
    own_b, oth_b = log_rows(own_ref, 1, dk), log_rows(oth_ref, 1, dk)
    factor_own = [
        [jnp.where(first, jnp.exp(oth_f[h]), one) for h in range(3)],
        [jnp.where(first, one, jnp.exp(oth_b[h])) for h in range(3)],
    ]
    factor_oth = [
        [jnp.where(first, one, jnp.exp(own_f[h])) for h in range(3)],
        [jnp.where(first, jnp.exp(own_b[h]), one) for h in range(3)],
    ]
    lane = iota((1, LANES), 1)
    left = lane < LANES // 2
    for d in range(2):
        for q in range(blocks):
            a = slice(q * LANES, (q + 1) * LANES)
            b = slice((blocks + q) * LANES, (blocks + q + 1) * LANES)

            def mine(ref):
                return jnp.where(first, ref[d, :dk, a].astype(F32), ref[d, :dk, b].astype(F32))

            total = factor_own[d][0] * mine(own_ref) + factor_oth[d][0] * mine(oth_ref)
            at = (d * blocks + q) * step
            out_ref[:, at : at + step, :] = total.astype(BF16).reshape(chips, step, LANES)
    per = (dv // LANES) * TILE // chips
    for q in range(dv // LANES):
        part = []
        for d in range(2):
            fo = jnp.where(left, factor_own[d][1], factor_own[d][2])
            ft = jnp.where(left, factor_oth[d][1], factor_oth[d][2])
            cut = slice(q * LANES, (q + 1) * LANES)
            part.append(
                fo * own_ref[d, dk : dk + TILE, cut].astype(F32)
                + ft * oth_ref[d, dk : dk + TILE, cut].astype(F32)
            )
        part = jnp.where(first, part[0], part[1])
        for k in range(TILE // per):
            ext_scr[q * (TILE // per) + k, 0:per, :] = part[k * per : (k + 1) * per]
    quarter = lane // (LANES // 4)

    def quarters(values):
        out = values[0]
        for k in range(1, len(values)):
            out = jnp.where(quarter == k, values[k], out)
        return out

    sums_f = [x + y for x, y in zip(own_f, oth_f)]
    sums_b = [x + y for x, y in zip(own_b, oth_b)]
    lines = [
        *split2(quarters([sums_f[1], sums_f[2], sums_f[0], sums_b[0]])),
        *split2(quarters([sums_b[1], sums_b[2]])),
    ]
    for k, line in enumerate(lines):
        ext_scr[:, per + k : per + k + 1, :] = jnp.broadcast_to(line[None], (chips, 1, LANES))
    at = 2 * blocks * step
    out_ref[:, at : at + SIDE, :] = ext_scr[...].astype(BF16)


def pack_states(core, own, other, chips):
    dv = own.shape[2]
    dk = own.shape[1] - 2 * TILE
    rows = dv // LANES * (dk // chips) + SIDE
    return pl.pallas_call(
        pack_body,
        out_shape=near_shape((chips, rows, LANES), BF16),
        in_specs=[SMEM_SPEC] + vmem(2),
        out_specs=vmem(1)[0],
        scratch_shapes=[pltpu.VMEM((chips, SIDE, LANES), F32)],
        interpret=INTERPRET,
        compiler_params=PARAMS,
        name="pack_states",
    )(core, near(own), near(other))


def scan_body(per, core_ref, in_ref, out_ref):
    chips, rows, _ = in_ref.shape
    main = rows - SIDE
    side = main // 2
    first = core_ref[0] == 0
    left = iota((1, LANES), 1) < LANES // 2
    ext = [in_ref[i, main:, :].astype(F32) for i in range(chips)]
    decays = []
    for e in ext:
        one = jnp.exp(e[per : per + 1] + e[per + 1 : per + 2])
        two = jnp.exp(e[per + 2 : per + 3] + e[per + 3 : per + 4])

        def lane(line, k):
            at = k * (LANES // 4)
            return line[:, at : at + 1]

        decays.append(
            [
                lane(one, 2),
                lane(one, 3),
                jnp.where(left, lane(one, 0), lane(one, 1)),
                jnp.where(left, lane(two, 0), lane(two, 1)),
            ]
        )
    carry = jnp.zeros((side, LANES), F32)
    group = jnp.zeros((SIDE, LANES), F32)
    into = []
    for i in range(chips):
        out_ref[i, :side, :] = carry.astype(BF16)
        into.append(group)
        carry = decays[i][0] * carry + in_ref[i, :side, :].astype(F32)
        group = decays[i][2] * group + ext[i]
    carry = jnp.zeros((side, LANES), F32)
    group = jnp.zeros((SIDE, LANES), F32)
    for i in reversed(range(chips)):
        out_ref[i, side:main, :] = carry.astype(BF16)
        out_ref[i, main:, :] = jnp.where(first, into[i], group).astype(BF16)
        carry = decays[i][1] * carry + in_ref[i, side:main, :].astype(F32)
        group = decays[i][3] * group + ext[i]


def scan_states(core, pieces, per):
    def body(*refs):
        scan_body(per, *refs)

    return pl.pallas_call(
        body,
        out_shape=near_shape(pieces.shape, BF16),
        in_specs=[SMEM_SPEC] + vmem(1),
        out_specs=vmem(1)[0],
        interpret=INTERPRET,
        compiler_params=PARAMS,
        name="scan_states",
    )(core, near(pieces))


def mix_body(
    core_ref, qa_ref, qb_ref, loc_ref, own_ref, oth_ref, pay_ref, dec_ref, wa_ref, wb_ref,
    out_ref, grp_scr,
):
    n, dk = qa_ref.shape
    width = qb_ref.shape[1]
    hb = width // 2
    dv = loc_ref.shape[1] - width
    chips, rows, _ = own_ref.shape
    step = dk // chips
    blocks = dv // LANES // 2
    main = rows - SIDE
    first = core_ref[0] == 0
    row, col = iota((n, n), 0), iota((n, n), 1)
    dec = dec_ref[...]
    cc = mm_nt((col <= row).astype(F32), dec, HIGHEST)
    rc = mm_nt((col >= row).astype(F32), dec, HIGHEST)
    col_f = [jnp.exp(cc[:, h : h + 1]) for h in range(3)]
    col_b = [jnp.exp(rc[:, 3 + h : 4 + h]) for h in range(3)]
    logs = [log_rows(pay_ref, d, dk) for d in range(2)]
    qa, qb = qa_ref[...], qb_ref[...]
    lane = iota((1, LANES), 1)
    left = lane < LANES // 2
    per = (dv // LANES) * TILE // chips
    total_a = loc_ref[:, :dv]
    total_b = loc_ref[:, dv:]
    for d in range(2):
        between = jnp.logical_not(first) if d == 0 else first
        factor = jnp.where(between, jnp.exp(logs[d][0]), jnp.ones((1, LANES), F32))
        keep = jnp.where(between, 1.0, 0.0)
        parts = []
        for b in range(2 * blocks):
            at = (d * blocks + b % blocks) * step
            own = own_ref[:, at : at + step, :].astype(F32)
            oth = oth_ref[:, at : at + step, :].astype(F32)
            use_own = first if b < blocks else jnp.logical_not(first)
            carry = jnp.where(use_own, own, oth).reshape(dk, LANES)
            near = pay_ref[d, :dk, b * LANES : (b + 1) * LANES].astype(F32)
            parts.append((factor * carry + keep * near).astype(BF16))
        state = jnp.concatenate(parts, axis=1)
        scale = col_f if d == 0 else col_b
        total_a = total_a + scale[0] * mm(qa, state)
        use_own = first if d == 0 else jnp.logical_not(first)
        ext = jnp.where(
            use_own, own_ref[:, main:, :].astype(F32), oth_ref[:, main:, :].astype(F32)
        )
        for i in range(chips):
            grp_scr[i * per : (i + 1) * per, :] = ext[i, 0:per, :]
        near = jnp.concatenate(
            [
                pay_ref[d, dk : dk + TILE, q * LANES : (q + 1) * LANES].astype(F32)
                for q in range(dv // LANES)
            ],
            axis=0,
        )
        factor = jnp.where(
            between,
            jnp.exp(jnp.where(left, logs[d][1], logs[d][2])),
            jnp.ones((1, LANES), F32),
        )
        group = factor * grp_scr[...] + keep * near
        blockdiag = jnp.concatenate(
            [jnp.where(left, group, 0.0), jnp.where(left, 0.0, group)], axis=0
        ).astype(BF16)
        total_b = total_b + jnp.where(left, scale[1], scale[2]) * mm(qb, blockdiag)
    square = jnp.mean(total_a * total_a, axis=1, keepdims=True)
    mixed_a = (total_a * lax.rsqrt(square + GROUP_EPS)).astype(BF16)
    sq = total_b * total_b
    s0 = jnp.sum(jnp.where(left, sq, 0.0), axis=1, keepdims=True) / hb
    s1 = jnp.sum(jnp.where(left, 0.0, sq), axis=1, keepdims=True) / hb
    mixed_b = (total_b * lax.rsqrt(jnp.where(left, s0, s1) + GROUP_EPS)).astype(BF16)
    out_ref[...] = (mm(mixed_a, wa_ref[...]) + mm(mixed_b, wb_ref[...])).astype(BF16)


def mix_project(core, qa, qb, loc, own, other, pay, dec, wa, wb):
    hb = qb.shape[1] // 2
    return pl.pallas_call(
        mix_body,
        out_shape=near_shape((qa.shape[0], wa.shape[1]), BF16),
        in_specs=[SMEM_SPEC] + vmem(9),
        out_specs=vmem(1)[0],
        scratch_shapes=[pltpu.VMEM((hb, qb.shape[1]), F32)],
        interpret=INTERPRET,
        compiler_params=PARAMS,
        name="mix_project",
    )(core, *map(far, (qa, qb, loc)), *map(near, (own, other, pay, dec, wa, wb)))


def layer_norm(stream, gain):
    center = stream - jnp.mean(stream, axis=-1, keepdims=True)
    spread = jnp.mean(center * center, axis=-1, keepdims=True)
    return center * lax.rsqrt(spread + NORM_EPS) * gain


def slots_by_route(ids):
    routes = ids.shape[1]
    row, col = iota((routes, routes), 0), iota((routes, routes), 1)
    ids_f = ids.astype(F32)
    ids_col = jnp.sum(jnp.where(row == col, ids_f, 0.0), axis=1, keepdims=True)
    same = (ids_col == ids_f) & (row < col)
    rank = jnp.sum(jnp.where(same, 1.0, 0.0), axis=0, keepdims=True)
    slot = ids_f * CAP + jnp.minimum(rank, CAP - 1.0)
    return jnp.where((row.astype(F32) == slot) & (rank < CAP), 1.0, 0.0)


def route_rows(rows, routes):
    return iota((rows, routes), 1) // TOP == iota((rows, routes), 0)


def store_chunks(value, out_ref, scr):
    rows, width = value.shape
    cuts = width // LANES
    for k in range(cuts):
        scr[pl.ds(k, rows, stride=cuts), :] = value[:, k * LANES : (k + 1) * LANES]
    out_ref[...] = scr[...].astype(BF16).reshape(out_ref.shape)


def load_chunks(ref, rows, scr):
    cuts = scr.shape[0] // rows
    scr[...] = ref[...].reshape(scr.shape).astype(F32)
    return jnp.concatenate(
        [scr[pl.ds(k, rows, stride=cuts), :] for k in range(cuts)], axis=1
    ).astype(BF16)


def dispatch_body(arr_ref, res_ref, gain_ref, ids_ref, hid_ref, out_ref, scr):
    mix = jnp.sum(arr_ref[...].astype(F32), axis=0)
    stream = RESIDUAL_SCALE * res_ref[...].astype(F32) + mix
    hidden = layer_norm(stream, gain_ref[0:1, :]).astype(BF16)
    hid_ref[...] = hidden
    hot = slots_by_route(ids_ref[...])
    belongs = jnp.where(route_rows(hidden.shape[0], hot.shape[1]), 1.0, 0.0)
    choose = mm_nt(hot.astype(BF16), belongs.astype(BF16)).astype(BF16)
    store_chunks(mm(choose, hidden), out_ref, scr)


def dispatch(arrived, residual, gain, ids, peers):
    rows, width = residual.shape
    lines = ids.shape[1] * width // LANES
    return pl.pallas_call(
        dispatch_body,
        out_shape=(
            near_shape((rows, width), BF16),
            near_shape((peers, lines // peers, LANES), BF16),
        ),
        in_specs=vmem(4),
        out_specs=tuple(vmem(2)),
        scratch_shapes=[pltpu.VMEM((lines, LANES), F32)],
        interpret=INTERPRET,
        compiler_params=PARAMS,
        name="dispatch",
    )(near(arrived), residual, gain, ids)


def hand_on(*arrays):
    count = len(arrays)

    def body(*refs):
        del refs

    return pl.pallas_call(
        body,
        out_shape=tuple(jax.ShapeDtypeStruct(x.shape, x.dtype) for x in arrays),
        in_specs=[ANY_SPEC] * count,
        out_specs=tuple([ANY_SPEC] * count),
        input_output_aliases={k: k for k in range(count)},
        interpret=INTERPRET,
        compiler_params=PARAMS,
        name="hand_on",
    )(*map(far, arrays))


def fetch(*arrays):
    count = len(arrays)

    def body(*refs):
        sems = refs[-1]
        copies = [
            pltpu.make_async_copy(refs[k], refs[count + k], sems.at[k]) for k in range(count)
        ]
        for copy in copies:
            copy.start()
        for copy in copies:
            copy.wait()

    return pl.pallas_call(
        body,
        out_shape=tuple(near_shape(x.shape, x.dtype) for x in arrays),
        in_specs=[ANY_SPEC] * count,
        out_specs=tuple(vmem(count)),
        scratch_shapes=[pltpu.SemaphoreType.DMA((count,))],
        interpret=INTERPRET,
        compiler_params=PARAMS,
        name="fetch",
    )(*map(far, arrays))


def pack_weights_body(part_ref, gate_ref, up_ref, down_ref, out_ref):
    _, width, units = gate_ref.shape
    half = units // 2
    part = part_ref[0]
    low = part == 0
    left = iota((width, units), 1) < half
    gate = gate_ref[0].astype(F32)
    up = up_ref[0].astype(F32)
    gate = jnp.where(low, gate, pltpu.roll(gate, half, 1))
    up = jnp.where(low, pltpu.roll(up, half, 1), up)
    out_ref[:width, :] = jnp.where(left, gate, up).astype(BF16)
    rows = pl.ds(pl.multiple_of(part * half, half), half)
    for k in range(width // units):
        out_ref[width + k * half : width + (k + 1) * half, :] = down_ref[
            0, rows, k * units : (k + 1) * units
        ]


def pack_weights(part, gate, up, down):
    _, width, units = gate.shape
    return pl.pallas_call(
        pack_weights_body,
        out_shape=far_shape((width + width // 2, units), BF16),
        in_specs=[SMEM_SPEC] + vmem(3),
        out_specs=vmem(1)[0],
        interpret=INTERPRET,
        compiler_params=PARAMS,
        name="pack_weights",
    )(part, far(gate), far(up), far(down))


def expert_body(own_ref, oth_ref, *refs):
    *held, mine_ref, send_ref, x_scr, blocks, acc_ref, sems = refs
    fetched, _, units = blocks.shape
    count = len(held)
    rows = mine_ref.shape[0]
    width = mine_ref.shape[1]
    half = units // 2
    copies = [pltpu.make_async_copy(held[k], blocks.at[k], sems.at[k]) for k in range(fetched)]
    for copy in copies:
        copy.start()

    def weights(k, at, size):
        if k < fetched:
            return blocks[k, at : at + size, :]
        return held[k][at : at + size, :]

    x = jnp.concatenate(
        [load_chunks(own_ref, rows, x_scr), load_chunks(oth_ref, rows, x_scr)], axis=0
    )
    left = iota((2 * rows, units), 1) < half

    def silu(v):
        return v / (1.0 + jnp.exp(-v))

    group = 4
    for first in range(0, count, group):
        hidden = []
        for k in range(first, first + group, 2):
            for j in (k, k + 1):
                if j < fetched:
                    copies[j].wait()
            both = mm(
                x, jnp.concatenate([weights(k, 0, width), weights(k + 1, 0, width)], axis=1)
            )
            one, two = both[:, :units], both[:, units:]
            one = silu(one) * pltpu.roll(one, half, 1)
            two = silu(pltpu.roll(two, half, 1)) * two
            hidden.append(jnp.where(left, one, two).astype(BF16))
        hidden = jnp.concatenate(hidden, axis=1)
        for c in range(0, width // units, 2):
            cols = []
            for j in (c, c + 1):
                at = width + j * half
                cols.append(
                    jnp.concatenate(
                        [weights(k, at, half) for k in range(first, first + group)], axis=0
                    )
                )
            part = mm(hidden, jnp.concatenate(cols, axis=1))
            cut = slice(c * units, (c + 2) * units)
            if first == 0:
                acc_ref[:, cut] = part
            elif first < count - group:
                acc_ref[:, cut] += part
            else:
                part = acc_ref[:, cut] + part
                mine_ref[:, cut] = part[:rows]
                send_ref[:, cut] = part[rows:].astype(BF16)


def experts(own, other, blocks, late):
    depth, units = blocks[0].shape
    width = depth * 2 // 3
    lines = own.shape[0] * own.shape[1]
    rows = lines * LANES // width
    return pl.pallas_call(
        expert_body,
        out_shape=(
            near_shape((rows, width), F32),
            near_shape((rows, width), BF16),
        ),
        in_specs=vmem(2) + [ANY_SPEC] * len(blocks) + vmem(len(late)),
        out_specs=tuple(vmem(2)),
        scratch_shapes=[
            pltpu.VMEM((lines, LANES), F32),
            pltpu.VMEM((len(blocks), depth, units), BF16),
            pltpu.VMEM((2 * rows, width), F32),
            pltpu.SemaphoreType.DMA((len(blocks),)),
        ],
        interpret=INTERPRET,
        compiler_params=PARAMS,
        name="experts",
    )(near(own), near(other), *map(far, blocks), *map(near, late))


def finish_body(mine_ref, arrived_ref, out_ref, scr):
    store_chunks(mine_ref[...] + arrived_ref[...].astype(F32), out_ref, scr)


def finish(mine, arrived, peers):
    rows, width = mine.shape
    lines = rows * width // LANES
    return pl.pallas_call(
        finish_body,
        out_shape=near_shape((peers, lines // peers, LANES), BF16),
        in_specs=vmem(2),
        out_specs=vmem(1)[0],
        scratch_shapes=[pltpu.VMEM((lines, LANES), F32)],
        interpret=INTERPRET,
        compiler_params=PARAMS,
        name="finish",
    )(near(mine), near(arrived))


def combine_body(ret_ref, hid_ref, gain_ref, ids_ref, w_ref, out_ref, scr):
    hidden = hid_ref[...]
    hot = slots_by_route(ids_ref[...])
    factor = jnp.where(route_rows(hidden.shape[0], hot.shape[1]), w_ref[...], 0.0)
    weights = mm_nt(factor, hot, HIGHEST)
    returned = load_chunks(ret_ref, hot.shape[0], scr)
    hi = weights.astype(BF16)
    rest = weights - hi.astype(F32)
    mid = rest.astype(BF16)
    low = (rest - mid.astype(F32)).astype(BF16)
    ffn = mm(hi, returned) + mm(mid, returned) + mm(low, returned)
    stream = RESIDUAL_SCALE * hidden.astype(F32) + ffn
    out_ref[...] = layer_norm(stream, gain_ref[1:2, :]).astype(BF16)


def combine(returned, hidden, gain, ids, weights):
    lines = returned.shape[0] * returned.shape[1]
    return pl.pallas_call(
        combine_body,
        out_shape=jax.ShapeDtypeStruct(hidden.shape, BF16),
        in_specs=vmem(5),
        out_specs=vmem(1)[0],
        scratch_shapes=[pltpu.VMEM((lines, LANES), F32)],
        interpret=INTERPRET,
        compiler_params=PARAMS,
        name="combine",
    )(near(returned), near(hidden), gain, ids, weights)


def exchange(array, axis):
    return lax.all_to_all(array, axis, split_axis=0, concat_axis=0, tiled=True)


def shards(
    query_a, key_a, value_a, decay_a, query_b, key_b, value_b, decay_b, out_weight_a,
    out_weight_b, residual, norm_gain, route_group, route_expert, route_weight, expert_gate,
    expert_up, expert_down,
):
    length = query_a.shape[0]
    chips = lax.axis_size("sp_0")
    sp_count = lax.axis_size(SP)
    tp = lax.axis_size("tp")
    rows_dev, width = residual.shape
    routes = rows_dev * TOP
    part = (lax.axis_index("grp") % 2).astype(jnp.int32).reshape(1)
    partner = [(k, k ^ 1) for k in range(lax.axis_size("grp"))]
    up_ring = [(k, (k + 1) % tp) for k in range(tp)]
    down_ring = [(k, (k - 1) % tp) for k in range(tp)]

    core = lax.axis_index("sp_1").astype(jnp.int32).reshape(1)
    local, base = angle_tables(
        length, query_a.shape[1] // 2, query_b.shape[1] // 4, sp_count
    )
    index = lax.axis_index(SP).astype(jnp.int32).reshape(1)
    qa, qb, loc, pay, dec = retention_local(
        index, query_a, key_a, value_a, query_b, key_b, value_b, decay_a, decay_b,
        jnp.asarray(local), jnp.asarray(base),
    )
    swap = [(0, 1), (1, 0)]
    pay_other = lax.ppermute(pay, "sp_1", swap)
    packed = pack_weights(part, expert_gate, expert_up, expert_down)
    blocks = [packed]

    def start(array, ring):
        return lax.ppermute(array, "tp", ring)

    def arrive(array):
        held = hand_on(array)[0]
        blocks.append(held)
        return held

    above = start(packed, up_ring)
    outgoing_states = pack_states(core, pay, pay_other, chips)
    pieces = exchange(outgoing_states, "sp_0")
    below = start(packed, down_ring)
    above = start(arrive(above), up_ring)
    per = value_a.shape[1] // LANES * TILE // chips
    scanned = scan_states(core, pieces, per)
    carried = exchange(scanned, "sp_0")
    below = start(arrive(below), down_ring)
    above = start(arrive(above), up_ring)
    out_a, out_b = fetch(out_weight_a, out_weight_b)
    carried_other = lax.ppermute(carried, "sp_1", swap)
    partial = mix_project(
        core, qa, qb, loc, carried, carried_other, pay_other, dec, out_a, out_b
    )
    arrived = exchange(partial.reshape(tp, rows_dev, width), "tp")
    ids = (route_group[:, None] * EXP_GROUP + route_expert).reshape(1, routes)
    hidden, outgoing = dispatch(arrived, residual, norm_gain, ids, sp_count)
    received = exchange(outgoing, SP)
    above = start(arrive(above), up_ring)
    below = start(arrive(below), down_ring)
    received_other = lax.ppermute(received, "grp", partner)
    mine, send = experts(received, received_other, blocks, [above, below])
    arrived_sums = lax.ppermute(send, "grp", partner)
    back = finish(mine, arrived_sums, sp_count)
    returned = exchange(back, SP)
    return combine(returned, hidden, norm_gain, ids, route_weight.reshape(1, routes))


def solution(mesh):
    sp = mesh.shape["sp"]
    finer = Mesh(
        mesh.devices.reshape(mesh.shape["grp"], sp // 2, 2, mesh.shape["tp"]),
        ("grp", "sp_0", "sp_1", "tp"),
    )
    in_specs = (
        P(GRP_SP, "tp"),
        P(GRP_SP, "tp"),
        P(GRP_SP, "tp"),
        P(None, "tp", GRP_SP),
        P(GRP_SP, "tp"),
        P(GRP_SP, "tp"),
        P(GRP_SP, "tp"),
        P(None, "tp", GRP_SP),
        P("tp", None),
        P("tp", None),
        P(GRP_SP_TP, None),
        P(),
        P(GRP_SP_TP),
        P(GRP_SP_TP, None),
        P(GRP_SP_TP, None),
        P(SP, None, "tp"),
        P(SP, None, "tp"),
        P(SP, "tp", None),
    )
    out_specs = P(GRP_SP_TP, None)

    return jax.shard_map(
        shards, mesh=finer, in_specs=in_specs, out_specs=out_specs, check_vma=False
    )
```

```python
import math

import jax
import jax.numpy as jnp
import numpy as np
from jax import lax
from jax.experimental import pallas as pl
from jax.experimental.pallas import tpu as pltpu
from jax.sharding import Mesh
from jax.sharding import PartitionSpec as P


CAP = 2
TOP = 2
EXP_GROUP = 8
SP = ("sp_0", "sp_1")
GRP_SP = ("grp", "sp_0", "sp_1")
GRP_SP_TP = ("grp", "sp_0", "sp_1", "tp")

RESIDUAL_SCALE = math.sqrt(2.0)
NORM_EPS = 1e-05
GROUP_EPS = 1e-06
ROPE_BASE = 10000.0

F32 = jnp.float32
BF16 = jnp.bfloat16
HIGHEST = lax.Precision.HIGHEST
INTERPRET = False

LANES = 128
TILE = 16
SIDE = 8


def vmem(count):
    return [pl.BlockSpec(memory_space=pltpu.VMEM)] * count


def near(array):
    return array if INTERPRET else pltpu.with_memory_space_constraint(array, pltpu.VMEM)


def far(array):
    return array if INTERPRET else pltpu.with_memory_space_constraint(array, pltpu.HBM)


def near_shape(shape, dtype):
    return jax.ShapeDtypeStruct(shape, dtype) if INTERPRET else pltpu.VMEM(shape, dtype)


SMEM_SPEC = pl.BlockSpec(memory_space=pltpu.SMEM)
PARAMS = pltpu.CompilerParams(vmem_limit_bytes=20 << 20)
ANY_SPEC = pl.BlockSpec(memory_space=pl.ANY)


def iota(shape, dim):
    return lax.broadcasted_iota(jnp.int32, shape, dim)


def mm(a, b):
    return jnp.dot(a, b, preferred_element_type=F32)


def mm_nt(a, b, precision=None):
    return lax.dot_general(
        a, b, (((1,), (1,)), ((), ())), precision=precision, preferred_element_type=F32
    )


def split2(x):
    hi = x.astype(BF16).astype(F32)
    return hi, x - hi


def angle_tables(length, half_a, half_b, devices):
    def freqs(half):
        f = np.float32(ROPE_BASE) ** (-np.arange(half, dtype=np.float32) / np.float32(half))
        return f.astype(np.float64)

    fa = freqs(half_a)
    fb = np.tile(freqs(half_b), LANES // half_b)
    inside = np.arange(length, dtype=np.float64)[:, None]
    first = (np.arange(devices, dtype=np.float64) * length)[:, None]
    local = np.stack(
        [np.cos(inside * fa), np.sin(inside * fa), np.cos(inside * fb), np.sin(inside * fb)]
    ).astype(np.float32)
    base = np.zeros((devices, 8, LANES), np.float32)
    for k, row in enumerate(
        [np.cos(first * fa), np.sin(first * fa), np.cos(first * fb), np.sin(first * fb)]
    ):
        base[:, k, :] = row
    return local, base


def retention_body(
    index_ref, qa_ref, ka_ref, va_ref, qb_ref, kb_ref, vb_ref, da_ref, db_ref, tab_ref, base_ref,
    qa_out, qb_out, loc_out, pay_out, dec_out,
):
    n, dk = qa_ref.shape
    dv = va_ref.shape[1]
    half = dk // 2
    hb = qb_ref.shape[1] // 2
    hq = hb // 2
    row, col = iota((n, n), 0), iota((n, n), 1)
    for d in range(2):
        dec_out[3 * d : 3 * d + 1, :] = da_ref[d]
        dec_out[3 * d + 1 : 3 * d + 3, :] = db_ref[d]
    dec_out[6:8, :] = jnp.zeros((2, n), F32)
    dec = dec_out[...]
    cr = jnp.dot(dec, (row <= col).astype(F32), precision=HIGHEST, preferred_element_type=F32)
    cc = mm_nt((col <= row).astype(F32), dec, HIGHEST)
    er = cr - dec
    ec = mm_nt((col < row).astype(F32), dec, HIGHEST)
    tot = cr[:, n - 1 : n]

    def pair_weights(h):
        forward = cc[:, h : h + 1] - cr[h : h + 1, :]
        backward = er[3 + h : 4 + h, :] - ec[:, 3 + h : 4 + h]
        return jnp.exp(jnp.where(col <= row, forward, backward))

    base = base_ref[index_ref[0]]
    cos_a = tab_ref[0] * base[0:1] - tab_ref[1] * base[1:2]
    sin_a = tab_ref[1] * base[0:1] + tab_ref[0] * base[1:2]

    def rotate_a(x, scale):
        x1, x2 = x[:, :half].astype(F32), x[:, half:].astype(F32)
        out = jnp.concatenate([x1 * cos_a - x2 * sin_a, x1 * sin_a + x2 * cos_a], axis=1)
        return (out * scale).astype(BF16)

    qa = rotate_a(qa_ref[...], 1.0)
    ka = rotate_a(ka_ref[...], 1.0 / math.sqrt(dk))
    qa_out[...] = qa

    width = 2 * hb
    lane = iota((n, width), 1)
    cos_b = tab_ref[2] * base[2:3] - tab_ref[3] * base[3:4]
    sin_b = tab_ref[3] * base[2:3] + tab_ref[2] * base[3:4]
    low = (lane % hb) < hq
    sin_b = jnp.where(low, -sin_b, sin_b)
    pr, pc = iota((width, width), 0), iota((width, width), 1)
    partner = jnp.where((pc % hb) < hq, pc + hq, pc - hq)
    swap = (pr == partner).astype(BF16)

    def rotate_b(x, scale):
        return ((x.astype(F32) * cos_b + mm(x, swap) * sin_b) * scale).astype(BF16)

    qb = rotate_b(qb_ref[...], 1.0)
    kb = rotate_b(kb_ref[...], 1.0 / math.sqrt(hb))
    qb_out[...] = qb

    va, vb = va_ref[...], vb_ref[...]
    kat = ka.astype(F32).T
    kbt = kb.astype(F32).T
    top = iota((width, n), 0) < hb
    for d in range(2):
        if d == 0:
            scale = [jnp.exp(tot[h : h + 1] - cr[h : h + 1, :]) for h in range(3)]
        else:
            scale = [jnp.exp(er[3 + h : 4 + h, :]) for h in range(3)]
        state = mm((kat * scale[0]).astype(BF16), va)
        pay_out[d, :dk, :] = state.astype(BF16)
        both = mm((kbt * jnp.where(top, scale[1], scale[2])).astype(BF16), vb)
        packed = jnp.where(iota((hb, width), 1) < hb, both[:hb], both[hb:]).astype(BF16)
        for q in range(dv // LANES):
            pay_out[d, dk : dk + TILE, q * LANES : (q + 1) * LANES] = packed[
                q * TILE : (q + 1) * TILE
            ]
        rows = iota((TILE, dv), 0)
        logs = jnp.zeros((TILE, dv), F32)
        for h in range(3):
            hi, lo = split2(tot[3 * d + h : 3 * d + h + 1])
            logs = jnp.where(rows == 2 * h, hi, jnp.where(rows == 2 * h + 1, lo, logs))
        pay_out[d, dk + TILE : dk + 2 * TILE, :] = logs.astype(BF16)
    weighted = (mm_nt(qa, ka) * pair_weights(0)).astype(BF16)
    loc_out[:, :dv] = mm(weighted, va)
    acc = jnp.zeros((n, width), F32)
    for h in range(2):
        mine = (lane < hb) if h == 0 else (lane >= hb)
        q_h = jnp.where(mine, qb.astype(F32), 0.0).astype(BF16)
        v_h = jnp.where(mine, vb.astype(F32), 0.0).astype(BF16)
        acc += mm((mm_nt(q_h, kb) * pair_weights(1 + h)).astype(BF16), v_h)
    loc_out[:, dv:] = acc


def retention_local(index, qa, ka, va, qb, kb, vb, da, db, tab, base):
    n, dk = qa.shape
    dv, wb = va.shape[1], vb.shape[1]
    return pl.pallas_call(
        retention_body,
        out_shape=(
            near_shape((n, dk), BF16),
            near_shape((n, wb), BF16),
            near_shape((n, dv + wb), F32),
            near_shape((2, dk + 2 * TILE, dv), BF16),
            near_shape((8, n), F32),
        ),
        in_specs=[SMEM_SPEC] + vmem(10),
        out_specs=tuple(vmem(5)),
        interpret=INTERPRET,
        compiler_params=PARAMS,
        name="retention_local",
    )(index, *map(far, (qa, ka, va, qb, kb, vb, da, db, tab, base)))


def log_rows(ref, d, dk):
    rows = ref[d, dk + TILE : dk + 2 * TILE, :LANES].astype(F32)
    return [rows[2 * h : 2 * h + 1] + rows[2 * h + 1 : 2 * h + 2] for h in range(3)]


def pack_body(core_ref, own_ref, oth_ref, out_ref, ext_scr):
    chips = out_ref.shape[0]
    dv = own_ref.shape[2]
    dk = own_ref.shape[1] - 2 * TILE
    first = core_ref[0] == 0
    step = dk // chips
    blocks = dv // LANES // 2
    one = jnp.ones((1, LANES), F32)
    own_f, oth_f = log_rows(own_ref, 0, dk), log_rows(oth_ref, 0, dk)
    own_b, oth_b = log_rows(own_ref, 1, dk), log_rows(oth_ref, 1, dk)
    factor_own = [
        [jnp.where(first, jnp.exp(oth_f[h]), one) for h in range(3)],
        [jnp.where(first, one, jnp.exp(oth_b[h])) for h in range(3)],
    ]
    factor_oth = [
        [jnp.where(first, one, jnp.exp(own_f[h])) for h in range(3)],
        [jnp.where(first, jnp.exp(own_b[h]), one) for h in range(3)],
    ]
    lane = iota((1, LANES), 1)
    left = lane < LANES // 2
    for d in range(2):
        for q in range(blocks):
            a = slice(q * LANES, (q + 1) * LANES)
            b = slice((blocks + q) * LANES, (blocks + q + 1) * LANES)

            def mine(ref):
                return jnp.where(first, ref[d, :dk, a].astype(F32), ref[d, :dk, b].astype(F32))

            total = factor_own[d][0] * mine(own_ref) + factor_oth[d][0] * mine(oth_ref)
            at = (d * blocks + q) * step
            out_ref[:, at : at + step, :] = total.astype(BF16).reshape(chips, step, LANES)
    per = (dv // LANES) * TILE // chips
    for q in range(dv // LANES):
        part = []
        for d in range(2):
            fo = jnp.where(left, factor_own[d][1], factor_own[d][2])
            ft = jnp.where(left, factor_oth[d][1], factor_oth[d][2])
            cut = slice(q * LANES, (q + 1) * LANES)
            part.append(
                fo * own_ref[d, dk : dk + TILE, cut].astype(F32)
                + ft * oth_ref[d, dk : dk + TILE, cut].astype(F32)
            )
        part = jnp.where(first, part[0], part[1])
        for k in range(TILE // per):
            ext_scr[q * (TILE // per) + k, 0:per, :] = part[k * per : (k + 1) * per]
    quarter = lane // (LANES // 4)

    def quarters(values):
        out = values[0]
        for k in range(1, len(values)):
            out = jnp.where(quarter == k, values[k], out)
        return out

    sums_f = [x + y for x, y in zip(own_f, oth_f)]
    sums_b = [x + y for x, y in zip(own_b, oth_b)]
    lines = [
        *split2(quarters([sums_f[1], sums_f[2], sums_f[0], sums_b[0]])),
        *split2(quarters([sums_b[1], sums_b[2]])),
    ]
    for k, line in enumerate(lines):
        ext_scr[:, per + k : per + k + 1, :] = jnp.broadcast_to(line[None], (chips, 1, LANES))
    at = 2 * blocks * step
    out_ref[:, at : at + SIDE, :] = ext_scr[...].astype(BF16)


def pack_states(core, own, other, chips):
    dv = own.shape[2]
    dk = own.shape[1] - 2 * TILE
    rows = dv // LANES * (dk // chips) + SIDE
    return pl.pallas_call(
        pack_body,
        out_shape=near_shape((chips, rows, LANES), BF16),
        in_specs=[SMEM_SPEC] + vmem(2),
        out_specs=vmem(1)[0],
        scratch_shapes=[pltpu.VMEM((chips, SIDE, LANES), F32)],
        interpret=INTERPRET,
        compiler_params=PARAMS,
        name="pack_states",
    )(core, near(own), near(other))


def scan_body(per, core_ref, in_ref, out_ref):
    chips, rows, _ = in_ref.shape
    main = rows - SIDE
    side = main // 2
    first = core_ref[0] == 0
    left = iota((1, LANES), 1) < LANES // 2
    ext = [in_ref[i, main:, :].astype(F32) for i in range(chips)]
    decays = []
    for e in ext:
        one = jnp.exp(e[per : per + 1] + e[per + 1 : per + 2])
        two = jnp.exp(e[per + 2 : per + 3] + e[per + 3 : per + 4])

        def lane(line, k):
            at = k * (LANES // 4)
            return line[:, at : at + 1]

        decays.append(
            [
                lane(one, 2),
                lane(one, 3),
                jnp.where(left, lane(one, 0), lane(one, 1)),
                jnp.where(left, lane(two, 0), lane(two, 1)),
            ]
        )
    carry = jnp.zeros((side, LANES), F32)
    group = jnp.zeros((SIDE, LANES), F32)
    into = []
    for i in range(chips):
        out_ref[i, :side, :] = carry.astype(BF16)
        into.append(group)
        carry = decays[i][0] * carry + in_ref[i, :side, :].astype(F32)
        group = decays[i][2] * group + ext[i]
    carry = jnp.zeros((side, LANES), F32)
    group = jnp.zeros((SIDE, LANES), F32)
    for i in reversed(range(chips)):
        out_ref[i, side:main, :] = carry.astype(BF16)
        out_ref[i, main:, :] = jnp.where(first, into[i], group).astype(BF16)
        carry = decays[i][1] * carry + in_ref[i, side:main, :].astype(F32)
        group = decays[i][3] * group + ext[i]


def scan_states(core, pieces, per):
    def body(*refs):
        scan_body(per, *refs)

    return pl.pallas_call(
        body,
        out_shape=near_shape(pieces.shape, BF16),
        in_specs=[SMEM_SPEC] + vmem(1),
        out_specs=vmem(1)[0],
        interpret=INTERPRET,
        compiler_params=PARAMS,
        name="scan_states",
    )(core, near(pieces))


def mix_body(
    core_ref, qa_ref, qb_ref, loc_ref, own_ref, oth_ref, pay_ref, dec_ref, wa_ref, wb_ref,
    out_ref, grp_scr,
):
    n, dk = qa_ref.shape
    width = qb_ref.shape[1]
    hb = width // 2
    dv = loc_ref.shape[1] - width
    chips, rows, _ = own_ref.shape
    step = dk // chips
    blocks = dv // LANES // 2
    main = rows - SIDE
    first = core_ref[0] == 0
    row, col = iota((n, n), 0), iota((n, n), 1)
    dec = dec_ref[...]
    cc = mm_nt((col <= row).astype(F32), dec, HIGHEST)
    rc = mm_nt((col >= row).astype(F32), dec, HIGHEST)
    col_f = [jnp.exp(cc[:, h : h + 1]) for h in range(3)]
    col_b = [jnp.exp(rc[:, 3 + h : 4 + h]) for h in range(3)]
    logs = [log_rows(pay_ref, d, dk) for d in range(2)]
    qa, qb = qa_ref[...], qb_ref[...]
    lane = iota((1, LANES), 1)
    left = lane < LANES // 2
    per = (dv // LANES) * TILE // chips
    total_a = loc_ref[:, :dv]
    total_b = loc_ref[:, dv:]
    for d in range(2):
        between = jnp.logical_not(first) if d == 0 else first
        factor = jnp.where(between, jnp.exp(logs[d][0]), jnp.ones((1, LANES), F32))
        keep = jnp.where(between, 1.0, 0.0)
        parts = []
        for b in range(2 * blocks):
            at = (d * blocks + b % blocks) * step
            own = own_ref[:, at : at + step, :].astype(F32)
            oth = oth_ref[:, at : at + step, :].astype(F32)
            use_own = first if b < blocks else jnp.logical_not(first)
            carry = jnp.where(use_own, own, oth).reshape(dk, LANES)
            near = pay_ref[d, :dk, b * LANES : (b + 1) * LANES].astype(F32)
            parts.append((factor * carry + keep * near).astype(BF16))
        state = jnp.concatenate(parts, axis=1)
        scale = col_f if d == 0 else col_b
        total_a = total_a + scale[0] * mm(qa, state)
        use_own = first if d == 0 else jnp.logical_not(first)
        ext = jnp.where(
            use_own, own_ref[:, main:, :].astype(F32), oth_ref[:, main:, :].astype(F32)
        )
        for i in range(chips):
            grp_scr[i * per : (i + 1) * per, :] = ext[i, 0:per, :]
        near = jnp.concatenate(
            [
                pay_ref[d, dk : dk + TILE, q * LANES : (q + 1) * LANES].astype(F32)
                for q in range(dv // LANES)
            ],
            axis=0,
        )
        factor = jnp.where(
            between,
            jnp.exp(jnp.where(left, logs[d][1], logs[d][2])),
            jnp.ones((1, LANES), F32),
        )
        group = factor * grp_scr[...] + keep * near
        blockdiag = jnp.concatenate(
            [jnp.where(left, group, 0.0), jnp.where(left, 0.0, group)], axis=0
        ).astype(BF16)
        total_b = total_b + jnp.where(left, scale[1], scale[2]) * mm(qb, blockdiag)
    square = jnp.mean(total_a * total_a, axis=1, keepdims=True)
    mixed_a = (total_a * lax.rsqrt(square + GROUP_EPS)).astype(BF16)
    sq = total_b * total_b
    s0 = jnp.sum(jnp.where(left, sq, 0.0), axis=1, keepdims=True) / hb
    s1 = jnp.sum(jnp.where(left, 0.0, sq), axis=1, keepdims=True) / hb
    mixed_b = (total_b * lax.rsqrt(jnp.where(left, s0, s1) + GROUP_EPS)).astype(BF16)
    out_ref[...] = (mm(mixed_a, wa_ref[...]) + mm(mixed_b, wb_ref[...])).astype(BF16)


def mix_project(core, qa, qb, loc, own, other, pay, dec, wa, wb):
    hb = qb.shape[1] // 2
    return pl.pallas_call(
        mix_body,
        out_shape=near_shape((qa.shape[0], wa.shape[1]), BF16),
        in_specs=[SMEM_SPEC] + vmem(9),
        out_specs=vmem(1)[0],
        scratch_shapes=[pltpu.VMEM((hb, qb.shape[1]), F32)],
        interpret=INTERPRET,
        compiler_params=PARAMS,
        name="mix_project",
    )(core, *map(near, (qa, qb, loc, own, other, pay, dec, wa, wb)))


def layer_norm(stream, gain):
    center = stream - jnp.mean(stream, axis=-1, keepdims=True)
    spread = jnp.mean(center * center, axis=-1, keepdims=True)
    return center * lax.rsqrt(spread + NORM_EPS) * gain


def slots_by_route(ids):
    routes = ids.shape[1]
    row, col = iota((routes, routes), 0), iota((routes, routes), 1)
    ids_f = ids.astype(F32)
    ids_col = jnp.sum(jnp.where(row == col, ids_f, 0.0), axis=1, keepdims=True)
    same = (ids_col == ids_f) & (row < col)
    rank = jnp.sum(jnp.where(same, 1.0, 0.0), axis=0, keepdims=True)
    slot = ids_f * CAP + jnp.minimum(rank, CAP - 1.0)
    return jnp.where((row.astype(F32) == slot) & (rank < CAP), 1.0, 0.0)


def route_rows(rows, routes):
    return iota((rows, routes), 1) // TOP == iota((rows, routes), 0)


def store_chunks(value, out_ref, scr):
    rows, width = value.shape
    cuts = width // LANES
    for k in range(cuts):
        scr[pl.ds(k, rows, stride=cuts), :] = value[:, k * LANES : (k + 1) * LANES]
    out_ref[...] = scr[...].astype(BF16).reshape(out_ref.shape)


def load_chunks(ref, rows, scr):
    cuts = scr.shape[0] // rows
    scr[...] = ref[...].reshape(scr.shape).astype(F32)
    return jnp.concatenate(
        [scr[pl.ds(k, rows, stride=cuts), :] for k in range(cuts)], axis=1
    ).astype(BF16)


def dispatch_body(arr_ref, res_ref, gain_ref, ids_ref, hid_ref, out_ref, scr):
    mix = jnp.sum(arr_ref[...].astype(F32), axis=0)
    stream = RESIDUAL_SCALE * res_ref[...].astype(F32) + mix
    hidden = layer_norm(stream, gain_ref[0:1, :]).astype(BF16)
    hid_ref[...] = hidden
    hot = slots_by_route(ids_ref[...])
    belongs = jnp.where(route_rows(hidden.shape[0], hot.shape[1]), 1.0, 0.0)
    choose = mm_nt(hot.astype(BF16), belongs.astype(BF16)).astype(BF16)
    store_chunks(mm(choose, hidden), out_ref, scr)


def dispatch(arrived, residual, gain, ids, peers):
    rows, width = residual.shape
    lines = ids.shape[1] * width // LANES
    return pl.pallas_call(
        dispatch_body,
        out_shape=(
            near_shape((rows, width), BF16),
            near_shape((peers, lines // peers, LANES), BF16),
        ),
        in_specs=vmem(4),
        out_specs=tuple(vmem(2)),
        scratch_shapes=[pltpu.VMEM((lines, LANES), F32)],
        interpret=INTERPRET,
        compiler_params=PARAMS,
        name="dispatch",
    )(near(arrived), residual, gain, ids)


def hand_on(*arrays):
    count = len(arrays)

    def body(*refs):
        del refs

    return pl.pallas_call(
        body,
        out_shape=tuple(jax.ShapeDtypeStruct(x.shape, x.dtype) for x in arrays),
        in_specs=[ANY_SPEC] * count,
        out_specs=tuple([ANY_SPEC] * count),
        input_output_aliases={k: k for k in range(count)},
        interpret=INTERPRET,
        compiler_params=PARAMS,
        name="hand_on",
    )(*map(far, arrays))


def fetch(*arrays):
    count = len(arrays)

    def body(*refs):
        sems = refs[-1]
        copies = [
            pltpu.make_async_copy(refs[k], refs[count + k], sems.at[k]) for k in range(count)
        ]
        for copy in copies:
            copy.start()
        for copy in copies:
            copy.wait()

    return pl.pallas_call(
        body,
        out_shape=tuple(near_shape(x.shape, x.dtype) for x in arrays),
        in_specs=[ANY_SPEC] * count,
        out_specs=tuple(vmem(count)),
        scratch_shapes=[pltpu.SemaphoreType.DMA((count,))],
        interpret=INTERPRET,
        compiler_params=PARAMS,
        name="fetch",
    )(*map(far, arrays))


def pack_weights_body(part_ref, gate_ref, up_ref, down_ref, out_ref):
    _, width, units = gate_ref.shape
    half = units // 2
    part = part_ref[0]
    low = part == 0
    left = iota((width, units), 1) < half
    gate = gate_ref[0].astype(F32)
    up = up_ref[0].astype(F32)
    gate = jnp.where(low, gate, pltpu.roll(gate, half, 1))
    up = jnp.where(low, pltpu.roll(up, half, 1), up)
    out_ref[:width, :] = jnp.where(left, gate, up).astype(BF16)
    rows = pl.ds(pl.multiple_of(part * half, half), half)
    for k in range(width // units):
        out_ref[width + k * half : width + (k + 1) * half, :] = down_ref[
            0, rows, k * units : (k + 1) * units
        ]


def pack_weights(part, gate, up, down):
    _, width, units = gate.shape
    return pl.pallas_call(
        pack_weights_body,
        out_shape=jax.ShapeDtypeStruct((width + width // 2, units), BF16),
        in_specs=[SMEM_SPEC] + vmem(3),
        out_specs=vmem(1)[0],
        interpret=INTERPRET,
        compiler_params=PARAMS,
        name="pack_weights",
    )(part, far(gate), far(up), far(down))


def expert_body(own_ref, oth_ref, *refs):
    *held, mine_ref, send_ref, x_scr, blocks, acc_ref, sems = refs
    fetched, _, units = blocks.shape
    count = len(held)
    rows = mine_ref.shape[0]
    width = mine_ref.shape[1]
    half = units // 2
    copies = [pltpu.make_async_copy(held[k], blocks.at[k], sems.at[k]) for k in range(fetched)]
    for copy in copies:
        copy.start()

    def weights(k, at, size):
        if k < fetched:
            return blocks[k, at : at + size, :]
        return held[k][at : at + size, :]

    x = jnp.concatenate(
        [load_chunks(own_ref, rows, x_scr), load_chunks(oth_ref, rows, x_scr)], axis=0
    )
    left = iota((2 * rows, units), 1) < half

    def silu(v):
        return v / (1.0 + jnp.exp(-v))

    group = 4
    for first in range(0, count, group):
        hidden = []
        for k in range(first, first + group, 2):
            for j in (k, k + 1):
                if j < fetched:
                    copies[j].wait()
            both = mm(
                x, jnp.concatenate([weights(k, 0, width), weights(k + 1, 0, width)], axis=1)
            )
            one, two = both[:, :units], both[:, units:]
            one = silu(one) * pltpu.roll(one, half, 1)
            two = silu(pltpu.roll(two, half, 1)) * two
            hidden.append(jnp.where(left, one, two).astype(BF16))
        hidden = jnp.concatenate(hidden, axis=1)
        for c in range(0, width // units, 2):
            cols = []
            for j in (c, c + 1):
                at = width + j * half
                cols.append(
                    jnp.concatenate(
                        [weights(k, at, half) for k in range(first, first + group)], axis=0
                    )
                )
            part = mm(hidden, jnp.concatenate(cols, axis=1))
            cut = slice(c * units, (c + 2) * units)
            if first == 0:
                acc_ref[:, cut] = part
            elif first < count - group:
                acc_ref[:, cut] += part
            else:
                part = acc_ref[:, cut] + part
                mine_ref[:, cut] = part[:rows]
                send_ref[:, cut] = part[rows:].astype(BF16)


def experts(own, other, blocks, late):
    depth, units = blocks[0].shape
    width = depth * 2 // 3
    lines = own.shape[0] * own.shape[1]
    rows = lines * LANES // width
    return pl.pallas_call(
        expert_body,
        out_shape=(
            near_shape((rows, width), F32),
            near_shape((rows, width), BF16),
        ),
        in_specs=vmem(2) + [ANY_SPEC] * len(blocks) + vmem(len(late)),
        out_specs=tuple(vmem(2)),
        scratch_shapes=[
            pltpu.VMEM((lines, LANES), F32),
            pltpu.VMEM((len(blocks), depth, units), BF16),
            pltpu.VMEM((2 * rows, width), F32),
            pltpu.SemaphoreType.DMA((len(blocks),)),
        ],
        interpret=INTERPRET,
        compiler_params=PARAMS,
        name="experts",
    )(near(own), near(other), *map(far, blocks), *map(near, late))


def finish_body(mine_ref, arrived_ref, out_ref, scr):
    store_chunks(mine_ref[...] + arrived_ref[...].astype(F32), out_ref, scr)


def finish(mine, arrived, peers):
    rows, width = mine.shape
    lines = rows * width // LANES
    return pl.pallas_call(
        finish_body,
        out_shape=near_shape((peers, lines // peers, LANES), BF16),
        in_specs=vmem(2),
        out_specs=vmem(1)[0],
        scratch_shapes=[pltpu.VMEM((lines, LANES), F32)],
        interpret=INTERPRET,
        compiler_params=PARAMS,
        name="finish",
    )(near(mine), near(arrived))


def combine_body(ret_ref, hid_ref, gain_ref, ids_ref, w_ref, out_ref, scr):
    hidden = hid_ref[...]
    hot = slots_by_route(ids_ref[...])
    factor = jnp.where(route_rows(hidden.shape[0], hot.shape[1]), w_ref[...], 0.0)
    weights = mm_nt(factor, hot, HIGHEST)
    returned = load_chunks(ret_ref, hot.shape[0], scr)
    hi = weights.astype(BF16)
    rest = weights - hi.astype(F32)
    mid = rest.astype(BF16)
    low = (rest - mid.astype(F32)).astype(BF16)
    ffn = mm(hi, returned) + mm(mid, returned) + mm(low, returned)
    stream = RESIDUAL_SCALE * hidden.astype(F32) + ffn
    out_ref[...] = layer_norm(stream, gain_ref[1:2, :]).astype(BF16)


def combine(returned, hidden, gain, ids, weights):
    lines = returned.shape[0] * returned.shape[1]
    return pl.pallas_call(
        combine_body,
        out_shape=jax.ShapeDtypeStruct(hidden.shape, BF16),
        in_specs=vmem(5),
        out_specs=vmem(1)[0],
        scratch_shapes=[pltpu.VMEM((lines, LANES), F32)],
        interpret=INTERPRET,
        compiler_params=PARAMS,
        name="combine",
    )(near(returned), near(hidden), gain, ids, weights)


def exchange(array, axis):
    return lax.all_to_all(array, axis, split_axis=0, concat_axis=0, tiled=True)


def shards(
    query_a, key_a, value_a, decay_a, query_b, key_b, value_b, decay_b, out_weight_a,
    out_weight_b, residual, norm_gain, route_group, route_expert, route_weight, expert_gate,
    expert_up, expert_down,
):
    length = query_a.shape[0]
    chips = lax.axis_size("sp_0")
    sp_count = lax.axis_size(SP)
    tp = lax.axis_size("tp")
    rows_dev, width = residual.shape
    routes = rows_dev * TOP
    part = (lax.axis_index("grp") % 2).astype(jnp.int32).reshape(1)
    partner = [(k, k ^ 1) for k in range(lax.axis_size("grp"))]
    up_ring = [(k, (k + 1) % tp) for k in range(tp)]
    down_ring = [(k, (k - 1) % tp) for k in range(tp)]

    core = lax.axis_index("sp_1").astype(jnp.int32).reshape(1)
    local, base = angle_tables(
        length, query_a.shape[1] // 2, query_b.shape[1] // 4, sp_count
    )
    index = lax.axis_index(SP).astype(jnp.int32).reshape(1)
    qa, qb, loc, pay, dec = retention_local(
        index, query_a, key_a, value_a, query_b, key_b, value_b, decay_a, decay_b,
        jnp.asarray(local), jnp.asarray(base),
    )
    swap = [(0, 1), (1, 0)]
    pay_other = lax.ppermute(pay, "sp_1", swap)
    packed = pack_weights(part, expert_gate, expert_up, expert_down)
    blocks = [packed]

    def start(array, ring):
        return lax.ppermute(array, "tp", ring)

    def arrive(array):
        held = hand_on(array)[0]
        blocks.append(held)
        return held

    above = start(packed, up_ring)
    outgoing_states = pack_states(core, pay, pay_other, chips)
    pieces = exchange(outgoing_states, "sp_0")
    below = start(packed, down_ring)
    above = start(arrive(above), up_ring)
    per = value_a.shape[1] // LANES * TILE // chips
    scanned = scan_states(core, pieces, per)
    carried = exchange(scanned, "sp_0")
    below = start(arrive(below), down_ring)
    above = start(arrive(above), up_ring)
    out_a, out_b = fetch(out_weight_a, out_weight_b)
    carried_other = lax.ppermute(carried, "sp_1", swap)
    partial = mix_project(
        core, qa, qb, loc, carried, carried_other, pay_other, dec, out_a, out_b
    )
    arrived = exchange(partial.reshape(tp, rows_dev, width), "tp")
    ids = (route_group[:, None] * EXP_GROUP + route_expert).reshape(1, routes)
    hidden, outgoing = dispatch(arrived, residual, norm_gain, ids, sp_count)
    received = exchange(outgoing, SP)
    above = start(arrive(above), up_ring)
    below = start(arrive(below), down_ring)
    received_other = lax.ppermute(received, "grp", partner)
    mine, send = experts(received, received_other, blocks, [above, below])
    arrived_sums = lax.ppermute(send, "grp", partner)
    back = finish(mine, arrived_sums, sp_count)
    returned = exchange(back, SP)
    return combine(returned, hidden, norm_gain, ids, route_weight.reshape(1, routes))


def solution(mesh):
    sp = mesh.shape["sp"]
    finer = Mesh(
        mesh.devices.reshape(mesh.shape["grp"], sp // 2, 2, mesh.shape["tp"]),
        ("grp", "sp_0", "sp_1", "tp"),
    )
    in_specs = (
        P(GRP_SP, "tp"),
        P(GRP_SP, "tp"),
        P(GRP_SP, "tp"),
        P(None, "tp", GRP_SP),
        P(GRP_SP, "tp"),
        P(GRP_SP, "tp"),
        P(GRP_SP, "tp"),
        P(None, "tp", GRP_SP),
        P("tp", None),
        P("tp", None),
        P(GRP_SP_TP, None),
        P(),
        P(GRP_SP_TP),
        P(GRP_SP_TP, None),
        P(GRP_SP_TP, None),
        P(SP, None, "tp"),
        P(SP, None, "tp"),
        P(SP, "tp", None),
    )
    out_specs = P(GRP_SP_TP, None)

    return jax.shard_map(
        shards, mesh=finer, in_specs=in_specs, out_specs=out_specs, check_vma=False
    )
```

```python
import math

import jax
import jax.numpy as jnp
import numpy as np
from jax import lax
from jax.experimental import pallas as pl
from jax.experimental.pallas import tpu as pltpu
from jax.sharding import Mesh
from jax.sharding import PartitionSpec as P


CAP = 2
TOP = 2
EXP_GROUP = 8
SP = ("sp_0", "sp_1")
GRP_SP = ("grp", "sp_0", "sp_1")
GRP_SP_TP = ("grp", "sp_0", "sp_1", "tp")

RESIDUAL_SCALE = math.sqrt(2.0)
NORM_EPS = 1e-05
GROUP_EPS = 1e-06
ROPE_BASE = 10000.0

F32 = jnp.float32
BF16 = jnp.bfloat16
HIGHEST = lax.Precision.HIGHEST
INTERPRET = False

LANES = 128
TILE = 16
SIDE = 8


def vmem(count):
    return [pl.BlockSpec(memory_space=pltpu.VMEM)] * count


def near(array):
    return array if INTERPRET else pltpu.with_memory_space_constraint(array, pltpu.VMEM)


def far(array):
    return array if INTERPRET else pltpu.with_memory_space_constraint(array, pltpu.HBM)


def near_shape(shape, dtype):
    return jax.ShapeDtypeStruct(shape, dtype) if INTERPRET else pltpu.VMEM(shape, dtype)


SMEM_SPEC = pl.BlockSpec(memory_space=pltpu.SMEM)
PARAMS = pltpu.CompilerParams(vmem_limit_bytes=20 << 20)
ANY_SPEC = pl.BlockSpec(memory_space=pl.ANY)


def iota(shape, dim):
    return lax.broadcasted_iota(jnp.int32, shape, dim)


def mm(a, b):
    return jnp.dot(a, b, preferred_element_type=F32)


def mm_nt(a, b, precision=None):
    return lax.dot_general(
        a, b, (((1,), (1,)), ((), ())), precision=precision, preferred_element_type=F32
    )


def split2(x):
    hi = x.astype(BF16).astype(F32)
    return hi, x - hi


def angle_tables(length, half_a, half_b, devices):
    def freqs(half):
        f = np.float32(ROPE_BASE) ** (-np.arange(half, dtype=np.float32) / np.float32(half))
        return f.astype(np.float64)

    fa = freqs(half_a)
    fb = np.tile(freqs(half_b), LANES // half_b)
    inside = np.arange(length, dtype=np.float64)[:, None]
    first = (np.arange(devices, dtype=np.float64) * length)[:, None]
    local = np.stack(
        [np.cos(inside * fa), np.sin(inside * fa), np.cos(inside * fb), np.sin(inside * fb)]
    ).astype(np.float32)
    base = np.zeros((devices, 8, LANES), np.float32)
    for k, row in enumerate(
        [np.cos(first * fa), np.sin(first * fa), np.cos(first * fb), np.sin(first * fb)]
    ):
        base[:, k, :] = row
    return local, base


def retention_body(
    index_ref, qa_ref, ka_ref, va_ref, qb_ref, kb_ref, vb_ref, da_ref, db_ref, tab_ref, base_ref,
    qa_out, ka_out, qb_out, kb_out, pay_out, dec_out,
):
    n, dk = qa_ref.shape
    dv = va_ref.shape[1]
    half = dk // 2
    hb = qb_ref.shape[1] // 2
    hq = hb // 2
    row, col = iota((n, n), 0), iota((n, n), 1)
    for d in range(2):
        dec_out[3 * d : 3 * d + 1, :] = da_ref[d]
        dec_out[3 * d + 1 : 3 * d + 3, :] = db_ref[d]
    dec_out[6:8, :] = jnp.zeros((2, n), F32)
    dec = dec_out[...]
    cr = jnp.dot(dec, (row <= col).astype(F32), precision=HIGHEST, preferred_element_type=F32)
    er = cr - dec
    tot = cr[:, n - 1 : n]

    base = base_ref[index_ref[0]]
    cos_a = tab_ref[0] * base[0:1] - tab_ref[1] * base[1:2]
    sin_a = tab_ref[1] * base[0:1] + tab_ref[0] * base[1:2]

    def rotate_a(x, scale):
        x1, x2 = x[:, :half].astype(F32), x[:, half:].astype(F32)
        out = jnp.concatenate([x1 * cos_a - x2 * sin_a, x1 * sin_a + x2 * cos_a], axis=1)
        return (out * scale).astype(BF16)

    qa = rotate_a(qa_ref[...], 1.0)
    ka = rotate_a(ka_ref[...], 1.0 / math.sqrt(dk))
    qa_out[...] = qa
    ka_out[...] = ka

    width = 2 * hb
    lane = iota((n, width), 1)
    cos_b = tab_ref[2] * base[2:3] - tab_ref[3] * base[3:4]
    sin_b = tab_ref[3] * base[2:3] + tab_ref[2] * base[3:4]
    low = (lane % hb) < hq
    sin_b = jnp.where(low, -sin_b, sin_b)
    pr, pc = iota((width, width), 0), iota((width, width), 1)
    partner = jnp.where((pc % hb) < hq, pc + hq, pc - hq)
    swap = (pr == partner).astype(BF16)

    def rotate_b(x, scale):
        return ((x.astype(F32) * cos_b + mm(x, swap) * sin_b) * scale).astype(BF16)

    qb = rotate_b(qb_ref[...], 1.0)
    kb = rotate_b(kb_ref[...], 1.0 / math.sqrt(hb))
    qb_out[...] = qb
    kb_out[...] = kb

    va, vb = va_ref[...], vb_ref[...]
    kat = ka.astype(F32).T
    kbt = kb.astype(F32).T
    top = iota((width, n), 0) < hb
    for d in range(2):
        if d == 0:
            scale = [jnp.exp(tot[h : h + 1] - cr[h : h + 1, :]) for h in range(3)]
        else:
            scale = [jnp.exp(er[3 + h : 4 + h, :]) for h in range(3)]
        state = mm((kat * scale[0]).astype(BF16), va)
        pay_out[d, :dk, :] = state.astype(BF16)
        both = mm((kbt * jnp.where(top, scale[1], scale[2])).astype(BF16), vb)
        packed = jnp.where(iota((hb, width), 1) < hb, both[:hb], both[hb:]).astype(BF16)
        for q in range(dv // LANES):
            pay_out[d, dk : dk + TILE, q * LANES : (q + 1) * LANES] = packed[
                q * TILE : (q + 1) * TILE
            ]
        rows = iota((TILE, dv), 0)
        logs = jnp.zeros((TILE, dv), F32)
        for h in range(3):
            hi, lo = split2(tot[3 * d + h : 3 * d + h + 1])
            logs = jnp.where(rows == 2 * h, hi, jnp.where(rows == 2 * h + 1, lo, logs))
        pay_out[d, dk + TILE : dk + 2 * TILE, :] = logs.astype(BF16)


def pairs_body(qa_ref, ka_ref, va_ref, qb_ref, kb_ref, vb_ref, dec_ref, loc_out):
    n = qa_ref.shape[0]
    dv = va_ref.shape[1]
    width = qb_ref.shape[1]
    hb = width // 2
    row, col = iota((n, n), 0), iota((n, n), 1)
    dec = dec_ref[...]
    cr = jnp.dot(dec, (row <= col).astype(F32), precision=HIGHEST, preferred_element_type=F32)
    cc = mm_nt((col <= row).astype(F32), dec, HIGHEST)
    er = cr - dec
    ec = mm_nt((col < row).astype(F32), dec, HIGHEST)

    def pair_weights(h):
        forward = cc[:, h : h + 1] - cr[h : h + 1, :]
        backward = er[3 + h : 4 + h, :] - ec[:, 3 + h : 4 + h]
        return jnp.exp(jnp.where(col <= row, forward, backward))

    weighted = (mm_nt(qa_ref[...], ka_ref[...]) * pair_weights(0)).astype(BF16)
    loc_out[:, :dv] = mm(weighted, va_ref[...])
    qb, kb, vb = qb_ref[...], kb_ref[...], vb_ref[...]
    lane = iota((n, width), 1)
    acc = jnp.zeros((n, width), F32)
    for h in range(2):
        mine = (lane < hb) if h == 0 else (lane >= hb)
        q_h = jnp.where(mine, qb.astype(F32), 0.0).astype(BF16)
        v_h = jnp.where(mine, vb.astype(F32), 0.0).astype(BF16)
        acc += mm((mm_nt(q_h, kb) * pair_weights(1 + h)).astype(BF16), v_h)
    loc_out[:, dv:] = acc


def retention_pairs(qa, ka, va, qb, kb, vb, dec):
    return pl.pallas_call(
        pairs_body,
        out_shape=near_shape((qa.shape[0], va.shape[1] + vb.shape[1]), F32),
        in_specs=vmem(7),
        out_specs=vmem(1)[0],
        interpret=INTERPRET,
        compiler_params=PARAMS,
        name="retention_pairs",
    )(near(qa), near(ka), far(va), near(qb), near(kb), far(vb), near(dec))


def retention_state(index, qa, ka, va, qb, kb, vb, da, db, tab, base):
    n, dk = qa.shape
    dv, wb = va.shape[1], vb.shape[1]
    return pl.pallas_call(
        retention_body,
        out_shape=(
            near_shape((n, dk), BF16),
            near_shape((n, dk), BF16),
            near_shape((n, wb), BF16),
            near_shape((n, wb), BF16),
            near_shape((2, dk + 2 * TILE, dv), BF16),
            near_shape((8, n), F32),
        ),
        in_specs=[SMEM_SPEC] + vmem(10),
        out_specs=tuple(vmem(6)),
        interpret=INTERPRET,
        compiler_params=PARAMS,
        name="retention_state",
    )(index, *map(far, (qa, ka, va, qb, kb, vb, da, db, tab, base)))


def log_rows(ref, d, dk):
    rows = ref[d, dk + TILE : dk + 2 * TILE, :LANES].astype(F32)
    return [rows[2 * h : 2 * h + 1] + rows[2 * h + 1 : 2 * h + 2] for h in range(3)]


def pack_body(core_ref, own_ref, oth_ref, out_ref, ext_scr):
    chips = out_ref.shape[0]
    dv = own_ref.shape[2]
    dk = own_ref.shape[1] - 2 * TILE
    first = core_ref[0] == 0
    step = dk // chips
    blocks = dv // LANES // 2
    one = jnp.ones((1, LANES), F32)
    own_f, oth_f = log_rows(own_ref, 0, dk), log_rows(oth_ref, 0, dk)
    own_b, oth_b = log_rows(own_ref, 1, dk), log_rows(oth_ref, 1, dk)
    factor_own = [
        [jnp.where(first, jnp.exp(oth_f[h]), one) for h in range(3)],
        [jnp.where(first, one, jnp.exp(oth_b[h])) for h in range(3)],
    ]
    factor_oth = [
        [jnp.where(first, one, jnp.exp(own_f[h])) for h in range(3)],
        [jnp.where(first, jnp.exp(own_b[h]), one) for h in range(3)],
    ]
    lane = iota((1, LANES), 1)
    left = lane < LANES // 2
    for d in range(2):
        for q in range(blocks):
            a = slice(q * LANES, (q + 1) * LANES)
            b = slice((blocks + q) * LANES, (blocks + q + 1) * LANES)

            def mine(ref):
                return jnp.where(first, ref[d, :dk, a].astype(F32), ref[d, :dk, b].astype(F32))

            total = factor_own[d][0] * mine(own_ref) + factor_oth[d][0] * mine(oth_ref)
            at = (d * blocks + q) * step
            out_ref[:, at : at + step, :] = total.astype(BF16).reshape(chips, step, LANES)
    per = (dv // LANES) * TILE // chips
    for q in range(dv // LANES):
        part = []
        for d in range(2):
            fo = jnp.where(left, factor_own[d][1], factor_own[d][2])
            ft = jnp.where(left, factor_oth[d][1], factor_oth[d][2])
            cut = slice(q * LANES, (q + 1) * LANES)
            part.append(
                fo * own_ref[d, dk : dk + TILE, cut].astype(F32)
                + ft * oth_ref[d, dk : dk + TILE, cut].astype(F32)
            )
        part = jnp.where(first, part[0], part[1])
        for k in range(TILE // per):
            ext_scr[q * (TILE // per) + k, 0:per, :] = part[k * per : (k + 1) * per]
    quarter = lane // (LANES // 4)

    def quarters(values):
        out = values[0]
        for k in range(1, len(values)):
            out = jnp.where(quarter == k, values[k], out)
        return out

    sums_f = [x + y for x, y in zip(own_f, oth_f)]
    sums_b = [x + y for x, y in zip(own_b, oth_b)]
    lines = [
        *split2(quarters([sums_f[1], sums_f[2], sums_f[0], sums_b[0]])),
        *split2(quarters([sums_b[1], sums_b[2]])),
    ]
    for k, line in enumerate(lines):
        ext_scr[:, per + k : per + k + 1, :] = jnp.broadcast_to(line[None], (chips, 1, LANES))
    at = 2 * blocks * step
    out_ref[:, at : at + SIDE, :] = ext_scr[...].astype(BF16)


def pack_states(core, own, other, chips):
    dv = own.shape[2]
    dk = own.shape[1] - 2 * TILE
    rows = dv // LANES * (dk // chips) + SIDE
    return pl.pallas_call(
        pack_body,
        out_shape=near_shape((chips, rows, LANES), BF16),
        in_specs=[SMEM_SPEC] + vmem(2),
        out_specs=vmem(1)[0],
        scratch_shapes=[pltpu.VMEM((chips, SIDE, LANES), F32)],
        interpret=INTERPRET,
        compiler_params=PARAMS,
        name="pack_states",
    )(core, near(own), near(other))


def scan_body(per, core_ref, in_ref, out_ref):
    chips, rows, _ = in_ref.shape
    main = rows - SIDE
    side = main // 2
    first = core_ref[0] == 0
    left = iota((1, LANES), 1) < LANES // 2
    ext = [in_ref[i, main:, :].astype(F32) for i in range(chips)]
    decays = []
    for e in ext:
        one = jnp.exp(e[per : per + 1] + e[per + 1 : per + 2])
        two = jnp.exp(e[per + 2 : per + 3] + e[per + 3 : per + 4])

        def lane(line, k):
            at = k * (LANES // 4)
            return line[:, at : at + 1]

        decays.append(
            [
                lane(one, 2),
                lane(one, 3),
                jnp.where(left, lane(one, 0), lane(one, 1)),
                jnp.where(left, lane(two, 0), lane(two, 1)),
            ]
        )
    carry = jnp.zeros((side, LANES), F32)
    group = jnp.zeros((SIDE, LANES), F32)
    into = []
    for i in range(chips):
        out_ref[i, :side, :] = carry.astype(BF16)
        into.append(group)
        carry = decays[i][0] * carry + in_ref[i, :side, :].astype(F32)
        group = decays[i][2] * group + ext[i]
    carry = jnp.zeros((side, LANES), F32)
    group = jnp.zeros((SIDE, LANES), F32)
    for i in reversed(range(chips)):
        out_ref[i, side:main, :] = carry.astype(BF16)
        out_ref[i, main:, :] = jnp.where(first, into[i], group).astype(BF16)
        carry = decays[i][1] * carry + in_ref[i, side:main, :].astype(F32)
        group = decays[i][3] * group + ext[i]


def scan_states(core, pieces, per):
    def body(*refs):
        scan_body(per, *refs)

    return pl.pallas_call(
        body,
        out_shape=near_shape(pieces.shape, BF16),
        in_specs=[SMEM_SPEC] + vmem(1),
        out_specs=vmem(1)[0],
        interpret=INTERPRET,
        compiler_params=PARAMS,
        name="scan_states",
    )(core, near(pieces))


def mix_body(
    core_ref, qa_ref, qb_ref, loc_ref, own_ref, oth_ref, pay_ref, dec_ref, wa_ref, wb_ref,
    out_ref, grp_scr,
):
    n, dk = qa_ref.shape
    width = qb_ref.shape[1]
    hb = width // 2
    dv = loc_ref.shape[1] - width
    chips, rows, _ = own_ref.shape
    step = dk // chips
    blocks = dv // LANES // 2
    main = rows - SIDE
    first = core_ref[0] == 0
    row, col = iota((n, n), 0), iota((n, n), 1)
    dec = dec_ref[...]
    cc = mm_nt((col <= row).astype(F32), dec, HIGHEST)
    rc = mm_nt((col >= row).astype(F32), dec, HIGHEST)
    col_f = [jnp.exp(cc[:, h : h + 1]) for h in range(3)]
    col_b = [jnp.exp(rc[:, 3 + h : 4 + h]) for h in range(3)]
    logs = [log_rows(pay_ref, d, dk) for d in range(2)]
    qa, qb = qa_ref[...], qb_ref[...]
    lane = iota((1, LANES), 1)
    left = lane < LANES // 2
    per = (dv // LANES) * TILE // chips
    total_a = loc_ref[:, :dv]
    total_b = loc_ref[:, dv:]
    for d in range(2):
        between = jnp.logical_not(first) if d == 0 else first
        factor = jnp.where(between, jnp.exp(logs[d][0]), jnp.ones((1, LANES), F32))
        keep = jnp.where(between, 1.0, 0.0)
        parts = []
        for b in range(2 * blocks):
            at = (d * blocks + b % blocks) * step
            own = own_ref[:, at : at + step, :].astype(F32)
            oth = oth_ref[:, at : at + step, :].astype(F32)
            use_own = first if b < blocks else jnp.logical_not(first)
            carry = jnp.where(use_own, own, oth).reshape(dk, LANES)
            near = pay_ref[d, :dk, b * LANES : (b + 1) * LANES].astype(F32)
            parts.append((factor * carry + keep * near).astype(BF16))
        state = jnp.concatenate(parts, axis=1)
        scale = col_f if d == 0 else col_b
        total_a = total_a + scale[0] * mm(qa, state)
        use_own = first if d == 0 else jnp.logical_not(first)
        ext = jnp.where(
            use_own, own_ref[:, main:, :].astype(F32), oth_ref[:, main:, :].astype(F32)
        )
        for i in range(chips):
            grp_scr[i * per : (i + 1) * per, :] = ext[i, 0:per, :]
        near = jnp.concatenate(
            [
                pay_ref[d, dk : dk + TILE, q * LANES : (q + 1) * LANES].astype(F32)
                for q in range(dv // LANES)
            ],
            axis=0,
        )
        factor = jnp.where(
            between,
            jnp.exp(jnp.where(left, logs[d][1], logs[d][2])),
            jnp.ones((1, LANES), F32),
        )
        group = factor * grp_scr[...] + keep * near
        blockdiag = jnp.concatenate(
            [jnp.where(left, group, 0.0), jnp.where(left, 0.0, group)], axis=0
        ).astype(BF16)
        total_b = total_b + jnp.where(left, scale[1], scale[2]) * mm(qb, blockdiag)
    square = jnp.mean(total_a * total_a, axis=1, keepdims=True)
    mixed_a = (total_a * lax.rsqrt(square + GROUP_EPS)).astype(BF16)
    sq = total_b * total_b
    s0 = jnp.sum(jnp.where(left, sq, 0.0), axis=1, keepdims=True) / hb
    s1 = jnp.sum(jnp.where(left, 0.0, sq), axis=1, keepdims=True) / hb
    mixed_b = (total_b * lax.rsqrt(jnp.where(left, s0, s1) + GROUP_EPS)).astype(BF16)
    out_ref[...] = (mm(mixed_a, wa_ref[...]) + mm(mixed_b, wb_ref[...])).astype(BF16)


def mix_project(core, qa, qb, loc, own, other, pay, dec, wa, wb):
    hb = qb.shape[1] // 2
    return pl.pallas_call(
        mix_body,
        out_shape=near_shape((qa.shape[0], wa.shape[1]), BF16),
        in_specs=[SMEM_SPEC] + vmem(9),
        out_specs=vmem(1)[0],
        scratch_shapes=[pltpu.VMEM((hb, qb.shape[1]), F32)],
        interpret=INTERPRET,
        compiler_params=PARAMS,
        name="mix_project",
    )(core, *map(near, (qa, qb, loc, own, other, pay, dec, wa, wb)))


def layer_norm(stream, gain):
    center = stream - jnp.mean(stream, axis=-1, keepdims=True)
    spread = jnp.mean(center * center, axis=-1, keepdims=True)
    return center * lax.rsqrt(spread + NORM_EPS) * gain


def slots_by_route(ids):
    routes = ids.shape[1]
    row, col = iota((routes, routes), 0), iota((routes, routes), 1)
    ids_f = ids.astype(F32)
    ids_col = jnp.sum(jnp.where(row == col, ids_f, 0.0), axis=1, keepdims=True)
    same = (ids_col == ids_f) & (row < col)
    rank = jnp.sum(jnp.where(same, 1.0, 0.0), axis=0, keepdims=True)
    slot = ids_f * CAP + jnp.minimum(rank, CAP - 1.0)
    return jnp.where((row.astype(F32) == slot) & (rank < CAP), 1.0, 0.0)


def route_rows(rows, routes):
    return iota((rows, routes), 1) // TOP == iota((rows, routes), 0)


def store_chunks(value, out_ref, scr):
    rows, width = value.shape
    cuts = width // LANES
    for k in range(cuts):
        scr[pl.ds(k, rows, stride=cuts), :] = value[:, k * LANES : (k + 1) * LANES]
    out_ref[...] = scr[...].astype(BF16).reshape(out_ref.shape)


def load_chunks(ref, rows, scr):
    cuts = scr.shape[0] // rows
    scr[...] = ref[...].reshape(scr.shape).astype(F32)
    return jnp.concatenate(
        [scr[pl.ds(k, rows, stride=cuts), :] for k in range(cuts)], axis=1
    ).astype(BF16)


def route_body(ids_ref, w_ref, choose_ref, weights_ref):
    hot = slots_by_route(ids_ref[...])
    belongs = route_rows(weights_ref.shape[0], hot.shape[1])
    choose = mm_nt(hot.astype(BF16), jnp.where(belongs, 1.0, 0.0).astype(BF16))
    choose_ref[...] = choose.astype(BF16)
    weights_ref[...] = mm_nt(jnp.where(belongs, w_ref[...], 0.0), hot, HIGHEST)


def route(ids, weights, rows):
    routes = ids.shape[1]
    return pl.pallas_call(
        route_body,
        out_shape=(near_shape((routes, rows), BF16), near_shape((rows, routes), F32)),
        in_specs=vmem(2),
        out_specs=tuple(vmem(2)),
        interpret=INTERPRET,
        compiler_params=PARAMS,
        name="route",
    )(ids, weights)


def dispatch_body(arr_ref, res_ref, gain_ref, choose_ref, hid_ref, out_ref, scr):
    mix = jnp.sum(arr_ref[...].astype(F32), axis=0)
    stream = RESIDUAL_SCALE * res_ref[...].astype(F32) + mix
    hidden = layer_norm(stream, gain_ref[0:1, :]).astype(BF16)
    hid_ref[...] = hidden
    store_chunks(mm(choose_ref[...], hidden), out_ref, scr)


def dispatch(arrived, residual, gain, choose, peers):
    rows, width = residual.shape
    lines = choose.shape[0] * width // LANES
    return pl.pallas_call(
        dispatch_body,
        out_shape=(
            near_shape((rows, width), BF16),
            near_shape((peers, lines // peers, LANES), BF16),
        ),
        in_specs=vmem(4),
        out_specs=tuple(vmem(2)),
        scratch_shapes=[pltpu.VMEM((lines, LANES), F32)],
        interpret=INTERPRET,
        compiler_params=PARAMS,
        name="dispatch",
    )(near(arrived), residual, gain, near(choose))


def hand_on(*arrays):
    count = len(arrays)

    def body(*refs):
        del refs

    return pl.pallas_call(
        body,
        out_shape=tuple(jax.ShapeDtypeStruct(x.shape, x.dtype) for x in arrays),
        in_specs=[ANY_SPEC] * count,
        out_specs=tuple([ANY_SPEC] * count),
        input_output_aliases={k: k for k in range(count)},
        interpret=INTERPRET,
        compiler_params=PARAMS,
        name="hand_on",
    )(*map(far, arrays))


def fetch(*arrays):
    count = len(arrays)

    def body(*refs):
        sems = refs[-1]
        copies = [
            pltpu.make_async_copy(refs[k], refs[count + k], sems.at[k]) for k in range(count)
        ]
        for copy in copies:
            copy.start()
        for copy in copies:
            copy.wait()

    return pl.pallas_call(
        body,
        out_shape=tuple(near_shape(x.shape, x.dtype) for x in arrays),
        in_specs=[ANY_SPEC] * count,
        out_specs=tuple(vmem(count)),
        scratch_shapes=[pltpu.SemaphoreType.DMA((count,))],
        interpret=INTERPRET,
        compiler_params=PARAMS,
        name="fetch",
    )(*map(far, arrays))


def pack_weights_body(part_ref, gate_ref, up_ref, down_ref, out_ref):
    _, width, units = gate_ref.shape
    half = units // 2
    part = part_ref[0]
    low = part == 0
    left = iota((width, units), 1) < half
    gate = gate_ref[0].astype(F32)
    up = up_ref[0].astype(F32)
    gate = jnp.where(low, gate, pltpu.roll(gate, half, 1))
    up = jnp.where(low, pltpu.roll(up, half, 1), up)
    out_ref[:width, :] = jnp.where(left, gate, up).astype(BF16)
    rows = pl.ds(pl.multiple_of(part * half, half), half)
    for k in range(width // units):
        out_ref[width + k * half : width + (k + 1) * half, :] = down_ref[
            0, rows, k * units : (k + 1) * units
        ]


def pack_weights(part, gate, up, down):
    _, width, units = gate.shape
    return pl.pallas_call(
        pack_weights_body,
        out_shape=jax.ShapeDtypeStruct((width + width // 2, units), BF16),
        in_specs=[SMEM_SPEC] + vmem(3),
        out_specs=vmem(1)[0],
        interpret=INTERPRET,
        compiler_params=PARAMS,
        name="pack_weights",
    )(part, far(gate), far(up), far(down))


def expert_body(own_ref, oth_ref, *refs):
    *held, mine_ref, send_ref, x_scr, blocks, acc_ref, sems = refs
    fetched, _, units = blocks.shape
    count = len(held)
    rows = mine_ref.shape[0]
    width = mine_ref.shape[1]
    half = units // 2
    copies = [pltpu.make_async_copy(held[k], blocks.at[k], sems.at[k]) for k in range(fetched)]
    for copy in copies:
        copy.start()

    def weights(k, at, size):
        if k < fetched:
            return blocks[k, at : at + size, :]
        return held[k][at : at + size, :]

    x = jnp.concatenate(
        [load_chunks(own_ref, rows, x_scr), load_chunks(oth_ref, rows, x_scr)], axis=0
    )
    left = iota((2 * rows, units), 1) < half

    def silu(v):
        return v / (1.0 + jnp.exp(-v))

    group = 4
    for first in range(0, count, group):
        hidden = []
        for k in range(first, first + group, 2):
            for j in (k, k + 1):
                if j < fetched:
                    copies[j].wait()
            both = mm(
                x, jnp.concatenate([weights(k, 0, width), weights(k + 1, 0, width)], axis=1)
            )
            one, two = both[:, :units], both[:, units:]
            one = silu(one) * pltpu.roll(one, half, 1)
            two = silu(pltpu.roll(two, half, 1)) * two
            hidden.append(jnp.where(left, one, two).astype(BF16))
        hidden = jnp.concatenate(hidden, axis=1)
        for c in range(0, width // units, 2):
            cols = []
            for j in (c, c + 1):
                at = width + j * half
                cols.append(
                    jnp.concatenate(
                        [weights(k, at, half) for k in range(first, first + group)], axis=0
                    )
                )
            part = mm(hidden, jnp.concatenate(cols, axis=1))
            cut = slice(c * units, (c + 2) * units)
            if first == 0:
                acc_ref[:, cut] = part
            elif first < count - group:
                acc_ref[:, cut] += part
            else:
                part = acc_ref[:, cut] + part
                mine_ref[:, cut] = part[:rows]
                send_ref[:, cut] = part[rows:].astype(BF16)


def experts(own, other, blocks, late):
    depth, units = blocks[0].shape
    width = depth * 2 // 3
    lines = own.shape[0] * own.shape[1]
    rows = lines * LANES // width
    return pl.pallas_call(
        expert_body,
        out_shape=(
            near_shape((rows, width), F32),
            near_shape((rows, width), BF16),
        ),
        in_specs=vmem(2) + [ANY_SPEC] * len(blocks) + vmem(len(late)),
        out_specs=tuple(vmem(2)),
        scratch_shapes=[
            pltpu.VMEM((lines, LANES), F32),
            pltpu.VMEM((len(blocks), depth, units), BF16),
            pltpu.VMEM((2 * rows, width), F32),
            pltpu.SemaphoreType.DMA((len(blocks),)),
        ],
        interpret=INTERPRET,
        compiler_params=PARAMS,
        name="experts",
    )(near(own), near(other), *map(far, blocks), *map(near, late))


def finish_body(mine_ref, arrived_ref, out_ref, scr):
    store_chunks(mine_ref[...] + arrived_ref[...].astype(F32), out_ref, scr)


def finish(mine, arrived, peers):
    rows, width = mine.shape
    lines = rows * width // LANES
    return pl.pallas_call(
        finish_body,
        out_shape=near_shape((peers, lines // peers, LANES), BF16),
        in_specs=vmem(2),
        out_specs=vmem(1)[0],
        scratch_shapes=[pltpu.VMEM((lines, LANES), F32)],
        interpret=INTERPRET,
        compiler_params=PARAMS,
        name="finish",
    )(near(mine), near(arrived))


def combine_body(ret_ref, hid_ref, gain_ref, w_ref, out_ref, scr):
    hidden = hid_ref[...]
    weights = w_ref[...]
    returned = load_chunks(ret_ref, weights.shape[1], scr)
    hi = weights.astype(BF16)
    rest = weights - hi.astype(F32)
    mid = rest.astype(BF16)
    low = (rest - mid.astype(F32)).astype(BF16)
    ffn = mm(hi, returned) + mm(mid, returned) + mm(low, returned)
    stream = RESIDUAL_SCALE * hidden.astype(F32) + ffn
    out_ref[...] = layer_norm(stream, gain_ref[1:2, :]).astype(BF16)


def combine(returned, hidden, gain, weights):
    lines = returned.shape[0] * returned.shape[1]
    return pl.pallas_call(
        combine_body,
        out_shape=jax.ShapeDtypeStruct(hidden.shape, BF16),
        in_specs=vmem(4),
        out_specs=vmem(1)[0],
        scratch_shapes=[pltpu.VMEM((lines, LANES), F32)],
        interpret=INTERPRET,
        compiler_params=PARAMS,
        name="combine",
    )(near(returned), near(hidden), gain, near(weights))


def exchange(array, axis):
    return lax.all_to_all(array, axis, split_axis=0, concat_axis=0, tiled=True)


def shards(
    query_a, key_a, value_a, decay_a, query_b, key_b, value_b, decay_b, out_weight_a,
    out_weight_b, residual, norm_gain, route_group, route_expert, route_weight, expert_gate,
    expert_up, expert_down,
):
    length = query_a.shape[0]
    chips = lax.axis_size("sp_0")
    sp_count = lax.axis_size(SP)
    tp = lax.axis_size("tp")
    rows_dev, width = residual.shape
    routes = rows_dev * TOP
    part = (lax.axis_index("grp") % 2).astype(jnp.int32).reshape(1)
    partner = [(k, k ^ 1) for k in range(lax.axis_size("grp"))]
    up_ring = [(k, (k + 1) % tp) for k in range(tp)]
    down_ring = [(k, (k - 1) % tp) for k in range(tp)]

    core = lax.axis_index("sp_1").astype(jnp.int32).reshape(1)
    local, base = angle_tables(
        length, query_a.shape[1] // 2, query_b.shape[1] // 4, sp_count
    )
    index = lax.axis_index(SP).astype(jnp.int32).reshape(1)
    qa, ka, qb, kb, pay, dec = retention_state(
        index, query_a, key_a, value_a, query_b, key_b, value_b, decay_a, decay_b,
        jnp.asarray(local), jnp.asarray(base),
    )
    swap = [(0, 1), (1, 0)]
    pay_other = lax.ppermute(pay, "sp_1", swap)
    packed = pack_weights(part, expert_gate, expert_up, expert_down)
    blocks = [packed]

    def start(array, ring):
        return lax.ppermute(array, "tp", ring)

    def arrive(array):
        held = hand_on(array)[0]
        blocks.append(held)
        return held

    above = start(packed, up_ring)
    outgoing_states = pack_states(core, pay, pay_other, chips)
    pieces = exchange(outgoing_states, "sp_0")
    below = start(packed, down_ring)
    above = start(arrive(above), up_ring)
    loc = retention_pairs(qa, ka, value_a, qb, kb, value_b, dec)
    per = value_a.shape[1] // LANES * TILE // chips
    scanned = scan_states(core, pieces, per)
    carried = exchange(scanned, "sp_0")
    below = start(arrive(below), down_ring)
    above = start(arrive(above), up_ring)
    out_a, out_b = fetch(out_weight_a, out_weight_b)
    carried_other = lax.ppermute(carried, "sp_1", swap)
    partial = mix_project(
        core, qa, qb, loc, carried, carried_other, pay_other, dec, out_a, out_b
    )
    arrived = exchange(partial.reshape(tp, rows_dev, width), "tp")
    ids = (route_group[:, None] * EXP_GROUP + route_expert).reshape(1, routes)
    choose, weights = route(ids, route_weight.reshape(1, routes), rows_dev)
    hidden, outgoing = dispatch(arrived, residual, norm_gain, choose, sp_count)
    received = exchange(outgoing, SP)
    above = start(arrive(above), up_ring)
    below = start(arrive(below), down_ring)
    received_other = lax.ppermute(received, "grp", partner)
    mine, send = experts(received, received_other, blocks, [above, below])
    arrived_sums = lax.ppermute(send, "grp", partner)
    back = finish(mine, arrived_sums, sp_count)
    returned = exchange(back, SP)
    return combine(returned, hidden, norm_gain, weights)


def solution(mesh):
    sp = mesh.shape["sp"]
    finer = Mesh(
        mesh.devices.reshape(mesh.shape["grp"], sp // 2, 2, mesh.shape["tp"]),
        ("grp", "sp_0", "sp_1", "tp"),
    )
    in_specs = (
        P(GRP_SP, "tp"),
        P(GRP_SP, "tp"),
        P(GRP_SP, "tp"),
        P(None, "tp", GRP_SP),
        P(GRP_SP, "tp"),
        P(GRP_SP, "tp"),
        P(GRP_SP, "tp"),
        P(None, "tp", GRP_SP),
        P("tp", None),
        P("tp", None),
        P(GRP_SP_TP, None),
        P(),
        P(GRP_SP_TP),
        P(GRP_SP_TP, None),
        P(GRP_SP_TP, None),
        P(SP, None, "tp"),
        P(SP, None, "tp"),
        P(SP, "tp", None),
    )
    out_specs = P(GRP_SP_TP, None)

    return jax.shard_map(
        shards, mesh=finer, in_specs=in_specs, out_specs=out_specs, check_vma=False
    )
```

```python
import math

import jax
import jax.numpy as jnp
import numpy as np
from jax import lax
from jax.experimental import pallas as pl
from jax.experimental.pallas import tpu as pltpu
from jax.sharding import Mesh
from jax.sharding import PartitionSpec as P


CAP = 2
TOP = 2
EXP_GROUP = 8
SP = ("sp_0", "sp_1")
GRP_SP = ("grp", "sp_0", "sp_1")
GRP_SP_TP = ("grp", "sp_0", "sp_1", "tp")

RESIDUAL_SCALE = math.sqrt(2.0)
NORM_EPS = 1e-05
GROUP_EPS = 1e-06
ROPE_BASE = 10000.0

F32 = jnp.float32
BF16 = jnp.bfloat16
HIGHEST = lax.Precision.HIGHEST
INTERPRET = False

LANES = 128
TILE = 16
SIDE = 8


def vmem(count):
    return [pl.BlockSpec(memory_space=pltpu.VMEM)] * count


def near(array):
    return array if INTERPRET else pltpu.with_memory_space_constraint(array, pltpu.VMEM)


def far(array):
    return array if INTERPRET else pltpu.with_memory_space_constraint(array, pltpu.HBM)


def near_shape(shape, dtype):
    return jax.ShapeDtypeStruct(shape, dtype) if INTERPRET else pltpu.VMEM(shape, dtype)


SMEM_SPEC = pl.BlockSpec(memory_space=pltpu.SMEM)
PARAMS = pltpu.CompilerParams(vmem_limit_bytes=20 << 20)
ANY_SPEC = pl.BlockSpec(memory_space=pl.ANY)


def iota(shape, dim):
    return lax.broadcasted_iota(jnp.int32, shape, dim)


def mm(a, b):
    return jnp.dot(a, b, preferred_element_type=F32)


def mm_nt(a, b, precision=None):
    return lax.dot_general(
        a, b, (((1,), (1,)), ((), ())), precision=precision, preferred_element_type=F32
    )


def split2(x):
    hi = x.astype(BF16).astype(F32)
    return hi, x - hi


def angle_tables(length, half_a, half_b, devices):
    def freqs(half):
        f = np.float32(ROPE_BASE) ** (-np.arange(half, dtype=np.float32) / np.float32(half))
        return f.astype(np.float64)

    fa = freqs(half_a)
    fb = np.tile(freqs(half_b), LANES // half_b)
    inside = np.arange(length, dtype=np.float64)[:, None]
    first = (np.arange(devices, dtype=np.float64) * length)[:, None]
    local = np.stack(
        [np.cos(inside * fa), np.sin(inside * fa), np.cos(inside * fb), np.sin(inside * fb)]
    ).astype(np.float32)
    base = np.zeros((devices, 8, LANES), np.float32)
    for k, row in enumerate(
        [np.cos(first * fa), np.sin(first * fa), np.cos(first * fb), np.sin(first * fb)]
    ):
        base[:, k, :] = row
    return local, base


def retention_body(
    index_ref, qa_ref, ka_ref, va_ref, qb_ref, kb_ref, vb_ref, da_ref, db_ref, tab_ref, base_ref,
    qa_out, ka_out, qb_out, kb_out, pay_out, dec_out,
):
    n, dk = qa_ref.shape
    dv = va_ref.shape[1]
    half = dk // 2
    hb = qb_ref.shape[1] // 2
    hq = hb // 2
    row, col = iota((n, n), 0), iota((n, n), 1)
    for d in range(2):
        dec_out[3 * d : 3 * d + 1, :] = da_ref[d]
        dec_out[3 * d + 1 : 3 * d + 3, :] = db_ref[d]
    dec_out[6:8, :] = jnp.zeros((2, n), F32)
    dec = dec_out[...]
    cr = jnp.dot(dec, (row <= col).astype(F32), precision=HIGHEST, preferred_element_type=F32)
    er = cr - dec
    tot = cr[:, n - 1 : n]

    base = base_ref[index_ref[0]]
    cos_a = tab_ref[0] * base[0:1] - tab_ref[1] * base[1:2]
    sin_a = tab_ref[1] * base[0:1] + tab_ref[0] * base[1:2]

    def rotate_a(x, scale):
        x1, x2 = x[:, :half].astype(F32), x[:, half:].astype(F32)
        out = jnp.concatenate([x1 * cos_a - x2 * sin_a, x1 * sin_a + x2 * cos_a], axis=1)
        return (out * scale).astype(BF16)

    qa = rotate_a(qa_ref[...], 1.0)
    ka = rotate_a(ka_ref[...], 1.0 / math.sqrt(dk))
    qa_out[...] = qa
    ka_out[...] = ka

    width = 2 * hb
    lane = iota((n, width), 1)
    cos_b = tab_ref[2] * base[2:3] - tab_ref[3] * base[3:4]
    sin_b = tab_ref[3] * base[2:3] + tab_ref[2] * base[3:4]
    low = (lane % hb) < hq
    sin_b = jnp.where(low, -sin_b, sin_b)
    pr, pc = iota((width, width), 0), iota((width, width), 1)
    partner = jnp.where((pc % hb) < hq, pc + hq, pc - hq)
    swap = (pr == partner).astype(BF16)

    def rotate_b(x, scale):
        return ((x.astype(F32) * cos_b + mm(x, swap) * sin_b) * scale).astype(BF16)

    qb = rotate_b(qb_ref[...], 1.0)
    kb = rotate_b(kb_ref[...], 1.0 / math.sqrt(hb))
    qb_out[...] = qb
    kb_out[...] = kb

    va, vb = va_ref[...], vb_ref[...]
    kat = ka.astype(F32).T
    kbt = kb.astype(F32).T
    top = iota((width, n), 0) < hb
    for d in range(2):
        if d == 0:
            scale = [jnp.exp(tot[h : h + 1] - cr[h : h + 1, :]) for h in range(3)]
        else:
            scale = [jnp.exp(er[3 + h : 4 + h, :]) for h in range(3)]
        state = mm((kat * scale[0]).astype(BF16), va)
        pay_out[d, :dk, :] = state.astype(BF16)
        both = mm((kbt * jnp.where(top, scale[1], scale[2])).astype(BF16), vb)
        packed = jnp.where(iota((hb, width), 1) < hb, both[:hb], both[hb:]).astype(BF16)
        for q in range(dv // LANES):
            pay_out[d, dk : dk + TILE, q * LANES : (q + 1) * LANES] = packed[
                q * TILE : (q + 1) * TILE
            ]
        rows = iota((TILE, dv), 0)
        logs = jnp.zeros((TILE, dv), F32)
        for h in range(3):
            hi, lo = split2(tot[3 * d + h : 3 * d + h + 1])
            logs = jnp.where(rows == 2 * h, hi, jnp.where(rows == 2 * h + 1, lo, logs))
        pay_out[d, dk + TILE : dk + 2 * TILE, :] = logs.astype(BF16)


def pairs_body(qa_ref, ka_ref, va_ref, qb_ref, kb_ref, vb_ref, dec_ref, loc_out):
    n = qa_ref.shape[0]
    dv = va_ref.shape[1]
    width = qb_ref.shape[1]
    hb = width // 2
    row, col = iota((n, n), 0), iota((n, n), 1)
    dec = dec_ref[...]
    cr = jnp.dot(dec, (row <= col).astype(F32), precision=HIGHEST, preferred_element_type=F32)
    cc = mm_nt((col <= row).astype(F32), dec, HIGHEST)
    er = cr - dec
    ec = mm_nt((col < row).astype(F32), dec, HIGHEST)

    def pair_weights(h):
        forward = cc[:, h : h + 1] - cr[h : h + 1, :]
        backward = er[3 + h : 4 + h, :] - ec[:, 3 + h : 4 + h]
        return jnp.exp(jnp.where(col <= row, forward, backward))

    weighted = (mm_nt(qa_ref[...], ka_ref[...]) * pair_weights(0)).astype(BF16)
    loc_out[:, :dv] = mm(weighted, va_ref[...])
    qb, kb, vb = qb_ref[...], kb_ref[...], vb_ref[...]
    lane = iota((n, width), 1)
    acc = jnp.zeros((n, width), F32)
    for h in range(2):
        mine = (lane < hb) if h == 0 else (lane >= hb)
        q_h = jnp.where(mine, qb.astype(F32), 0.0).astype(BF16)
        v_h = jnp.where(mine, vb.astype(F32), 0.0).astype(BF16)
        acc += mm((mm_nt(q_h, kb) * pair_weights(1 + h)).astype(BF16), v_h)
    loc_out[:, dv:] = acc


def retention_pairs(qa, ka, va, qb, kb, vb, dec):
    return pl.pallas_call(
        pairs_body,
        out_shape=near_shape((qa.shape[0], va.shape[1] + vb.shape[1]), F32),
        in_specs=vmem(7),
        out_specs=vmem(1)[0],
        interpret=INTERPRET,
        compiler_params=PARAMS,
        name="retention_pairs",
    )(near(qa), near(ka), far(va), near(qb), near(kb), far(vb), near(dec))


def retention_state(index, qa, ka, va, qb, kb, vb, da, db, tab, base):
    n, dk = qa.shape
    dv, wb = va.shape[1], vb.shape[1]
    return pl.pallas_call(
        retention_body,
        out_shape=(
            near_shape((n, dk), BF16),
            near_shape((n, dk), BF16),
            near_shape((n, wb), BF16),
            near_shape((n, wb), BF16),
            near_shape((2, dk + 2 * TILE, dv), BF16),
            near_shape((8, n), F32),
        ),
        in_specs=[SMEM_SPEC] + vmem(10),
        out_specs=tuple(vmem(6)),
        interpret=INTERPRET,
        compiler_params=PARAMS,
        name="retention_state",
    )(index, *map(far, (qa, ka, va, qb, kb, vb, da, db, tab, base)))


def log_rows(ref, d, dk):
    rows = ref[d, dk + TILE : dk + 2 * TILE, :LANES].astype(F32)
    return [rows[2 * h : 2 * h + 1] + rows[2 * h + 1 : 2 * h + 2] for h in range(3)]


def pack_body(core_ref, own_ref, oth_ref, out_ref, ext_scr):
    chips = out_ref.shape[0]
    dv = own_ref.shape[2]
    dk = own_ref.shape[1] - 2 * TILE
    first = core_ref[0] == 0
    step = dk // chips
    blocks = dv // LANES // 2
    one = jnp.ones((1, LANES), F32)
    own_f, oth_f = log_rows(own_ref, 0, dk), log_rows(oth_ref, 0, dk)
    own_b, oth_b = log_rows(own_ref, 1, dk), log_rows(oth_ref, 1, dk)
    factor_own = [
        [jnp.where(first, jnp.exp(oth_f[h]), one) for h in range(3)],
        [jnp.where(first, one, jnp.exp(oth_b[h])) for h in range(3)],
    ]
    factor_oth = [
        [jnp.where(first, one, jnp.exp(own_f[h])) for h in range(3)],
        [jnp.where(first, jnp.exp(own_b[h]), one) for h in range(3)],
    ]
    lane = iota((1, LANES), 1)
    left = lane < LANES // 2
    for d in range(2):
        for q in range(blocks):
            a = slice(q * LANES, (q + 1) * LANES)
            b = slice((blocks + q) * LANES, (blocks + q + 1) * LANES)

            def mine(ref):
                return jnp.where(first, ref[d, :dk, a].astype(F32), ref[d, :dk, b].astype(F32))

            total = factor_own[d][0] * mine(own_ref) + factor_oth[d][0] * mine(oth_ref)
            at = (d * blocks + q) * step
            out_ref[:, at : at + step, :] = total.astype(BF16).reshape(chips, step, LANES)
    per = (dv // LANES) * TILE // chips
    for q in range(dv // LANES):
        part = []
        for d in range(2):
            fo = jnp.where(left, factor_own[d][1], factor_own[d][2])
            ft = jnp.where(left, factor_oth[d][1], factor_oth[d][2])
            cut = slice(q * LANES, (q + 1) * LANES)
            part.append(
                fo * own_ref[d, dk : dk + TILE, cut].astype(F32)
                + ft * oth_ref[d, dk : dk + TILE, cut].astype(F32)
            )
        part = jnp.where(first, part[0], part[1])
        for k in range(TILE // per):
            ext_scr[q * (TILE // per) + k, 0:per, :] = part[k * per : (k + 1) * per]
    quarter = lane // (LANES // 4)

    def quarters(values):
        out = values[0]
        for k in range(1, len(values)):
            out = jnp.where(quarter == k, values[k], out)
        return out

    sums_f = [x + y for x, y in zip(own_f, oth_f)]
    sums_b = [x + y for x, y in zip(own_b, oth_b)]
    lines = [
        *split2(quarters([sums_f[1], sums_f[2], sums_f[0], sums_b[0]])),
        *split2(quarters([sums_b[1], sums_b[2]])),
    ]
    for k, line in enumerate(lines):
        ext_scr[:, per + k : per + k + 1, :] = jnp.broadcast_to(line[None], (chips, 1, LANES))
    at = 2 * blocks * step
    out_ref[:, at : at + SIDE, :] = ext_scr[...].astype(BF16)


def pack_states(core, own, other, chips):
    dv = own.shape[2]
    dk = own.shape[1] - 2 * TILE
    rows = dv // LANES * (dk // chips) + SIDE
    return pl.pallas_call(
        pack_body,
        out_shape=near_shape((chips, rows, LANES), BF16),
        in_specs=[SMEM_SPEC] + vmem(2),
        out_specs=vmem(1)[0],
        scratch_shapes=[pltpu.VMEM((chips, SIDE, LANES), F32)],
        interpret=INTERPRET,
        compiler_params=PARAMS,
        name="pack_states",
    )(core, near(own), near(other))


def scan_body(per, core_ref, in_ref, out_ref):
    chips, rows, _ = in_ref.shape
    main = rows - SIDE
    side = main // 2
    first = core_ref[0] == 0
    left = iota((1, LANES), 1) < LANES // 2
    ext = [in_ref[i, main:, :].astype(F32) for i in range(chips)]
    decays = []
    for e in ext:
        one = jnp.exp(e[per : per + 1] + e[per + 1 : per + 2])
        two = jnp.exp(e[per + 2 : per + 3] + e[per + 3 : per + 4])

        def lane(line, k):
            at = k * (LANES // 4)
            return line[:, at : at + 1]

        decays.append(
            [
                lane(one, 2),
                lane(one, 3),
                jnp.where(left, lane(one, 0), lane(one, 1)),
                jnp.where(left, lane(two, 0), lane(two, 1)),
            ]
        )
    carry = jnp.zeros((side, LANES), F32)
    group = jnp.zeros((SIDE, LANES), F32)
    into = []
    for i in range(chips):
        out_ref[i, :side, :] = carry.astype(BF16)
        into.append(group)
        carry = decays[i][0] * carry + in_ref[i, :side, :].astype(F32)
        group = decays[i][2] * group + ext[i]
    carry = jnp.zeros((side, LANES), F32)
    group = jnp.zeros((SIDE, LANES), F32)
    for i in reversed(range(chips)):
        out_ref[i, side:main, :] = carry.astype(BF16)
        out_ref[i, main:, :] = jnp.where(first, into[i], group).astype(BF16)
        carry = decays[i][1] * carry + in_ref[i, side:main, :].astype(F32)
        group = decays[i][3] * group + ext[i]


def scan_states(core, pieces, per):
    def body(*refs):
        scan_body(per, *refs)

    return pl.pallas_call(
        body,
        out_shape=near_shape(pieces.shape, BF16),
        in_specs=[SMEM_SPEC] + vmem(1),
        out_specs=vmem(1)[0],
        interpret=INTERPRET,
        compiler_params=PARAMS,
        name="scan_states",
    )(core, near(pieces))


def mix_body(
    core_ref, qa_ref, qb_ref, loc_ref, own_ref, oth_ref, pay_ref, dec_ref, wa_ref, wb_ref,
    out_ref, grp_scr,
):
    n, dk = qa_ref.shape
    width = qb_ref.shape[1]
    hb = width // 2
    dv = loc_ref.shape[1] - width
    chips, rows, _ = own_ref.shape
    step = dk // chips
    blocks = dv // LANES // 2
    main = rows - SIDE
    first = core_ref[0] == 0
    row, col = iota((n, n), 0), iota((n, n), 1)
    dec = dec_ref[...]
    cc = mm_nt((col <= row).astype(F32), dec, HIGHEST)
    rc = mm_nt((col >= row).astype(F32), dec, HIGHEST)
    col_f = [jnp.exp(cc[:, h : h + 1]) for h in range(3)]
    col_b = [jnp.exp(rc[:, 3 + h : 4 + h]) for h in range(3)]
    logs = [log_rows(pay_ref, d, dk) for d in range(2)]
    qa, qb = qa_ref[...], qb_ref[...]
    lane = iota((1, LANES), 1)
    left = lane < LANES // 2
    per = (dv // LANES) * TILE // chips
    total_a = loc_ref[:, :dv]
    total_b = loc_ref[:, dv:]
    for d in range(2):
        between = jnp.logical_not(first) if d == 0 else first
        factor = jnp.where(between, jnp.exp(logs[d][0]), jnp.ones((1, LANES), F32))
        keep = jnp.where(between, 1.0, 0.0)
        parts = []
        for b in range(2 * blocks):
            at = (d * blocks + b % blocks) * step
            own = own_ref[:, at : at + step, :].astype(F32)
            oth = oth_ref[:, at : at + step, :].astype(F32)
            use_own = first if b < blocks else jnp.logical_not(first)
            carry = jnp.where(use_own, own, oth).reshape(dk, LANES)
            near = pay_ref[d, :dk, b * LANES : (b + 1) * LANES].astype(F32)
            parts.append((factor * carry + keep * near).astype(BF16))
        state = jnp.concatenate(parts, axis=1)
        scale = col_f if d == 0 else col_b
        total_a = total_a + scale[0] * mm(qa, state)
        use_own = first if d == 0 else jnp.logical_not(first)
        ext = jnp.where(
            use_own, own_ref[:, main:, :].astype(F32), oth_ref[:, main:, :].astype(F32)
        )
        for i in range(chips):
            grp_scr[i * per : (i + 1) * per, :] = ext[i, 0:per, :]
        near = jnp.concatenate(
            [
                pay_ref[d, dk : dk + TILE, q * LANES : (q + 1) * LANES].astype(F32)
                for q in range(dv // LANES)
            ],
            axis=0,
        )
        factor = jnp.where(
            between,
            jnp.exp(jnp.where(left, logs[d][1], logs[d][2])),
            jnp.ones((1, LANES), F32),
        )
        group = factor * grp_scr[...] + keep * near
        blockdiag = jnp.concatenate(
            [jnp.where(left, group, 0.0), jnp.where(left, 0.0, group)], axis=0
        ).astype(BF16)
        total_b = total_b + jnp.where(left, scale[1], scale[2]) * mm(qb, blockdiag)
    square = jnp.mean(total_a * total_a, axis=1, keepdims=True)
    mixed_a = (total_a * lax.rsqrt(square + GROUP_EPS)).astype(BF16)
    sq = total_b * total_b
    s0 = jnp.sum(jnp.where(left, sq, 0.0), axis=1, keepdims=True) / hb
    s1 = jnp.sum(jnp.where(left, 0.0, sq), axis=1, keepdims=True) / hb
    mixed_b = (total_b * lax.rsqrt(jnp.where(left, s0, s1) + GROUP_EPS)).astype(BF16)
    out_ref[...] = (mm(mixed_a, wa_ref[...]) + mm(mixed_b, wb_ref[...])).astype(BF16)


def mix_project(core, qa, qb, loc, own, other, pay, dec, wa, wb):
    hb = qb.shape[1] // 2
    return pl.pallas_call(
        mix_body,
        out_shape=near_shape((qa.shape[0], wa.shape[1]), BF16),
        in_specs=[SMEM_SPEC] + vmem(9),
        out_specs=vmem(1)[0],
        scratch_shapes=[pltpu.VMEM((hb, qb.shape[1]), F32)],
        interpret=INTERPRET,
        compiler_params=PARAMS,
        name="mix_project",
    )(core, *map(near, (qa, qb, loc, own, other, pay, dec, wa, wb)))


def layer_norm(stream, gain):
    center = stream - jnp.mean(stream, axis=-1, keepdims=True)
    spread = jnp.mean(center * center, axis=-1, keepdims=True)
    return center * lax.rsqrt(spread + NORM_EPS) * gain


def slots_by_route(ids):
    routes = ids.shape[1]
    row, col = iota((routes, routes), 0), iota((routes, routes), 1)
    ids_f = ids.astype(F32)
    ids_col = jnp.sum(jnp.where(row == col, ids_f, 0.0), axis=1, keepdims=True)
    same = (ids_col == ids_f) & (row < col)
    rank = jnp.sum(jnp.where(same, 1.0, 0.0), axis=0, keepdims=True)
    slot = ids_f * CAP + jnp.minimum(rank, CAP - 1.0)
    return jnp.where((row.astype(F32) == slot) & (rank < CAP), 1.0, 0.0)


def route_rows(rows, routes):
    return iota((rows, routes), 1) // TOP == iota((rows, routes), 0)


def store_chunks(value, out_ref, scr):
    rows, width = value.shape
    cuts = width // LANES
    for k in range(cuts):
        scr[pl.ds(k, rows, stride=cuts), :] = value[:, k * LANES : (k + 1) * LANES]
    out_ref[...] = scr[...].astype(BF16).reshape(out_ref.shape)


def load_chunks(ref, rows, scr):
    cuts = scr.shape[0] // rows
    scr[...] = ref[...].reshape(scr.shape).astype(F32)
    return jnp.concatenate(
        [scr[pl.ds(k, rows, stride=cuts), :] for k in range(cuts)], axis=1
    ).astype(BF16)


def route_body(ids_ref, w_ref, choose_ref, weights_ref):
    hot = slots_by_route(ids_ref[...])
    belongs = route_rows(weights_ref.shape[0], hot.shape[1])
    choose = mm_nt(hot.astype(BF16), jnp.where(belongs, 1.0, 0.0).astype(BF16))
    choose_ref[...] = choose.astype(BF16)
    weights_ref[...] = mm_nt(jnp.where(belongs, w_ref[...], 0.0), hot, HIGHEST)


def route(ids, weights, rows):
    routes = ids.shape[1]
    return pl.pallas_call(
        route_body,
        out_shape=(near_shape((routes, rows), BF16), near_shape((rows, routes), F32)),
        in_specs=vmem(2),
        out_specs=tuple(vmem(2)),
        interpret=INTERPRET,
        compiler_params=PARAMS,
        name="route",
    )(ids, weights)


def dispatch_body(arr_ref, res_ref, gain_ref, choose_ref, hid_ref, out_ref, scr):
    mix = jnp.sum(arr_ref[...].astype(F32), axis=0)
    stream = RESIDUAL_SCALE * res_ref[...].astype(F32) + mix
    hidden = layer_norm(stream, gain_ref[0:1, :]).astype(BF16)
    hid_ref[...] = hidden
    store_chunks(mm(choose_ref[...], hidden), out_ref, scr)


def dispatch(arrived, residual, gain, choose, peers):
    rows, width = residual.shape
    lines = choose.shape[0] * width // LANES
    return pl.pallas_call(
        dispatch_body,
        out_shape=(
            near_shape((rows, width), BF16),
            near_shape((peers, lines // peers, LANES), BF16),
        ),
        in_specs=vmem(4),
        out_specs=tuple(vmem(2)),
        scratch_shapes=[pltpu.VMEM((lines, LANES), F32)],
        interpret=INTERPRET,
        compiler_params=PARAMS,
        name="dispatch",
    )(near(arrived), residual, gain, near(choose))


def hand_on(*arrays):
    count = len(arrays)

    def body(*refs):
        del refs

    return pl.pallas_call(
        body,
        out_shape=tuple(jax.ShapeDtypeStruct(x.shape, x.dtype) for x in arrays),
        in_specs=[ANY_SPEC] * count,
        out_specs=tuple([ANY_SPEC] * count),
        input_output_aliases={k: k for k in range(count)},
        interpret=INTERPRET,
        compiler_params=PARAMS,
        name="hand_on",
    )(*map(far, arrays))


def fetch(*arrays):
    count = len(arrays)

    def body(*refs):
        sems = refs[-1]
        copies = [
            pltpu.make_async_copy(refs[k], refs[count + k], sems.at[k]) for k in range(count)
        ]
        for copy in copies:
            copy.start()
        for copy in copies:
            copy.wait()

    return pl.pallas_call(
        body,
        out_shape=tuple(near_shape(x.shape, x.dtype) for x in arrays),
        in_specs=[ANY_SPEC] * count,
        out_specs=tuple(vmem(count)),
        scratch_shapes=[pltpu.SemaphoreType.DMA((count,))],
        interpret=INTERPRET,
        compiler_params=PARAMS,
        name="fetch",
    )(*map(far, arrays))


def pack_weights_body(part_ref, gate_ref, up_ref, down_ref, out_ref):
    _, width, units = gate_ref.shape
    half = units // 2
    part = part_ref[0]
    low = part == 0
    left = iota((width, units), 1) < half
    gate = gate_ref[0].astype(F32)
    up = up_ref[0].astype(F32)
    gate = jnp.where(low, gate, pltpu.roll(gate, half, 1))
    up = jnp.where(low, pltpu.roll(up, half, 1), up)
    out_ref[:width, :] = jnp.where(left, gate, up).astype(BF16)
    rows = pl.ds(pl.multiple_of(part * half, half), half)
    for k in range(width // units):
        out_ref[width + k * half : width + (k + 1) * half, :] = down_ref[
            0, rows, k * units : (k + 1) * units
        ]


def pack_weights(part, gate, up, down):
    _, width, units = gate.shape
    return pl.pallas_call(
        pack_weights_body,
        out_shape=jax.ShapeDtypeStruct((width + width // 2, units), BF16),
        in_specs=[SMEM_SPEC] + vmem(3),
        out_specs=vmem(1)[0],
        interpret=INTERPRET,
        compiler_params=PARAMS,
        name="pack_weights",
    )(part, far(gate), far(up), far(down))


def expert_body(x_ref, *refs):
    *held, out_ref, x_scr, blocks, acc_ref, sems = refs
    fetched, _, units = blocks.shape
    count = len(held)
    rows, width = out_ref.shape
    half = units // 2
    copies = [pltpu.make_async_copy(held[k], blocks.at[k], sems.at[k]) for k in range(fetched)]
    for copy in copies:
        copy.start()

    def weights(k, at, size):
        if k < fetched:
            return blocks[k, at : at + size, :]
        return held[k][at : at + size, :]

    x = load_chunks(x_ref, rows, x_scr)
    left = iota((rows, units), 1) < half

    def silu(v):
        return v / (1.0 + jnp.exp(-v))

    group = 4
    for first in range(0, count, group):
        hidden = []
        for k in range(first, first + group, 2):
            for j in (k, k + 1):
                if j < fetched:
                    copies[j].wait()
            both = mm(
                x, jnp.concatenate([weights(k, 0, width), weights(k + 1, 0, width)], axis=1)
            )
            one, two = both[:, :units], both[:, units:]
            one = silu(one) * pltpu.roll(one, half, 1)
            two = silu(pltpu.roll(two, half, 1)) * two
            hidden.append(jnp.where(left, one, two).astype(BF16))
        hidden = jnp.concatenate(hidden, axis=1)
        for c in range(0, width // units, 2):
            cols = []
            for j in (c, c + 1):
                at = width + j * half
                cols.append(
                    jnp.concatenate(
                        [weights(k, at, half) for k in range(first, first + group)], axis=0
                    )
                )
            part = mm(hidden, jnp.concatenate(cols, axis=1))
            cut = slice(c * units, (c + 2) * units)
            if first == 0:
                acc_ref[:, cut] = part
            elif first < count - group:
                acc_ref[:, cut] += part
            else:
                out_ref[:, cut] = (acc_ref[:, cut] + part).astype(out_ref.dtype)


def experts(x, blocks, late, dtype):
    depth, units = blocks[0].shape
    width = depth * 2 // 3
    lines = x.shape[0] * x.shape[1]
    rows = lines * LANES // width
    return pl.pallas_call(
        expert_body,
        out_shape=near_shape((rows, width), dtype),
        in_specs=vmem(1) + [ANY_SPEC] * len(blocks) + vmem(len(late)),
        out_specs=vmem(1)[0],
        scratch_shapes=[
            pltpu.VMEM((lines, LANES), F32),
            pltpu.VMEM((len(blocks), depth, units), BF16),
            pltpu.VMEM((rows, width), F32),
            pltpu.SemaphoreType.DMA((len(blocks),)),
        ],
        interpret=INTERPRET,
        compiler_params=PARAMS,
        name="experts",
    )(near(x), *map(far, blocks), *map(near, late))


def finish_body(mine_ref, arrived_ref, out_ref, scr):
    store_chunks(mine_ref[...] + arrived_ref[...].astype(F32), out_ref, scr)


def finish(mine, arrived, peers):
    rows, width = mine.shape
    lines = rows * width // LANES
    return pl.pallas_call(
        finish_body,
        out_shape=near_shape((peers, lines // peers, LANES), BF16),
        in_specs=vmem(2),
        out_specs=vmem(1)[0],
        scratch_shapes=[pltpu.VMEM((lines, LANES), F32)],
        interpret=INTERPRET,
        compiler_params=PARAMS,
        name="finish",
    )(near(mine), near(arrived))


def combine_body(ret_ref, hid_ref, gain_ref, w_ref, out_ref, scr):
    hidden = hid_ref[...]
    weights = w_ref[...]
    returned = load_chunks(ret_ref, weights.shape[1], scr)
    hi = weights.astype(BF16)
    rest = weights - hi.astype(F32)
    mid = rest.astype(BF16)
    low = (rest - mid.astype(F32)).astype(BF16)
    ffn = mm(hi, returned) + mm(mid, returned) + mm(low, returned)
    stream = RESIDUAL_SCALE * hidden.astype(F32) + ffn
    out_ref[...] = layer_norm(stream, gain_ref[1:2, :]).astype(BF16)


def combine(returned, hidden, gain, weights):
    lines = returned.shape[0] * returned.shape[1]
    return pl.pallas_call(
        combine_body,
        out_shape=jax.ShapeDtypeStruct(hidden.shape, BF16),
        in_specs=vmem(4),
        out_specs=vmem(1)[0],
        scratch_shapes=[pltpu.VMEM((lines, LANES), F32)],
        interpret=INTERPRET,
        compiler_params=PARAMS,
        name="combine",
    )(near(returned), near(hidden), gain, near(weights))


def exchange(array, axis):
    return lax.all_to_all(array, axis, split_axis=0, concat_axis=0, tiled=True)


def shards(
    query_a, key_a, value_a, decay_a, query_b, key_b, value_b, decay_b, out_weight_a,
    out_weight_b, residual, norm_gain, route_group, route_expert, route_weight, expert_gate,
    expert_up, expert_down,
):
    length = query_a.shape[0]
    chips = lax.axis_size("sp_0")
    sp_count = lax.axis_size(SP)
    tp = lax.axis_size("tp")
    rows_dev, width = residual.shape
    routes = rows_dev * TOP
    part = (lax.axis_index("grp") % 2).astype(jnp.int32).reshape(1)
    partner = [(k, k ^ 1) for k in range(lax.axis_size("grp"))]
    up_ring = [(k, (k + 1) % tp) for k in range(tp)]
    down_ring = [(k, (k - 1) % tp) for k in range(tp)]

    core = lax.axis_index("sp_1").astype(jnp.int32).reshape(1)
    local, base = angle_tables(
        length, query_a.shape[1] // 2, query_b.shape[1] // 4, sp_count
    )
    index = lax.axis_index(SP).astype(jnp.int32).reshape(1)
    qa, ka, qb, kb, pay, dec = retention_state(
        index, query_a, key_a, value_a, query_b, key_b, value_b, decay_a, decay_b,
        jnp.asarray(local), jnp.asarray(base),
    )
    swap = [(0, 1), (1, 0)]
    pay_other = lax.ppermute(pay, "sp_1", swap)
    packed = pack_weights(part, expert_gate, expert_up, expert_down)
    blocks = [packed]

    def start(array, ring):
        return lax.ppermute(array, "tp", ring)

    def arrive(array):
        held = hand_on(array)[0]
        blocks.append(held)
        return held

    above = start(packed, up_ring)
    outgoing_states = pack_states(core, pay, pay_other, chips)
    pieces = exchange(outgoing_states, "sp_0")
    below = start(packed, down_ring)
    above = start(arrive(above), up_ring)
    loc = retention_pairs(qa, ka, value_a, qb, kb, value_b, dec)
    per = value_a.shape[1] // LANES * TILE // chips
    scanned = scan_states(core, pieces, per)
    carried = exchange(scanned, "sp_0")
    below = start(arrive(below), down_ring)
    above = start(arrive(above), up_ring)
    out_a, out_b = fetch(out_weight_a, out_weight_b)
    carried_other = lax.ppermute(carried, "sp_1", swap)
    partial = mix_project(
        core, qa, qb, loc, carried, carried_other, pay_other, dec, out_a, out_b
    )
    arrived = exchange(partial.reshape(tp, rows_dev, width), "tp")
    ids = (route_group[:, None] * EXP_GROUP + route_expert).reshape(1, routes)
    choose, weights = route(ids, route_weight.reshape(1, routes), rows_dev)
    hidden, outgoing = dispatch(arrived, residual, norm_gain, choose, sp_count)
    received = exchange(outgoing, SP)
    above = start(arrive(above), up_ring)
    below = start(arrive(below), down_ring)
    received_other = lax.ppermute(received, "grp", partner)
    send = experts(received_other, blocks, [above, below], BF16)
    arrived_sums = lax.ppermute(send, "grp", partner)
    mine = experts(received, blocks, [above, below], F32)
    back = finish(mine, arrived_sums, sp_count)
    returned = exchange(back, SP)
    return combine(returned, hidden, norm_gain, weights)


def solution(mesh):
    sp = mesh.shape["sp"]
    finer = Mesh(
        mesh.devices.reshape(mesh.shape["grp"], sp // 2, 2, mesh.shape["tp"]),
        ("grp", "sp_0", "sp_1", "tp"),
    )
    in_specs = (
        P(GRP_SP, "tp"),
        P(GRP_SP, "tp"),
        P(GRP_SP, "tp"),
        P(None, "tp", GRP_SP),
        P(GRP_SP, "tp"),
        P(GRP_SP, "tp"),
        P(GRP_SP, "tp"),
        P(None, "tp", GRP_SP),
        P("tp", None),
        P("tp", None),
        P(GRP_SP_TP, None),
        P(),
        P(GRP_SP_TP),
        P(GRP_SP_TP, None),
        P(GRP_SP_TP, None),
        P(SP, None, "tp"),
        P(SP, None, "tp"),
        P(SP, "tp", None),
    )
    out_specs = P(GRP_SP_TP, None)

    return jax.shard_map(
        shards, mesh=finer, in_specs=in_specs, out_specs=out_specs, check_vma=False
    )
```
